512 devices in a mesh: ep: 32 (over z, core), tp: 16 (over y, x).
Axes of the slice: x: 4, y: 4, z: 16, core: 2. Of those that a mesh axis runs over, the one named last changes fastest.
Arguments:
- query_maps: bfloat16 [4096, 16, 128], P('ep', 'tp'), may hold values from -6 to 6
- key_maps: bfloat16 [4096, 16, 128], P('ep', 'tp'), may hold values from -6 to 6
- value_rows: bfloat16 [4096, 16, 128], P('ep', 'tp'), may hold values from -6 to 6
- head_lambda: float32 [16], P('tp'), may hold values from 0.3 to 0.8
- head_gain: float32 [128], replicated, may hold values from 0.1 to 1.9
- out_weight: bfloat16 [2048, 2048], P('tp'), may hold values from -0.125 to 0.125
- token_rows: bfloat16 [4096, 2048], P('ep'), may hold values from -36 to 36
- norm_gain: float32 [2048], replicated, may hold values from 0.1 to 1.9
- expert_ids: int32 [4096, 4], P('ep'), may hold values from 0 to 31, all different within a row; in each aligned block of 128 rows (0 to 127, 128 to 255, ...) at most 20 rows name the same one
- route_weights: float32 [4096, 4], P('ep'), may hold values from 0.1 to 0.5
- gate_weight: bfloat16 [32, 2048, 4096], P('ep', None, 'tp'), may hold values from -0.82864076 to 0.82864076
- up_weight: bfloat16 [32, 2048, 4096], P('ep', None, 'tp'), may hold values from -0.82864076 to 0.82864076
- down_weight: bfloat16 [32, 4096, 2048], P('ep', 'tp'), may hold values from -0.03125 to 0.03125
Outputs:
- mixed_rows: bfloat16 [4096, 2048], P(('ep', 'tp'))
- mixed_experts: bfloat16 [4096, 2048], P('ep', 'tp')
The draws below stay inside these ranges and needn't reach their ends.
Inputs may be any that keep to these rules, and one draw needn't show every extreme that they name: `expert_ids`: each row names 4 different experts. Among the rows of one index of ep no expert is named more than 20 times, and in every draw some expert is named exactly 20 times there.
All inputs are finite; a program needn't handle non-finite values.
Results may differ from the reference program's by a relative error of at most 0.015.
Values may be sent and summed in bfloat16 or wider, within the bound.
No kernel may reach another device: no remote copies, remote signals or barrier semaphores. Data moves between devices by JAX's collectives and lax.ppermute only.
A program may use at most 64 MiB of HBM per device.

```python
import math
import jax
import jax.numpy as jnp
import numpy as np
from jax import lax

D = 2048
HEADS = 16
HEAD_DIM = 64
FF = 4096
TOPK = 4
TOKB_DEV = 128
EXPERTS = 32
TOKA = 4096
TOKB = 4096
CAP = 20
N_EP = 32
N_TP = 16


def score_pair(key):
    parts = jax.random.split(jax.random.fold_in(key, 11), 3)
    full_shape = (TOKA, HEADS, 2 * HEAD_DIM)
    query_vals = jnp.clip(1.3 * jax.random.normal(parts[1], full_shape, jnp.float32), -6.0, 6.0)
    key_vals = jnp.clip(1.3 * jax.random.normal(parts[2], full_shape, jnp.float32), -6.0, 6.0)
    return (query_vals.astype(jnp.bfloat16), key_vals.astype(jnp.bfloat16))


def draw_query_maps(key, part):
    return score_pair(key)[0]


def draw_key_maps(key, part):
    return score_pair(key)[1]


def draw_token_rows(key, part):
    parts = jax.random.split(jax.random.fold_in(key, 23), 3)
    row_scales = jnp.exp(jax.random.uniform(parts[0], (TOKB, 1), jnp.float32, math.log(0.3), math.log(3.0)))
    values = jnp.clip(jax.random.normal(parts[1], (TOKB, D), jnp.float32), -4.0, 4.0)
    col_scales = jnp.exp(jax.random.uniform(parts[2], (1, D), jnp.float32, math.log(0.3), math.log(3.0)))
    return (values * row_scales * col_scales).astype(jnp.bfloat16)


def expert_matrix(key, salt_value):
    parts = jax.random.split(jax.random.fold_in(key, salt_value), 1)
    full_shape = (EXPERTS, D, FF)
    values = jnp.clip(jax.random.normal(parts[0], full_shape, jnp.float32), -6.0, 6.0) * (2.5 * D ** (-0.5))
    return values.astype(jnp.bfloat16)


def draw_gate_weight(key, part):
    return expert_matrix(key, 31)


def draw_up_weight(key, part):
    return expert_matrix(key, 37)


def block_levels(own_key, shape, shards, smallest, high):
    def one(axis_at, shards_of):
        heights = jax.random.uniform(jax.random.fold_in(jax.random.fold_in(own_key, 6), axis_at), (shards_of,), jnp.float32, smallest / len(shards), high / len(shards))
        return jnp.repeat(jnp.exp(heights), shape[axis_at] // shards_of).reshape((-1,) + (1,) * (len(shape) - axis_at - 1))

    gain = one(*shards[0])
    for cut in shards[1:]:
        gain = gain * one(*cut)
    return gain


def assign_block(stream_key, own, number, rows, number_of, top, limit, lean):
    ranking = jax.random.permutation(stream_key, number_of)
    crowded, common = load_shares(number_of, rows * top, limit, lean, True), load_shares(number_of, rows * top, limit, lean, False)
    places = jnp.arange(number_of)

    def named(sizes, rotation):
        used = int((sizes > 0).sum())
        fixed = max(1, used // 4)
        moved = fixed + (places - fixed + rotation * (used - fixed)) % max(1, number_of - fixed)
        return jnp.zeros((number_of,), jnp.int32).at[ranking[jnp.where(places < fixed, places, moved)]].set(jnp.asarray(sizes, jnp.int32))

    sizes = jnp.where(number % 4 == 0, named(crowded, number // 4), named(common, number - number // 4 - 1))
    mixed = jax.random.permutation(jax.random.fold_in(own, 3), number_of)
    giver, receiver = mixed[0:number_of // 2 * 2:2], mixed[1:number_of // 2 * 2:2]
    margin = jnp.minimum(sizes[giver] - 1, limit - sizes[receiver]) // 2
    margin = jnp.where((giver == ranking[0]) | (receiver == ranking[0]) | (sizes[receiver] == 0), 0, jnp.maximum(margin, 0))
    moved = jax.random.randint(jax.random.fold_in(own, 4), (number_of // 2,), 0, 1 << 20) % (margin + 1)
    sizes = sizes.at[giver].add(-moved).at[receiver].add(moved)
    members = jnp.searchsorted(jnp.cumsum(sizes), jnp.arange(rows * top), side="right").astype(jnp.int32)
    table = members.reshape(top, rows).T
    table = table[jax.random.permutation(jax.random.fold_in(own, 1), rows)]
    rotation = jax.random.randint(jax.random.fold_in(own, 2), (rows, 1), 0, top)
    return jnp.take_along_axis(table, (jnp.arange(top)[None, :] + rotation) % top, axis=1)


def load_shares(number_of, total, limit, lean, full):
    loads = [(1 << 20) // math.isqrt(rank ** lean) + 1 for rank in range(1, number_of + 1)]
    largest = limit if full else min(limit, max(-(-total // number_of), total * loads[0] // sum(loads)))
    least = 1 if total - largest >= number_of - 1 else 0
    given, spare = [largest] + [least] * (number_of - 1), total - largest - least * (number_of - 1)
    while spare > 0:
        movable = [i for i in range(1, number_of) if given[i] < largest] or [i for i in range(1, number_of) if given[i] < limit]
        mass, left = sum([loads[i] for i in movable]), spare
        for i in movable:
            extra = min(limit - given[i], max(1, left * loads[i] // mass), spare)
            given[i] = given[i] + extra
            spare = spare - extra
    return np.array(given)


def scatter_about(stream_key, dims, width, most, cuts=(), kind=jnp.bfloat16):
    entries = width * jax.random.normal(stream_key, dims, jnp.float32)
    if cuts:
        entries = entries * block_levels(stream_key, dims, cuts, -0.22, 0.18)
    return jnp.clip(entries, -most, most).astype(kind)


def setup_inputs(seed: int = 0) -> dict:
    keys = jax.random.split(jax.random.key(seed), 14)
    query_maps = draw_query_maps(jax.random.fold_in(keys[13], 71), 0)
    key_maps = draw_key_maps(jax.random.fold_in(keys[13], 71), 0)
    value_rows = scatter_about(keys[2], (TOKA, HEADS, 2 * HEAD_DIM), 1.0, 6.0, ((0, 32), (1, 16)))
    head_lambda = jnp.clip(0.3 + 0.5 * jax.random.uniform(keys[3], (HEADS,), jnp.float32) ** block_levels(keys[3], (HEADS,), ((0, 16),), -0.2, 0.2), 0.3, 0.8)
    head_gain = jnp.clip(1.0 + 0.18 * jax.random.normal(keys[4], (2 * HEAD_DIM,), jnp.float32), 0.1, 1.9)
    out_weight = scatter_about(keys[5], (HEADS * 2 * HEAD_DIM, D), (HEADS * 2 * HEAD_DIM) ** -0.5, 0.125, ((0, 16),))
    token_rows = draw_token_rows(jax.random.fold_in(keys[13], 71), 0)
    norm_gain = jnp.clip(1.0 + 0.18 * jax.random.normal(keys[7], (D,), jnp.float32), 0.1, 1.9)
    expert_ids_keys = jax.random.split(jax.random.fold_in(keys[8], 1), TOKB // TOKB_DEV)
    expert_ids_turns = jax.random.permutation(jax.random.fold_in(keys[8], 3), TOKB // TOKB_DEV)
    expert_ids = jax.vmap(lambda own, number: assign_block(jax.random.fold_in(keys[8], 2), own, number, TOKB_DEV, EXPERTS, TOPK, CAP, 1))(expert_ids_keys, expert_ids_turns).reshape((TOKB, TOPK))
    route_weights = jnp.clip(0.1 + 0.4 * jax.random.uniform(keys[9], (TOKB, TOPK), jnp.float32) ** block_levels(keys[9], (TOKB, TOPK), ((0, 32),), -0.2, 0.2), 0.1, 0.5)
    gate_weight = draw_gate_weight(jax.random.fold_in(keys[13], 71), 0)
    up_weight = draw_up_weight(jax.random.fold_in(keys[13], 71), 0)
    down_weight = scatter_about(keys[12], (EXPERTS, FF, D), (8 * FF) ** -0.5, 0.03125, ((0, 32), (1, 16)))
    return dict(query_maps=query_maps, key_maps=key_maps, value_rows=value_rows, head_lambda=head_lambda, head_gain=head_gain, out_weight=out_weight, token_rows=token_rows, norm_gain=norm_gain, expert_ids=expert_ids, route_weights=route_weights, gate_weight=gate_weight, up_weight=up_weight, down_weight=down_weight)


NORM_EPS = 1e-05
CLAMP_LIMIT = 7.0
GATE_SLOPE = 1.702

def rounded(values):
    return lax.optimization_barrier(values.astype(jnp.bfloat16)).astype(jnp.float32)

def mixer_half(query_maps, key_maps, value_rows, head_lambda, head_gain, out_weight):
    head_width = HEAD_DIM
    score_scale = head_width ** (-0.5)
    block_len = math.gcd(TOKA, 256)
    key_float = key_maps.astype(jnp.float32)
    value_float = value_rows.astype(jnp.float32)
    outputs = []
    for begin_at in range(0, TOKA, block_len):
        ending = begin_at + block_len
        query_float = query_maps[begin_at:ending].astype(jnp.float32)
        query_pos = begin_at + jnp.arange(block_len, dtype=jnp.int32)
        key_pos = jnp.arange(ending, dtype=jnp.int32)
        causal = key_pos[None, :] <= query_pos[:, None]
        results = []
        for map_index in range(2):
            col_low = map_index * head_width
            col_high = col_low + head_width
            scores = jnp.einsum('qhd,khd->hqk', query_float[:, :, col_low:col_high], key_float[:ending, :, col_low:col_high]) * score_scale
            scores = jnp.where(causal[None], scores, -jnp.inf)
            row_max = lax.optimization_barrier(jnp.max(scores, axis=-1, keepdims=True))
            exp_terms = jnp.exp(scores - row_max)
            denominator = lax.optimization_barrier(jnp.sum(exp_terms, axis=-1))
            weights = rounded(exp_terms)
            numerator = jnp.einsum('hqk,khd->qhd', weights, value_float[:ending])
            results.append(numerator / jnp.transpose(denominator)[:, :, None])
        attended = results[0] - head_lambda[None, :, None] * results[1]
        mean_sq = lax.optimization_barrier(jnp.mean(attended * attended, axis=-1, keepdims=True))
        normed = attended * lax.rsqrt(mean_sq + NORM_EPS) * head_gain
        outputs.append(normed.astype(jnp.bfloat16))
    head_rows = jnp.concatenate(outputs, axis=0).reshape(TOKA, HEADS * 2 * HEAD_DIM)
    group_width = HEADS * 2 * HEAD_DIM // N_TP
    summed = jnp.zeros((TOKA, D), jnp.float32)
    for group_index in range(N_TP):
        group_rows = head_rows[:, group_index * group_width:(group_index + 1) * group_width]
        group_weight = out_weight[group_index * group_width:(group_index + 1) * group_width]
        summed = summed + rounded(jnp.dot(group_rows, group_weight, preferred_element_type=jnp.float32))
    return summed.astype(jnp.bfloat16)

def expert_half(token_rows, norm_gain, expert_ids, route_weights, gate_weight, up_weight, down_weight):
    rows_float = token_rows.astype(jnp.float32)
    mean_sq = lax.optimization_barrier(jnp.mean(rows_float * rows_float, axis=-1, keepdims=True))
    normed = (rows_float * lax.rsqrt(mean_sq + NORM_EPS) * norm_gain).astype(jnp.bfloat16)
    flat_ids = expert_ids.reshape(N_EP, TOKB_DEV * TOPK)
    onehot = (flat_ids[:, :, None] == jnp.arange(EXPERTS, dtype=jnp.int32)[None, None, :]).astype(jnp.int32)
    rank_before = jnp.cumsum(onehot, axis=1) - onehot
    slot_of = lax.optimization_barrier(jnp.sum(rank_before * onehot, axis=2)).astype(jnp.int32)
    sources = jnp.arange(N_EP, dtype=jnp.int32)[:, None]
    token_of = sources * TOKB_DEV + jnp.arange(TOKB_DEV * TOPK, dtype=jnp.int32)[None, :] // TOPK
    row_index = sources * CAP + slot_of
    slot_table = jnp.full((EXPERTS, N_EP * CAP), TOKB, jnp.int32).at[flat_ids, row_index].set(token_of)
    padded = jnp.concatenate([normed, jnp.zeros((1, D), jnp.bfloat16)], axis=0)

    def one_expert(inputs):
        row_ids, gate_matrix, up_matrix, down_matrix = inputs
        chosen = padded[row_ids]
        gate_pre = jnp.dot(chosen, gate_matrix, preferred_element_type=jnp.float32)
        up_pre = jnp.dot(chosen, up_matrix, preferred_element_type=jnp.float32)
        gated = jnp.minimum(gate_pre, CLAMP_LIMIT)
        clipped = jnp.clip(up_pre, -CLAMP_LIMIT, CLAMP_LIMIT)
        active = rounded((clipped + 1.0) * gated * jax.nn.sigmoid(GATE_SLOPE * gated))
        grouped = active.reshape(N_EP * CAP, N_TP, FF // N_TP)
        down_grouped = down_matrix.astype(jnp.float32).reshape(N_TP, FF // N_TP, D)
        terms = jnp.einsum('rgf,gfd->rgd', grouped, down_grouped)
        return lax.optimization_barrier(jnp.sum(rounded(terms), axis=1)).astype(jnp.bfloat16)
    expert_out = lax.map(one_expert, (slot_table, gate_weight, up_weight, down_weight))
    picked = expert_out[flat_ids.reshape(-1), row_index.reshape(-1)].astype(jnp.float32)
    combined = lax.optimization_barrier(jnp.sum(picked.reshape(TOKB, TOPK, D) * route_weights[:, :, None], axis=1))
    return combined.astype(jnp.bfloat16)

def reference(query_maps, key_maps, value_rows, head_lambda, head_gain, out_weight, token_rows, norm_gain, expert_ids, route_weights, gate_weight, up_weight, down_weight):
    mixed_rows = mixer_half(query_maps, key_maps, value_rows, head_lambda, head_gain, out_weight)
    mixed_experts = expert_half(token_rows, norm_gain, expert_ids, route_weights, gate_weight, up_weight, down_weight)
    return (mixed_rows, mixed_experts)
```

```python
import jax
import jax.numpy as jnp
from jax import lax
from jax.experimental import pallas as pl
from jax.experimental.pallas import tpu as pltpu
from jax.sharding import Mesh, PartitionSpec as P

NORM_EPS = 1e-05
CLAMP_LIMIT = 7.0
GATE_SLOPE = 1.702
BF16 = jnp.bfloat16
F32 = jnp.float32

Z, CORE, Y, X = 16, 2, 4, 4
EP = ("z", "core")
TP = ("y", "x")
N_EP = Z * CORE
N_TP = Y * X
TOK = 128
CAP = 20
PAD = 24
ROWS = N_EP * CAP
PADDED = N_EP * PAD
WIDE = 128
MODEL = N_TP * WIDE
OUT_ROWS = ROWS + TOK

LANE_OFFSETS = (-4, 0, 4, 8, -5, -1, 3, 7, -3, 1, 5, 9, -6, -2, 2, 6)


def routing(ids, values=None):
    expert = lax.broadcasted_iota(jnp.int32, (N_EP, TOK), 0)
    named = jnp.zeros((N_EP, TOK), F32)
    weight = jnp.zeros((N_EP, TOK), F32)
    for k in range(ids.shape[0]):
        hit = ids[k : k + 1, :] == expert
        named = named + jnp.where(hit, 1.0, 0.0)
        if values is not None:
            weight = weight + jnp.where(hit, values[k : k + 1, :], 0.0)
    earlier = lax.broadcasted_iota(jnp.int32, (TOK, TOK), 0) < lax.broadcasted_iota(
        jnp.int32, (TOK, TOK), 1
    )
    rank = jnp.dot(
        named.astype(BF16),
        jnp.where(earlier, 1.0, 0.0).astype(BF16),
        preferred_element_type=F32,
    )
    slot = jnp.where(named > 0.5, rank.astype(jnp.int32), -1)
    place = lax.broadcasted_iota(jnp.int32, (PAD, TOK), 0)
    pieces = []
    for e in range(N_EP):
        here = slot[e : e + 1, :] == place
        pieces.append(jnp.where(here, 1.0 if values is None else weight[e : e + 1, :], 0.0))
    return jnp.concatenate(pieces, axis=0)


def dispatch_kernel(at_ref, rows_ref, part_ref, gain_ref, ids_ref, out_ref):
    rows = rows_ref[...].astype(F32)
    mean_sq = jnp.mean(rows * rows, axis=-1, keepdims=True)
    part = part_ref[...].astype(F32) * lax.rsqrt(mean_sq + NORM_EPS) * gain_ref[...]
    chosen = routing(ids_ref[...]).astype(BF16)
    packed = jnp.dot(chosen, part.astype(BF16), preferred_element_type=F32)
    out_ref[...] = packed.astype(BF16).reshape(N_EP, PAD, WIDE)


def dispatch(at, token_rows, gain, ids):
    return pl.pallas_call(
        dispatch_kernel,
        out_shape=jax.ShapeDtypeStruct((N_EP, PAD, WIDE), BF16),
        grid_spec=pltpu.PrefetchScalarGridSpec(
            num_scalar_prefetch=1,
            grid=(1,),
            in_specs=[
                pl.BlockSpec((TOK, MODEL), lambda i, at: (0, 0)),
                pl.BlockSpec((TOK, WIDE), lambda i, at: (0, at[0])),
                pl.BlockSpec((1, WIDE), lambda i, at: (0, at[0])),
                pl.BlockSpec((4, TOK), lambda i, at: (0, 0)),
            ],
            out_specs=pl.BlockSpec((N_EP, PAD, WIDE), lambda i, at: (0, 0, 0)),
        ),
        name="dispatch",
    )(at, token_rows, token_rows, gain, ids)


def compact_kernel(in_ref, out_ref):
    to = lax.broadcasted_iota(jnp.int32, (2 * CAP, 2 * PAD), 0)
    src = lax.broadcasted_iota(jnp.int32, (2 * CAP, 2 * PAD), 1)
    pick = jnp.where(src == jnp.where(to < CAP, to, to + (PAD - CAP)), 1.0, 0.0).astype(BF16)
    for g in range(N_EP // 2):
        block = in_ref[2 * g : 2 * g + 2].reshape(2 * PAD, WIDE)
        kept = jnp.dot(pick, block, preferred_element_type=F32).astype(BF16)
        for t in range(N_TP):
            out_ref[t, 2 * CAP * g : 2 * CAP * (g + 1), :] = kept


def compact(arrived):
    return pl.pallas_call(
        compact_kernel,
        out_shape=jax.ShapeDtypeStruct((N_TP, ROWS, WIDE), BF16),
        name="compact",
    )(arrived)


SPLIT = OUT_ROWS // 2


def ffn_rows(x_ref, wg_ref, wu_ref, wd_ref, out_ref, count):
    rows = jnp.concatenate([x_ref[t, :count, :] for t in range(N_TP)], axis=-1)
    gate = jnp.dot(rows, wg_ref[...], preferred_element_type=F32)
    up = jnp.dot(rows, wu_ref[...], preferred_element_type=F32)
    gated = jnp.minimum(gate, CLAMP_LIMIT)
    clipped = jnp.clip(up, -CLAMP_LIMIT, CLAMP_LIMIT)
    active = ((clipped + 1.0) * gated * jax.nn.sigmoid(GATE_SLOPE * gated)).astype(BF16)
    terms = jnp.dot(active, wd_ref[...], preferred_element_type=F32).astype(BF16)
    for t in range(N_TP):
        out_ref[t, :count, :] = terms[:, t * WIDE : (t + 1) * WIDE]


def ffn_kernel(x_ref, wg_ref, wu_ref, wd_ref, proj_ref, out_ref):
    step = pl.program_id(0)

    @pl.when(step == 0)
    def _():
        ffn_rows(x_ref, wg_ref, wu_ref, wd_ref, out_ref, SPLIT)

    @pl.when(step == 1)
    def _():
        ffn_rows(x_ref, wg_ref, wu_ref, wd_ref, out_ref, ROWS - SPLIT)
        out_ref[:, ROWS - SPLIT :, :] = proj_ref[...]


def ffn(x, wg, wu, wd, proj):
    whole = lambda *shape: pl.BlockSpec(shape, lambda i: (0,) * len(shape))
    return pl.pallas_call(
        ffn_kernel,
        out_shape=jax.ShapeDtypeStruct((N_TP, OUT_ROWS, WIDE), BF16),
        grid=(2,),
        in_specs=[
            pl.BlockSpec((N_TP, SPLIT, WIDE), lambda i: (0, i, 0)),
            whole(*wg.shape),
            whole(*wu.shape),
            whole(*wd.shape),
            whole(*proj.shape),
        ],
        out_specs=pl.BlockSpec((N_TP, SPLIT, WIDE), lambda i: (0, i, 0)),
        name="ffn",
    )(x, wg, wu, wd, proj)


REDUCE_STEPS = 4
REDUCE_ROWS = ROWS // REDUCE_STEPS
REDUCE_SRC = N_EP // REDUCE_STEPS


def reduce_kernel(in_ref, pack_ref, mixed_ref):
    step = pl.program_id(0)
    summed = in_ref[0].astype(F32)
    for t in range(1, N_TP):
        summed = summed + in_ref[t].astype(F32)
    summed = summed.astype(BF16)

    @pl.when(step < REDUCE_STEPS)
    def _():
        to = lax.broadcasted_iota(jnp.int32, (2 * PAD, 2 * CAP), 0)
        src = lax.broadcasted_iota(jnp.int32, (2 * PAD, 2 * CAP), 1)
        hit = to == jnp.where(src < CAP, src, src + (PAD - CAP))
        place = jnp.where(hit, 1.0, 0.0).astype(BF16)
        for g in range(REDUCE_SRC // 2):
            block = summed[2 * CAP * g : 2 * CAP * (g + 1)]
            spread = jnp.dot(place, block, preferred_element_type=F32).astype(BF16)
            pack_ref[2 * g : 2 * g + 2] = spread.reshape(2, PAD, WIDE)

    @pl.when(step == REDUCE_STEPS)
    def _():
        for c in range(N_TP):
            mixed_ref[:, c * WIDE : (c + 1) * WIDE] = summed[8 * c : 8 * (c + 1)]


def reduce_terms(y):
    return pl.pallas_call(
        reduce_kernel,
        out_shape=(
            jax.ShapeDtypeStruct((N_EP, PAD, WIDE), BF16),
            jax.ShapeDtypeStruct((TOK // N_TP, MODEL), BF16),
        ),
        grid=(REDUCE_STEPS + 1,),
        in_specs=[pl.BlockSpec((N_TP, REDUCE_ROWS, WIDE), lambda i: (0, i, 0))],
        out_specs=(
            pl.BlockSpec(
                (REDUCE_SRC, PAD, WIDE), lambda i: (jnp.minimum(i, REDUCE_STEPS - 1), 0, 0)
            ),
            pl.BlockSpec((TOK // N_TP, MODEL), lambda i: (0, 0)),
        ),
        name="reduce_terms",
    )(y)


def combine_kernel(back_ref, ids_ref, weights_ref, out_ref):
    spread = routing(ids_ref[...], weights_ref[...])
    high = spread.astype(BF16)
    low = (spread - high.astype(F32)).astype(BF16)
    back = back_ref[...].reshape(PADDED, WIDE)
    over = (((0,), (0,)), ((), ()))
    mixed = lax.dot_general(high, back, over, preferred_element_type=F32)
    mixed = mixed + lax.dot_general(low, back, over, preferred_element_type=F32)
    out_ref[...] = mixed.astype(BF16)


def combine(back, ids, weights):
    return pl.pallas_call(
        combine_kernel,
        out_shape=jax.ShapeDtypeStruct((TOK, WIDE), BF16),
        name="combine",
    )(back, ids, weights)


def attend_kernel(
    place_ref, lam_ref, q_ref, own_ref, other_ref, gain_ref, w_ref, out_ref, score_ref
):
    q = q_ref[...]
    q = (q.astype(F32) * (64**-0.5)).astype(BF16)
    lane = lax.broadcasted_iota(jnp.int32, (TOK, WIDE), 1)
    zero = jnp.zeros_like(q)
    both = jnp.concatenate(
        [jnp.where(lane < 64, q, zero), jnp.where(lane < 64, zero, q)], axis=0
    )
    row = lax.broadcasted_iota(jnp.int32, (2 * TOK, TOK), 0)
    row = jnp.where(row < TOK, row, row - TOK)
    ahead = lax.broadcasted_iota(jnp.int32, (2 * TOK, TOK), 1) - row
    me = place_ref[N_EP]
    top = jnp.full((2 * TOK, TOK), -1e30, F32)
    for b in range(N_EP):
        ref = own_ref if b < Z else other_ref
        keys = ref[b % Z, :, :WIDE]
        scores = lax.dot_general(
            both, keys, (((1,), (1,)), ((), ())), preferred_element_type=F32
        )
        scores = jnp.where(ahead <= (me - place_ref[b]) * TOK, scores, -1e30)
        score_ref[b] = scores
        top = jnp.maximum(top, scores)
    row_max = jnp.max(top, axis=-1, keepdims=True)
    total = jnp.zeros((2 * TOK, TOK), F32)
    value_sum = jnp.zeros((2 * TOK, WIDE), F32)
    for b in range(N_EP):
        ref = own_ref if b < Z else other_ref
        terms = jnp.exp(score_ref[b] - row_max)
        total = total + terms
        value_sum = value_sum + jnp.dot(
            terms.astype(BF16), ref[b % Z, :, WIDE:], preferred_element_type=F32
        )
    ratio = value_sum / jnp.sum(total, axis=-1, keepdims=True)
    attended = ratio[:TOK] - lam_ref[0] * ratio[TOK:]
    mean_sq = jnp.mean(attended * attended, axis=-1, keepdims=True)
    head_rows = (attended * lax.rsqrt(mean_sq + NORM_EPS) * gain_ref[...]).astype(BF16)
    product = jnp.dot(head_rows, w_ref[...], preferred_element_type=F32).astype(BF16)
    for c in range(N_TP):
        piece = product[:, c * WIDE : (c + 1) * WIDE].reshape(N_TP, TOK // N_TP, WIDE)
        out_ref[:, 8 * c : 8 * (c + 1), :] = piece


def attend(place, lam, q, own, other, gain, w):
    vmem = pl.BlockSpec(memory_space=pltpu.VMEM)
    smem = pl.BlockSpec(memory_space=pltpu.SMEM)
    return pl.pallas_call(
        attend_kernel,
        out_shape=jax.ShapeDtypeStruct((N_TP, TOK, WIDE), BF16),
        in_specs=[smem, smem, vmem, vmem, vmem, vmem, vmem],
        out_specs=vmem,
        scratch_shapes=[pltpu.VMEM((N_EP, 2 * TOK, TOK), F32)],
        name="attend",
    )(place, lam, q, own, other, gain, w)


def shifted(array, axis, by):
    length = lax.axis_size(axis)
    return lax.ppermute(array, axis, [(i, (i + by) % length) for i in range(length)])


def exchanged(array, axes):
    return lax.all_to_all(array, axes, split_axis=0, concat_axis=0, tiled=True)


def collect_keys(keys, values):
    mine = jnp.concatenate([keys, values], axis=-1)
    far = jnp.stack(
        [shifted(mine, "z", 4), mine, shifted(mine, "z", -4), shifted(mine, "z", 8)]
    )
    near = [
        shifted(far, "z", 1),
        shifted(far, "z", -1),
        shifted(far[0:2], "z", 2),
        shifted(far[1:3], "z", -2),
    ]
    return jnp.concatenate([far, *near], axis=0)


def body(
    query_maps,
    key_maps,
    value_rows,
    head_lambda,
    head_gain,
    out_weight,
    token_rows,
    norm_gain,
    expert_ids,
    route_weights,
    gate_weight,
    up_weight,
    down_weight,
):
    z_at = lax.axis_index("z").astype(jnp.int32)
    core_at = lax.axis_index("core").astype(jnp.int32)
    tp_at = lax.axis_index(TP).astype(jnp.int32)
    ids = expert_ids.T
    packed = dispatch(tp_at.reshape(1), token_rows, norm_gain.reshape(1, MODEL), ids)
    arrived = exchanged(packed, EP)

    own = collect_keys(key_maps.reshape(TOK, WIDE), value_rows.reshape(TOK, WIDE))
    other = shifted(own, "core", 1)
    chips = (z_at + jnp.array(LANE_OFFSETS, jnp.int32) + Z) % Z
    place = jnp.concatenate(
        [chips * CORE + core_at, chips * CORE + 1 - core_at, (z_at * CORE + core_at).reshape(1)]
    )
    proj = attend(
        place,
        head_lambda,
        query_maps.reshape(TOK, WIDE),
        own,
        other,
        head_gain.reshape(1, WIDE),
        out_weight,
    )

    x = exchanged(compact(arrived), TP)
    terms = ffn(x, gate_weight[0], up_weight[0], down_weight[0], proj)
    back, mixed_rows = reduce_terms(exchanged(terms, TP))
    mixed_experts = combine(exchanged(back, EP), ids, route_weights.T)
    return (mixed_rows, mixed_experts)


def solution(mesh):
    fine = Mesh(mesh.devices.reshape(Z, CORE, Y, X), ("z", "core", "y", "x"))
    placed = (
        P(EP, TP, None),
        P(EP, TP, None),
        P(EP, TP, None),
        P(TP),
        P(),
        P(TP, None),
        P(EP, None),
        P(),
        P(EP, None),
        P(EP, None),
        P(EP, None, TP),
        P(EP, None, TP),
        P(EP, TP, None),
    )
    return jax.shard_map(
        body,
        mesh=fine,
        in_specs=placed,
        out_specs=(P((*EP, *TP), None), P(EP, TP)),
        check_vma=False,
    )
```

```python
import jax
import jax.numpy as jnp
from jax import lax
from jax.experimental import pallas as pl
from jax.experimental.pallas import tpu as pltpu
from jax.sharding import Mesh, PartitionSpec as P


NORM_EPS = 1e-05
CLAMP_LIMIT = 7.0
GATE_SLOPE = 1.702
BF16 = jnp.bfloat16
F32 = jnp.float32

Z, CORE, Y, X = 16, 2, 4, 4
EP = ("z", "core")
TP = ("y", "x")
N_EP = Z * CORE
N_TP = Y * X
TOK = 128
CAP = 20
PAD = 24
ROWS = N_EP * CAP
PADDED = N_EP * PAD
WIDE = 128
MODEL = N_TP * WIDE
OUT_ROWS = ROWS + TOK

STEPS = (0, 4, 2, 6, 1, 5, 3, 7)
MIB = 1 << 20


def in_vmem(array):
    return pltpu.with_memory_space_constraint(array, pltpu.VMEM)


def params(mib):
    return pltpu.CompilerParams(vmem_limit_bytes=mib * MIB)


def routing(ids, values=None):
    expert = lax.broadcasted_iota(jnp.int32, (N_EP, TOK), 0)
    named = jnp.zeros((N_EP, TOK), F32)
    weight = jnp.zeros((N_EP, TOK), F32)
    for k in range(ids.shape[0]):
        hit = ids[k : k + 1, :] == expert
        named = named + jnp.where(hit, 1.0, 0.0)
        if values is not None:
            weight = weight + jnp.where(hit, values[k : k + 1, :], 0.0)
    earlier = lax.broadcasted_iota(jnp.int32, (TOK, TOK), 0) < lax.broadcasted_iota(
        jnp.int32, (TOK, TOK), 1
    )
    rank = jnp.dot(
        named.astype(BF16),
        jnp.where(earlier, 1.0, 0.0).astype(BF16),
        preferred_element_type=F32,
    )
    slot = jnp.where(named > 0.5, rank.astype(jnp.int32), -1)
    place = lax.broadcasted_iota(jnp.int32, (PAD, TOK), 0)
    pieces = []
    for e in range(N_EP):
        here = slot[e : e + 1, :] == place
        pieces.append(jnp.where(here, 1.0 if values is None else weight[e : e + 1, :], 0.0))
    return jnp.concatenate(pieces, axis=0)


def dispatch_kernel(at_ref, rows_ref, part_ref, gain_ref, ids_ref, out_ref):
    rows = rows_ref[...].astype(F32)
    mean_sq = jnp.mean(rows * rows, axis=-1, keepdims=True)
    part = part_ref[...].astype(F32) * lax.rsqrt(mean_sq + NORM_EPS) * gain_ref[...]
    chosen = routing(ids_ref[...]).astype(BF16)
    packed = jnp.dot(chosen, part.astype(BF16), preferred_element_type=F32)
    out_ref[...] = packed.astype(BF16).reshape(N_EP, PAD, WIDE)


def dispatch(at, token_rows, gain, ids):
    return pl.pallas_call(
        dispatch_kernel,
        out_shape=jax.ShapeDtypeStruct((N_EP, PAD, WIDE), BF16),
        grid_spec=pltpu.PrefetchScalarGridSpec(
            num_scalar_prefetch=1,
            grid=(1,),
            in_specs=[
                pl.BlockSpec((TOK, MODEL), lambda i, at: (0, 0)),
                pl.BlockSpec((TOK, WIDE), lambda i, at: (0, at[0])),
                pl.BlockSpec((1, WIDE), lambda i, at: (0, at[0])),
                pl.BlockSpec((4, TOK), lambda i, at: (0, 0)),
            ],
            out_specs=pl.BlockSpec((N_EP, PAD, WIDE), lambda i, at: (0, 0, 0)),
        ),
        compiler_params=params(8),
        name="dispatch",
    )(at, token_rows, token_rows, gain, ids)


COMPACT_STEPS = 4
COMPACT_SRC = N_EP // COMPACT_STEPS


def compact_kernel(in_ref, out_ref):
    to = lax.broadcasted_iota(jnp.int32, (2 * CAP, 2 * PAD), 0)
    src = lax.broadcasted_iota(jnp.int32, (2 * CAP, 2 * PAD), 1)
    pick = jnp.where(src == jnp.where(to < CAP, to, to + (PAD - CAP)), 1.0, 0.0).astype(BF16)
    for g in range(0, COMPACT_SRC, 2):
        block = in_ref[g : g + 2].reshape(2 * PAD, WIDE)
        kept = jnp.dot(pick, block, preferred_element_type=F32).astype(BF16)
        for t in range(N_TP):
            out_ref[t, CAP * g : CAP * (g + 2), :] = kept


def compact(arrived):
    return pl.pallas_call(
        compact_kernel,
        out_shape=pltpu.HBM((N_TP, ROWS, WIDE), BF16),
        grid=(COMPACT_STEPS,),
        in_specs=[pl.BlockSpec((COMPACT_SRC, PAD, WIDE), lambda i: (i, 0, 0))],
        out_specs=pl.BlockSpec((N_TP, COMPACT_SRC * CAP, WIDE), lambda i: (0, i, 0)),
        compiler_params=params(8),
        name="compact",
    )(arrived)


FFN_ROWS = ROWS // 2


def ffn_kernel(x_ref, wg_hbm, wu_hbm, wd_hbm, proj_ref, out_ref, wg_ref, wu_ref, wd_ref, sems):
    loads = [
        pltpu.make_async_copy(src, dst, sems.at[n])
        for n, (src, dst) in enumerate(((wg_hbm, wg_ref), (wu_hbm, wu_ref), (wd_hbm, wd_ref)))
    ]
    for load in loads:
        load.start()
    out_ref[:, ROWS:, :] = proj_ref[...]
    for low in range(0, ROWS, FFN_ROWS):
        here = slice(low, low + FFN_ROWS)
        rows = jnp.concatenate([x_ref[t, here, :] for t in range(N_TP)], axis=-1)
        if low == 0:
            loads[0].wait()
        gate = jnp.dot(rows, wg_ref[...], preferred_element_type=F32)
        if low == 0:
            loads[1].wait()
        up = jnp.dot(rows, wu_ref[...], preferred_element_type=F32)
        gated = jnp.minimum(gate, CLAMP_LIMIT)
        clipped = jnp.clip(up, -CLAMP_LIMIT, CLAMP_LIMIT)
        active = ((clipped + 1.0) * gated * jax.nn.sigmoid(GATE_SLOPE * gated)).astype(BF16)
        if low == 0:
            loads[2].wait()
        terms = jnp.dot(active, wd_ref[...], preferred_element_type=F32).astype(BF16)
        for t in range(N_TP):
            out_ref[t, here, :] = terms[:, t * WIDE : (t + 1) * WIDE]


def ffn(x, wg, wu, wd, proj):
    vmem = pl.BlockSpec(memory_space=pltpu.VMEM)
    hbm = pl.BlockSpec(memory_space=pl.ANY)
    return pl.pallas_call(
        ffn_kernel,
        out_shape=pltpu.VMEM((N_TP, OUT_ROWS, WIDE), BF16),
        in_specs=[vmem, hbm, hbm, hbm, vmem],
        out_specs=vmem,
        scratch_shapes=[
            pltpu.VMEM(wg.shape, BF16),
            pltpu.VMEM(wu.shape, BF16),
            pltpu.VMEM(wd.shape, BF16),
            pltpu.SemaphoreType.DMA((3,)),
        ],
        compiler_params=params(16),
        name="ffn",
    )(
        in_vmem(x),
        *(pltpu.with_memory_space_constraint(w, pltpu.HBM) for w in (wg, wu, wd)),
        in_vmem(proj),
    )


def summed_rows(in_ref, low, count):
    total = in_ref[0, low : low + count, :].astype(F32)
    for t in range(1, N_TP):
        total = total + in_ref[t, low : low + count, :].astype(F32)
    return total.astype(BF16)


def reduce_kernel(in_ref, pack_ref, mixed_ref):
    to = lax.broadcasted_iota(jnp.int32, (2 * PAD, 2 * CAP), 0)
    src = lax.broadcasted_iota(jnp.int32, (2 * PAD, 2 * CAP), 1)
    hit = to == jnp.where(src < CAP, src, src + (PAD - CAP))
    place = jnp.where(hit, 1.0, 0.0).astype(BF16)
    for g in range(0, N_EP, 2):
        block = summed_rows(in_ref, CAP * g, 2 * CAP)
        spread = jnp.dot(place, block, preferred_element_type=F32).astype(BF16)
        pack_ref[g : g + 2] = spread.reshape(2, PAD, WIDE)
    for c in range(N_TP):
        mixed_ref[:, c * WIDE : (c + 1) * WIDE] = summed_rows(in_ref, ROWS + 8 * c, 8)


def reduce_terms(y):
    vmem = pl.BlockSpec(memory_space=pltpu.VMEM)
    return pl.pallas_call(
        reduce_kernel,
        out_shape=(
            pltpu.VMEM((N_EP, PAD, WIDE), BF16),
            jax.ShapeDtypeStruct((TOK // N_TP, MODEL), BF16),
        ),
        in_specs=[vmem],
        out_specs=(vmem, vmem),
        compiler_params=params(8),
        name="reduce_terms",
    )(in_vmem(y))


def weigh_kernel(ids_ref, weights_ref, high_ref, low_ref):
    spread = routing(ids_ref[...], weights_ref[...]).T
    high = spread.astype(BF16)
    high_ref[...] = high
    low_ref[...] = (spread - high.astype(F32)).astype(BF16)


def weigh(ids, weights):
    vmem = pl.BlockSpec(memory_space=pltpu.VMEM)
    return pl.pallas_call(
        weigh_kernel,
        out_shape=(pltpu.VMEM((TOK, PADDED), BF16),) * 2,
        in_specs=[vmem] * 2,
        out_specs=(vmem, vmem),
        compiler_params=params(8),
        name="weigh",
    )(ids, weights)


def combine_kernel(back_ref, high_ref, low_ref, out_ref):
    back = back_ref[...].reshape(PADDED, WIDE)
    mixed = jnp.dot(high_ref[...], back, preferred_element_type=F32)
    mixed = mixed + jnp.dot(low_ref[...], back, preferred_element_type=F32)
    out_ref[...] = mixed.astype(BF16)


def combine(back, high, low):
    vmem = pl.BlockSpec(memory_space=pltpu.VMEM)
    return pl.pallas_call(
        combine_kernel,
        out_shape=jax.ShapeDtypeStruct((TOK, WIDE), BF16),
        in_specs=[vmem] * 3,
        out_specs=vmem,
        compiler_params=params(8),
        name="combine",
    )(*(in_vmem(a) for a in (back, high, low)))


def attend_kernel(
    z_ref, core_ref, lam_ref, q_ref, a_ref, b_ref, c_ref, d_ref, gain_ref, w_ref, out_ref, score_ref
):
    q = q_ref[...]
    q = (q.astype(F32) * (64**-0.5)).astype(BF16)
    lane = lax.broadcasted_iota(jnp.int32, (TOK, WIDE), 1)
    zero = jnp.zeros_like(q)
    both = jnp.concatenate(
        [jnp.where(lane < 64, q, zero), jnp.where(lane < 64, zero, q)], axis=0
    )
    row = lax.broadcasted_iota(jnp.int32, (2 * TOK, TOK), 0)
    row = jnp.where(row < TOK, row, row - TOK)
    ahead = lax.broadcasted_iota(jnp.int32, (2 * TOK, TOK), 1) - row
    z, core = z_ref[0], core_ref[0]
    me = CORE * z + core
    chips = []
    for half, refs in ((core, (a_ref, b_ref)), (1 - core, (c_ref, d_ref))):
        for n, step in enumerate(STEPS):
            down = CORE * ((z - step) & (Z - 1))
            up = CORE * ((z + 1 + step) & (Z - 1))
            first = jnp.where(half == 0, down + 1, up)
            second = jnp.where(half == 0, down, up + 1)
            chips.append((refs[n // 4], 2 * (n % 4), (first, second)))
    top = jnp.full((2 * TOK, TOK), -1e30, F32)
    for n, (ref, low, blocks) in enumerate(chips):
        keys = ref[low : low + 2, :, :WIDE].reshape(2 * TOK, WIDE)
        scores = lax.dot_general(
            both, keys, (((1,), (1,)), ((), ())), preferred_element_type=F32
        )
        for h in range(2):
            part = scores[:, h * TOK : (h + 1) * TOK]
            part = jnp.where(ahead <= (me - blocks[h]) * TOK, part, -1e30)
            score_ref[n, :, h * TOK : (h + 1) * TOK] = part
            top = jnp.maximum(top, part)
    row_max = jnp.max(top, axis=-1, keepdims=True)
    total = jnp.zeros((2 * TOK, 2 * TOK), F32)
    value_sum = jnp.zeros((2 * TOK, WIDE), F32)
    for n, (ref, low, _) in enumerate(chips):
        terms = jnp.exp(score_ref[n] - row_max)
        total = total + terms
        values = ref[low : low + 2, :, WIDE:].reshape(2 * TOK, WIDE)
        value_sum = value_sum + jnp.dot(terms.astype(BF16), values, preferred_element_type=F32)
    ratio = value_sum / jnp.sum(total, axis=-1, keepdims=True)
    attended = ratio[:TOK] - lam_ref[0] * ratio[TOK:]
    mean_sq = jnp.mean(attended * attended, axis=-1, keepdims=True)
    head_rows = (attended * lax.rsqrt(mean_sq + NORM_EPS) * gain_ref[...]).astype(BF16)
    product = jnp.dot(head_rows, w_ref[...], preferred_element_type=F32).astype(BF16)
    for c in range(N_TP):
        piece = product[:, c * WIDE : (c + 1) * WIDE].reshape(N_TP, TOK // N_TP, WIDE)
        out_ref[:, 8 * c : 8 * (c + 1), :] = piece


def attend(z_at, core_at, lam, q, blocks, gain, w):
    vmem = pl.BlockSpec(memory_space=pltpu.VMEM)
    smem = pl.BlockSpec(memory_space=pltpu.SMEM)
    return pl.pallas_call(
        attend_kernel,
        out_shape=pltpu.VMEM((N_TP, TOK, WIDE), BF16),
        in_specs=[smem] * 3 + [vmem] * 7,
        out_specs=vmem,
        scratch_shapes=[pltpu.VMEM((Z, 2 * TOK, 2 * TOK), F32)],
        compiler_params=params(16),
        name="attend",
    )(z_at, core_at, lam, q, *blocks, gain, w)


def moved(array, source):
    pairs = []
    for z in range(Z):
        for core in range(CORE):
            sender = source(z, core)
            if sender is not None:
                pairs.append((sender[0] % Z * CORE + sender[1], z * CORE + core))
    return lax.ppermute(array, EP, pairs)


def along(array, by):
    return moved(array, lambda z, core: (z + by if core else z - by, core))


def across(array):
    return moved(array, lambda z, core: (z, 1 - core))


def exchanged(array, axes):
    return lax.all_to_all(array, axes, split_axis=0, concat_axis=0, tiled=True)


def collect_keys(keys, values, core_at):
    mine = jnp.concatenate([keys, values], axis=-1)
    first = moved(mine, lambda z, core: (z + 1, 0) if core else (z, 1))
    second = moved(mine, lambda z, core: (z + 1, 1) if core else None)
    pair = jnp.stack([first, jnp.where(core_at == 0, mine, second)])
    two = jnp.concatenate([pair, along(pair, 4)], axis=0)
    four = jnp.concatenate([two, along(two, 2)], axis=0)
    rest = along(four, 1)
    other = across(four)
    return four, rest, other, across(rest)


def body(
    query_maps,
    key_maps,
    value_rows,
    head_lambda,
    head_gain,
    out_weight,
    token_rows,
    norm_gain,
    expert_ids,
    route_weights,
    gate_weight,
    up_weight,
    down_weight,
):
    z_at = lax.axis_index("z").astype(jnp.int32)
    core_at = lax.axis_index("core").astype(jnp.int32)
    tp_at = lax.axis_index(TP).astype(jnp.int32)
    ids = expert_ids.T
    packed = dispatch(tp_at.reshape(1), token_rows, norm_gain.reshape(1, MODEL), ids)
    arrived = exchanged(packed, EP)
    blocks = collect_keys(
        key_maps.reshape(TOK, WIDE), value_rows.reshape(TOK, WIDE), core_at
    )
    proj = attend(
        z_at.reshape(1),
        core_at.reshape(1),
        head_lambda,
        query_maps.reshape(TOK, WIDE),
        blocks,
        head_gain.reshape(1, WIDE),
        out_weight,
    )
    high, low = weigh(ids, route_weights.T)
    spread = compact(arrived)
    x = exchanged(spread, TP)
    terms = ffn(x, gate_weight[0], up_weight[0], down_weight[0], proj)
    y = exchanged(terms, TP)
    back, mixed_rows = reduce_terms(y)
    returned = exchanged(back, EP)
    mixed_experts = combine(returned, high, low)
    return (mixed_rows, mixed_experts)


def solution(mesh):
    fine = Mesh(mesh.devices.reshape(Z, CORE, Y, X), ("z", "core", "y", "x"))
    placed = (
        P(EP, TP, None),
        P(EP, TP, None),
        P(EP, TP, None),
        P(TP),
        P(),
        P(TP, None),
        P(EP, None),
        P(),
        P(EP, None),
        P(EP, None),
        P(EP, None, TP),
        P(EP, None, TP),
        P(EP, TP, None),
    )
    return jax.shard_map(
        body,
        mesh=fine,
        in_specs=placed,
        out_specs=(P((*EP, *TP), None), P(EP, TP)),
        check_vma=False,
    )
```

```python
import jax
import jax.numpy as jnp
from jax import lax
from jax.experimental import pallas as pl
from jax.experimental.pallas import tpu as pltpu
from jax.sharding import Mesh, PartitionSpec as P


NORM_EPS = 1e-05
CLAMP_LIMIT = 7.0
GATE_SLOPE = 1.702
BF16 = jnp.bfloat16
F32 = jnp.float32

Z, CORE, Y, X = 16, 2, 4, 4
EP = ("z", "core")
TP = ("y", "x")
N_EP = Z * CORE
N_TP = Y * X
TOK = 128
CAP = 20
PAD = 24
ROWS = N_EP * CAP
PADDED = N_EP * PAD
WIDE = 128
MODEL = N_TP * WIDE
OWN_ROWS = TOK // N_TP

STEPS = (0, 4, 2, 6, 1, 5, 3, 7)
MIB = 1 << 20


def in_vmem(array):
    return pltpu.with_memory_space_constraint(array, pltpu.VMEM)


def params(mib):
    return pltpu.CompilerParams(vmem_limit_bytes=mib * MIB)


def routing(ids, values=None):
    expert = lax.broadcasted_iota(jnp.int32, (N_EP, TOK), 0)
    named = jnp.zeros((N_EP, TOK), F32)
    weight = jnp.zeros((N_EP, TOK), F32)
    for k in range(ids.shape[0]):
        hit = ids[k : k + 1, :] == expert
        named = named + jnp.where(hit, 1.0, 0.0)
        if values is not None:
            weight = weight + jnp.where(hit, values[k : k + 1, :], 0.0)
    earlier = lax.broadcasted_iota(jnp.int32, (TOK, TOK), 0) < lax.broadcasted_iota(
        jnp.int32, (TOK, TOK), 1
    )
    rank = jnp.dot(
        named.astype(BF16),
        jnp.where(earlier, 1.0, 0.0).astype(BF16),
        preferred_element_type=F32,
    )
    slot = jnp.where(named > 0.5, rank.astype(jnp.int32), -1)
    place = lax.broadcasted_iota(jnp.int32, (PAD, TOK), 0)
    pieces = []
    for e in range(N_EP):
        here = slot[e : e + 1, :] == place
        pieces.append(jnp.where(here, 1.0 if values is None else weight[e : e + 1, :], 0.0))
    return jnp.concatenate(pieces, axis=0)


def dispatch_kernel(at_ref, rows_ref, part_ref, gain_ref, ids_ref, out_ref):
    rows = rows_ref[...].astype(F32)
    mean_sq = jnp.mean(rows * rows, axis=-1, keepdims=True)
    part = part_ref[...].astype(F32) * lax.rsqrt(mean_sq + NORM_EPS) * gain_ref[...]
    chosen = routing(ids_ref[...]).astype(BF16)
    packed = jnp.dot(chosen, part.astype(BF16), preferred_element_type=F32)
    out_ref[...] = packed.astype(BF16).reshape(N_EP, PAD, WIDE)


def dispatch(at, token_rows, gain, ids):
    return pl.pallas_call(
        dispatch_kernel,
        out_shape=jax.ShapeDtypeStruct((N_EP, PAD, WIDE), BF16),
        grid_spec=pltpu.PrefetchScalarGridSpec(
            num_scalar_prefetch=1,
            grid=(1,),
            in_specs=[
                pl.BlockSpec((TOK, MODEL), lambda i, at: (0, 0)),
                pl.BlockSpec((TOK, WIDE), lambda i, at: (0, at[0])),
                pl.BlockSpec((1, WIDE), lambda i, at: (0, at[0])),
                pl.BlockSpec((4, TOK), lambda i, at: (0, 0)),
            ],
            out_specs=pl.BlockSpec((N_EP, PAD, WIDE), lambda i, at: (0, 0, 0)),
        ),
        compiler_params=params(8),
        name="dispatch",
    )(at, *(pltpu.with_memory_space_constraint(a, pltpu.HBM) for a in (token_rows, token_rows, gain, ids)))


COMPACT_STEPS = 4
COMPACT_SRC = N_EP // COMPACT_STEPS


def compact_kernel(in_ref, out_ref):
    to = lax.broadcasted_iota(jnp.int32, (2 * CAP, 2 * PAD), 0)
    src = lax.broadcasted_iota(jnp.int32, (2 * CAP, 2 * PAD), 1)
    pick = jnp.where(src == jnp.where(to < CAP, to, to + (PAD - CAP)), 1.0, 0.0).astype(BF16)
    for g in range(0, COMPACT_SRC, 2):
        block = in_ref[g : g + 2].reshape(2 * PAD, WIDE)
        kept = jnp.dot(pick, block, preferred_element_type=F32).astype(BF16)
        for t in range(N_TP):
            out_ref[t, CAP * g : CAP * (g + 2), :] = kept


def compact(arrived):
    return pl.pallas_call(
        compact_kernel,
        out_shape=pltpu.HBM((N_TP, ROWS, WIDE), BF16),
        grid=(COMPACT_STEPS,),
        in_specs=[pl.BlockSpec((COMPACT_SRC, PAD, WIDE), lambda i: (i, 0, 0))],
        out_specs=pl.BlockSpec((N_TP, COMPACT_SRC * CAP, WIDE), lambda i: (0, i, 0)),
        compiler_params=params(8),
        name="compact",
    )(arrived)


FFN_ROWS = ROWS // 2


def ffn_kernel(
    x_ref, wg_hbm, wu_hbm, wd_hbm, out_hbm, wg_ref, wu_ref, wd_ref, out_ref, load_sems, store_sems
):
    loads = [
        pltpu.make_async_copy(src, dst, load_sems.at[n])
        for n, (src, dst) in enumerate(((wg_hbm, wg_ref), (wu_hbm, wu_ref), (wd_hbm, wd_ref)))
    ]
    for load in loads:
        load.start()
    stores = []
    for n in range(ROWS // FFN_ROWS):
        here = slice(n * FFN_ROWS, (n + 1) * FFN_ROWS)
        rows = jnp.concatenate([x_ref[t, here, :] for t in range(N_TP)], axis=-1)
        if n == 0:
            loads[0].wait()
        gate = jnp.dot(rows, wg_ref[...], preferred_element_type=F32)
        if n == 0:
            loads[1].wait()
        up = jnp.dot(rows, wu_ref[...], preferred_element_type=F32)
        gated = jnp.minimum(gate, CLAMP_LIMIT)
        clipped = jnp.clip(up, -CLAMP_LIMIT, CLAMP_LIMIT)
        active = ((clipped + 1.0) * gated * jax.nn.sigmoid(GATE_SLOPE * gated)).astype(BF16)
        if n == 0:
            loads[2].wait()
        terms = jnp.dot(active, wd_ref[...], preferred_element_type=F32).astype(BF16)
        for t in range(N_TP):
            out_ref[n, t] = terms[:, t * WIDE : (t + 1) * WIDE]
        stores.append(
            pltpu.make_async_copy(
                out_ref.at[n], out_hbm.at[:, pl.ds(n * FFN_ROWS, FFN_ROWS), :], store_sems.at[n]
            )
        )
        stores[-1].start()
    for store in stores:
        store.wait()


def ffn(x, wg, wu, wd):
    vmem = pl.BlockSpec(memory_space=pltpu.VMEM)
    hbm = pl.BlockSpec(memory_space=pl.ANY)
    steps = ROWS // FFN_ROWS
    return pl.pallas_call(
        ffn_kernel,
        out_shape=pltpu.HBM((N_TP, ROWS, WIDE), BF16),
        in_specs=[vmem, hbm, hbm, hbm],
        out_specs=hbm,
        scratch_shapes=[
            pltpu.VMEM(wg.shape, BF16),
            pltpu.VMEM(wu.shape, BF16),
            pltpu.VMEM(wd.shape, BF16),
            pltpu.VMEM((steps, N_TP, FFN_ROWS, WIDE), BF16),
            pltpu.SemaphoreType.DMA((3,)),
            pltpu.SemaphoreType.DMA((steps,)),
        ],
        compiler_params=params(20),
        name="ffn",
    )(in_vmem(x), *(pltpu.with_memory_space_constraint(w, pltpu.HBM) for w in (wg, wu, wd)))


def summed_rows(in_ref, low, count):
    total = in_ref[0, low : low + count, :].astype(F32)
    for t in range(1, N_TP):
        total = total + in_ref[t, low : low + count, :].astype(F32)
    return total.astype(BF16)


def reduce_kernel(in_ref, pack_ref):
    to = lax.broadcasted_iota(jnp.int32, (2 * PAD, 2 * CAP), 0)
    src = lax.broadcasted_iota(jnp.int32, (2 * PAD, 2 * CAP), 1)
    hit = to == jnp.where(src < CAP, src, src + (PAD - CAP))
    place = jnp.where(hit, 1.0, 0.0).astype(BF16)
    for g in range(0, N_EP, 2):
        block = summed_rows(in_ref, CAP * g, 2 * CAP)
        spread = jnp.dot(place, block, preferred_element_type=F32).astype(BF16)
        pack_ref[g : g + 2] = spread.reshape(2, PAD, WIDE)


def reduce_terms(y):
    vmem = pl.BlockSpec(memory_space=pltpu.VMEM)
    return pl.pallas_call(
        reduce_kernel,
        out_shape=jax.ShapeDtypeStruct((N_EP, PAD, WIDE), BF16),
        in_specs=[vmem],
        out_specs=vmem,
        compiler_params=params(8),
        name="reduce_terms",
    )(in_vmem(y))


def partial_kernel(at_ref, *refs):
    inputs, outputs = refs[:Y], refs[Y:]
    total = inputs[0][...].astype(F32)
    for ref in inputs[1:]:
        total = total + ref[...].astype(F32)
    if len(outputs) == 1:
        outputs[0][...] = total.astype(BF16)
        return
    *outputs, total_ref = outputs
    total_ref[...] = total
    for step, ref in enumerate(outputs):
        to = (at_ref[0] + step) % Y
        ref[...] = total_ref[pl.ds(pl.multiple_of(to * OWN_ROWS, OWN_ROWS), OWN_ROWS), :].astype(BF16)


def partial_sum(at, terms, last):
    vmem = pl.BlockSpec(memory_space=pltpu.VMEM)
    one = jax.ShapeDtypeStruct((OWN_ROWS, MODEL), BF16)
    return pl.pallas_call(
        partial_kernel,
        out_shape=one if last else (one,) * Y,
        in_specs=[pl.BlockSpec(memory_space=pltpu.SMEM)] + [vmem] * Y,
        out_specs=vmem if last else (vmem,) * Y,
        scratch_shapes=[] if last else [pltpu.VMEM((Y * OWN_ROWS, MODEL), F32)],
        compiler_params=params(8),
        name="sum_last" if last else "sum_first",
    )(at, *terms)


def weigh_kernel(ids_ref, weights_ref, high_ref, low_ref):
    spread = routing(ids_ref[...], weights_ref[...]).T
    high = spread.astype(BF16)
    high_ref[...] = high
    low_ref[...] = (spread - high.astype(F32)).astype(BF16)


def weigh(ids, weights):
    vmem = pl.BlockSpec(memory_space=pltpu.VMEM)
    return pl.pallas_call(
        weigh_kernel,
        out_shape=(pltpu.VMEM((TOK, PADDED), BF16),) * 2,
        in_specs=[vmem] * 2,
        out_specs=(vmem, vmem),
        compiler_params=params(8),
        name="weigh",
    )(ids, weights)


def combine_kernel(back_ref, high_ref, low_ref, out_ref):
    back = back_ref[...].reshape(PADDED, WIDE)
    mixed = jnp.dot(high_ref[...], back, preferred_element_type=F32)
    mixed = mixed + jnp.dot(low_ref[...], back, preferred_element_type=F32)
    out_ref[...] = mixed.astype(BF16)


def combine(back, high, low):
    vmem = pl.BlockSpec(memory_space=pltpu.VMEM)
    return pl.pallas_call(
        combine_kernel,
        out_shape=jax.ShapeDtypeStruct((TOK, WIDE), BF16),
        in_specs=[vmem] * 3,
        out_specs=vmem,
        compiler_params=params(8),
        name="combine",
    )(*(in_vmem(a) for a in (back, high, low)))


def attend_kernel(
    z_ref,
    core_ref,
    x_ref,
    lam_ref,
    q_ref,
    a_ref,
    b_ref,
    c_ref,
    d_ref,
    gain_ref,
    w_ref,
    *out_and_scratch,
):
    *out_refs, score_ref, product_ref = out_and_scratch
    q = q_ref[...]
    q = (q.astype(F32) * (64**-0.5)).astype(BF16)
    lane = lax.broadcasted_iota(jnp.int32, (TOK, WIDE), 1)
    zero = jnp.zeros_like(q)
    both = jnp.concatenate(
        [jnp.where(lane < 64, q, zero), jnp.where(lane < 64, zero, q)], axis=0
    )
    row = lax.broadcasted_iota(jnp.int32, (2 * TOK, TOK), 0)
    row = jnp.where(row < TOK, row, row - TOK)
    ahead = lax.broadcasted_iota(jnp.int32, (2 * TOK, TOK), 1) - row
    z, core = z_ref[0], core_ref[0]
    me = CORE * z + core
    chips = []
    for half, refs in ((core, (a_ref, b_ref)), (1 - core, (c_ref, d_ref))):
        for n, step in enumerate(STEPS):
            down = CORE * ((z - step) & (Z - 1))
            up = CORE * ((z + 1 + step) & (Z - 1))
            first = jnp.where(half == 0, down + 1, up)
            second = jnp.where(half == 0, down, up + 1)
            chips.append((refs[n // 4], 2 * (n % 4), (first, second)))
    top = jnp.full((2 * TOK, TOK), -1e30, F32)
    for n, (ref, low, blocks) in enumerate(chips):
        keys = ref[low : low + 2, :, :WIDE].reshape(2 * TOK, WIDE)
        scores = lax.dot_general(
            both, keys, (((1,), (1,)), ((), ())), preferred_element_type=F32
        )
        for h in range(2):
            part = scores[:, h * TOK : (h + 1) * TOK]
            part = jnp.where(ahead <= (me - blocks[h]) * TOK, part, -1e30)
            score_ref[n, :, h * TOK : (h + 1) * TOK] = part
            top = jnp.maximum(top, part)
    row_max = jnp.max(top, axis=-1, keepdims=True)
    total = jnp.zeros((2 * TOK, 2 * TOK), F32)
    value_sum = jnp.zeros((2 * TOK, WIDE), F32)
    for n, (ref, low, _) in enumerate(chips):
        terms = jnp.exp(score_ref[n] - row_max)
        total = total + terms
        values = ref[low : low + 2, :, WIDE:].reshape(2 * TOK, WIDE)
        value_sum = value_sum + jnp.dot(terms.astype(BF16), values, preferred_element_type=F32)
    ratio = value_sum / jnp.sum(total, axis=-1, keepdims=True)
    attended = ratio[:TOK] - lam_ref[0] * ratio[TOK:]
    mean_sq = jnp.mean(attended * attended, axis=-1, keepdims=True)
    head_rows = (attended * lax.rsqrt(mean_sq + NORM_EPS) * gain_ref[...]).astype(BF16)
    product_ref[...] = jnp.dot(head_rows, w_ref[...], preferred_element_type=F32)
    for step, out_ref in enumerate(out_refs):
        to = (x_ref[0] + step) % X
        for y in range(Y):
            low = pl.multiple_of((y * X + to) * OWN_ROWS, OWN_ROWS)
            piece = product_ref[pl.ds(low, OWN_ROWS), :]
            out_ref[y * OWN_ROWS : (y + 1) * OWN_ROWS, :] = piece.astype(BF16)


def attend(z_at, core_at, x_at, lam, q, blocks, gain, w):
    vmem = pl.BlockSpec(memory_space=pltpu.VMEM)
    smem = pl.BlockSpec(memory_space=pltpu.SMEM)
    return pl.pallas_call(
        attend_kernel,
        out_shape=(jax.ShapeDtypeStruct((Y * OWN_ROWS, MODEL), BF16),) * X,
        in_specs=[smem] * 4 + [vmem] * 7,
        out_specs=(vmem,) * X,
        scratch_shapes=[
            pltpu.VMEM((Z, 2 * TOK, 2 * TOK), F32),
            pltpu.VMEM((TOK, MODEL), F32),
        ],
        compiler_params=params(16),
        name="attend",
    )(z_at, core_at, x_at, lam, q, *blocks, gain, w)


def moved(array, source):
    pairs = []
    for z in range(Z):
        for core in range(CORE):
            sender = source(z, core)
            if sender is not None:
                pairs.append((sender[0] % Z * CORE + sender[1], z * CORE + core))
    return lax.ppermute(array, EP, pairs)


def along(array, by):
    return moved(array, lambda z, core: (z + by if core else z - by, core))


def across(array):
    return moved(array, lambda z, core: (z, 1 - core))


def gathered(pieces, axis):
    length = lax.axis_size(axis)
    arrived = [pieces[0]]
    for step in range(1, length):
        pairs = [(i, (i + step) % length) for i in range(length)]
        arrived.append(lax.ppermute(pieces[step], axis, pairs))
    return arrived


def exchanged(array, axes):
    return lax.all_to_all(array, axes, split_axis=0, concat_axis=0, tiled=True)


def collect_keys(keys, values, core_at):
    mine = jnp.concatenate([keys, values], axis=-1)
    first = moved(mine, lambda z, core: (z + 1, 0) if core else (z, 1))
    second = moved(mine, lambda z, core: (z + 1, 1) if core else None)
    pair = jnp.stack([first, jnp.where(core_at == 0, mine, second)])
    two = jnp.concatenate([pair, along(pair, 4)], axis=0)
    four = jnp.concatenate([two, along(two, 2)], axis=0)
    rest = along(four, 1)
    other = across(four)
    return four, rest, other, across(rest)


def body(
    query_maps,
    key_maps,
    value_rows,
    head_lambda,
    head_gain,
    out_weight,
    token_rows,
    norm_gain,
    expert_ids,
    route_weights,
    gate_weight,
    up_weight,
    down_weight,
):
    z_at = lax.axis_index("z").astype(jnp.int32)
    core_at = lax.axis_index("core").astype(jnp.int32)
    tp_at = lax.axis_index(TP).astype(jnp.int32)
    y_at = lax.axis_index("y").astype(jnp.int32).reshape(1)
    x_at = lax.axis_index("x").astype(jnp.int32).reshape(1)
    ids = expert_ids.T
    packed = dispatch(tp_at.reshape(1), token_rows, norm_gain.reshape(1, MODEL), ids)
    arrived = exchanged(packed, EP)
    blocks = collect_keys(
        key_maps.reshape(TOK, WIDE), value_rows.reshape(TOK, WIDE), core_at
    )
    pieces = attend(
        z_at.reshape(1),
        core_at.reshape(1),
        x_at,
        head_lambda,
        query_maps.reshape(TOK, WIDE),
        blocks,
        head_gain.reshape(1, WIDE),
        out_weight,
    )
    pieces = partial_sum(y_at, gathered(pieces, "x"), last=False)
    mixed_rows = partial_sum(y_at, gathered(pieces, "y"), last=True)
    high, low = weigh(ids, route_weights.T)
    spread = compact(arrived)
    x = exchanged(spread, TP)
    terms = ffn(x, gate_weight[0], up_weight[0], down_weight[0])
    y = exchanged(terms, TP)
    back = reduce_terms(y)
    returned = exchanged(back, EP)
    mixed_experts = combine(returned, high, low)
    return (mixed_rows, mixed_experts)


def solution(mesh):
    fine = Mesh(mesh.devices.reshape(Z, CORE, Y, X), ("z", "core", "y", "x"))
    placed = (
        P(EP, TP, None),
        P(EP, TP, None),
        P(EP, TP, None),
        P(TP),
        P(),
        P(TP, None),
        P(EP, None),
        P(),
        P(EP, None),
        P(EP, None),
        P(EP, None, TP),
        P(EP, None, TP),
        P(EP, TP, None),
    )
    return jax.shard_map(
        body,
        mesh=fine,
        in_specs=placed,
        out_specs=(P((*EP, *TP), None), P(EP, TP)),
        check_vma=False,
    )
```

```python
import jax
import jax.numpy as jnp
from jax import lax
from jax.experimental import pallas as pl
from jax.experimental.pallas import tpu as pltpu
from jax.sharding import Mesh, PartitionSpec as P


NORM_EPS = 1e-05
CLAMP_LIMIT = 7.0
GATE_SLOPE = 1.702
BF16 = jnp.bfloat16
F32 = jnp.float32

Z, CORE, Y, X = 16, 2, 4, 4
EP = ("z", "core")
TP = ("y", "x")
N_EP = Z * CORE
N_TP = Y * X
TOK = 128
CAP = 20
PAD = 24
ROWS = N_EP * CAP
PADDED = N_EP * PAD
WIDE = 128
MODEL = N_TP * WIDE
OUT_ROWS = ROWS + TOK

STEPS = (0, 4, 2, 6, 1, 5, 3, 7)
MIB = 1 << 20


def in_vmem(array):
    return pltpu.with_memory_space_constraint(array, pltpu.VMEM)


def in_hbm(array):
    return pltpu.with_memory_space_constraint(array, pltpu.HBM)


def params(mib):
    return pltpu.CompilerParams(vmem_limit_bytes=mib * MIB)


def routing(ids, values=None):
    expert = lax.broadcasted_iota(jnp.int32, (N_EP, TOK), 0)
    named = jnp.zeros((N_EP, TOK), F32)
    weight = jnp.zeros((N_EP, TOK), F32)
    for k in range(ids.shape[0]):
        hit = ids[k : k + 1, :] == expert
        named = named + jnp.where(hit, 1.0, 0.0)
        if values is not None:
            weight = weight + jnp.where(hit, values[k : k + 1, :], 0.0)
    earlier = lax.broadcasted_iota(jnp.int32, (TOK, TOK), 0) < lax.broadcasted_iota(
        jnp.int32, (TOK, TOK), 1
    )
    rank = jnp.dot(
        named.astype(BF16),
        jnp.where(earlier, 1.0, 0.0).astype(BF16),
        preferred_element_type=F32,
    )
    slot = jnp.where(named > 0.5, rank.astype(jnp.int32), -1)
    place = lax.broadcasted_iota(jnp.int32, (PAD, TOK), 0)
    pieces = []
    for e in range(N_EP):
        here = slot[e : e + 1, :] == place
        pieces.append(jnp.where(here, 1.0 if values is None else weight[e : e + 1, :], 0.0))
    return jnp.concatenate(pieces, axis=0)


def dispatch_kernel(at_ref, rows_ref, part_ref, gain_ref, ids_ref, out_ref):
    rows = rows_ref[...].astype(F32)
    mean_sq = jnp.mean(rows * rows, axis=-1, keepdims=True)
    part = part_ref[...].astype(F32) * lax.rsqrt(mean_sq + NORM_EPS) * gain_ref[...]
    chosen = routing(ids_ref[...]).astype(BF16)
    packed = jnp.dot(chosen, part.astype(BF16), preferred_element_type=F32)
    out_ref[...] = packed.astype(BF16).reshape(N_EP, PAD, WIDE)


def dispatch(at, token_rows, gain, ids):
    return pl.pallas_call(
        dispatch_kernel,
        out_shape=jax.ShapeDtypeStruct((N_EP, PAD, WIDE), BF16),
        grid_spec=pltpu.PrefetchScalarGridSpec(
            num_scalar_prefetch=1,
            grid=(1,),
            in_specs=[
                pl.BlockSpec((TOK, MODEL), lambda i, at: (0, 0)),
                pl.BlockSpec((TOK, WIDE), lambda i, at: (0, at[0])),
                pl.BlockSpec((1, WIDE), lambda i, at: (0, at[0])),
                pl.BlockSpec((4, TOK), lambda i, at: (0, 0)),
            ],
            out_specs=pl.BlockSpec((N_EP, PAD, WIDE), lambda i, at: (0, 0, 0)),
        ),
        compiler_params=params(8),
        name="dispatch",
    )(at, *(in_hbm(a) for a in (token_rows, token_rows, gain, ids)))


COMPACT_STEPS = 4
COMPACT_SRC = N_EP // COMPACT_STEPS


def compact_kernel(in_ref, out_ref):
    to = lax.broadcasted_iota(jnp.int32, (2 * CAP, 2 * PAD), 0)
    src = lax.broadcasted_iota(jnp.int32, (2 * CAP, 2 * PAD), 1)
    pick = jnp.where(src == jnp.where(to < CAP, to, to + (PAD - CAP)), 1.0, 0.0).astype(BF16)
    for g in range(0, COMPACT_SRC, 2):
        block = in_ref[g : g + 2].reshape(2 * PAD, WIDE)
        kept = jnp.dot(pick, block, preferred_element_type=F32).astype(BF16)
        for t in range(N_TP):
            out_ref[t, CAP * g : CAP * (g + 2), :] = kept


def compact(arrived):
    return pl.pallas_call(
        compact_kernel,
        out_shape=pltpu.HBM((N_TP, ROWS, WIDE), BF16),
        grid=(COMPACT_STEPS,),
        in_specs=[pl.BlockSpec((COMPACT_SRC, PAD, WIDE), lambda i: (i, 0, 0))],
        out_specs=pl.BlockSpec((N_TP, COMPACT_SRC * CAP, WIDE), lambda i: (0, i, 0)),
        compiler_params=params(8),
        name="compact",
    )(arrived)


FFN_ROWS = ROWS // 2


def ffn_kernel(x_ref, wg_hbm, wu_hbm, wd_hbm, proj_ref, out_ref, wg_ref, wu_ref, wd_ref, sems):
    loads = [
        pltpu.make_async_copy(src, dst, sems.at[n])
        for n, (src, dst) in enumerate(((wg_hbm, wg_ref), (wu_hbm, wu_ref), (wd_hbm, wd_ref)))
    ]
    for load in loads:
        load.start()
    out_ref[:, ROWS:, :] = proj_ref[...]
    for low in range(0, ROWS, FFN_ROWS):
        here = slice(low, low + FFN_ROWS)
        rows = jnp.concatenate([x_ref[t, here, :] for t in range(N_TP)], axis=-1)
        if low == 0:
            loads[0].wait()
        gate = jnp.dot(rows, wg_ref[...], preferred_element_type=F32)
        if low == 0:
            loads[1].wait()
        up = jnp.dot(rows, wu_ref[...], preferred_element_type=F32)
        gated = jnp.minimum(gate, CLAMP_LIMIT)
        clipped = jnp.clip(up, -CLAMP_LIMIT, CLAMP_LIMIT)
        active = ((clipped + 1.0) * gated * jax.nn.sigmoid(GATE_SLOPE * gated)).astype(BF16)
        if low == 0:
            loads[2].wait()
        terms = jnp.dot(active, wd_ref[...], preferred_element_type=F32).astype(BF16)
        for t in range(N_TP):
            out_ref[t, here, :] = terms[:, t * WIDE : (t + 1) * WIDE]


def ffn(x, wg, wu, wd, proj):
    vmem = pl.BlockSpec(memory_space=pltpu.VMEM)
    hbm = pl.BlockSpec(memory_space=pl.ANY)
    return pl.pallas_call(
        ffn_kernel,
        out_shape=pltpu.VMEM((N_TP, OUT_ROWS, WIDE), BF16),
        in_specs=[vmem, hbm, hbm, hbm, vmem],
        out_specs=vmem,
        scratch_shapes=[
            pltpu.VMEM(wg.shape, BF16),
            pltpu.VMEM(wu.shape, BF16),
            pltpu.VMEM(wd.shape, BF16),
            pltpu.SemaphoreType.DMA((3,)),
        ],
        compiler_params=params(16),
        name="ffn",
    )(
        in_vmem(x),
        *(in_hbm(w) for w in (wg, wu, wd)),
        in_vmem(proj),
    )


def summed_rows(in_ref, low, count):
    total = in_ref[0, low : low + count, :].astype(F32)
    for t in range(1, N_TP):
        total = total + in_ref[t, low : low + count, :].astype(F32)
    return total.astype(BF16)


def reduce_kernel(in_ref, pack_ref, mixed_ref):
    to = lax.broadcasted_iota(jnp.int32, (2 * PAD, 2 * CAP), 0)
    src = lax.broadcasted_iota(jnp.int32, (2 * PAD, 2 * CAP), 1)
    hit = to == jnp.where(src < CAP, src, src + (PAD - CAP))
    place = jnp.where(hit, 1.0, 0.0).astype(BF16)
    for g in range(0, N_EP, 2):
        block = summed_rows(in_ref, CAP * g, 2 * CAP)
        spread = jnp.dot(place, block, preferred_element_type=F32).astype(BF16)
        pack_ref[g : g + 2] = spread.reshape(2, PAD, WIDE)
    for c in range(N_TP):
        mixed_ref[:, c * WIDE : (c + 1) * WIDE] = summed_rows(in_ref, ROWS + 8 * c, 8)


def reduce_terms(y):
    vmem = pl.BlockSpec(memory_space=pltpu.VMEM)
    return pl.pallas_call(
        reduce_kernel,
        out_shape=(
            pltpu.VMEM((N_EP, PAD, WIDE), BF16),
            jax.ShapeDtypeStruct((TOK // N_TP, MODEL), BF16),
        ),
        in_specs=[vmem],
        out_specs=(vmem, vmem),
        compiler_params=params(8),
        name="reduce_terms",
    )(in_vmem(y))


def weigh_kernel(ids_ref, weights_ref, high_ref, low_ref):
    spread = routing(ids_ref[...], weights_ref[...]).T
    high = spread.astype(BF16)
    high_ref[...] = high
    low_ref[...] = (spread - high.astype(F32)).astype(BF16)


def weigh(ids, weights):
    vmem = pl.BlockSpec(memory_space=pltpu.VMEM)
    return pl.pallas_call(
        weigh_kernel,
        out_shape=(pltpu.VMEM((TOK, PADDED), BF16),) * 2,
        in_specs=[vmem] * 2,
        out_specs=(vmem, vmem),
        compiler_params=params(8),
        name="weigh",
    )(ids, weights)


def combine_kernel(back_ref, high_ref, low_ref, out_ref):
    back = back_ref[...].reshape(PADDED, WIDE)
    mixed = jnp.dot(high_ref[...], back, preferred_element_type=F32)
    mixed = mixed + jnp.dot(low_ref[...], back, preferred_element_type=F32)
    out_ref[...] = mixed.astype(BF16)


def combine(back, high, low):
    vmem = pl.BlockSpec(memory_space=pltpu.VMEM)
    return pl.pallas_call(
        combine_kernel,
        out_shape=jax.ShapeDtypeStruct((TOK, WIDE), BF16),
        in_specs=[vmem] * 3,
        out_specs=vmem,
        compiler_params=params(8),
        name="combine",
    )(*(in_vmem(a) for a in (back, high, low)))


def attend_kernel(
    z_ref, core_ref, lam_ref, q_ref, a_ref, b_ref, c_ref, d_ref, gain_ref, w_ref, out_ref, score_ref
):
    q = q_ref[...]
    q = (q.astype(F32) * (64**-0.5)).astype(BF16)
    lane = lax.broadcasted_iota(jnp.int32, (TOK, WIDE), 1)
    zero = jnp.zeros_like(q)
    both = jnp.concatenate(
        [jnp.where(lane < 64, q, zero), jnp.where(lane < 64, zero, q)], axis=0
    )
    row = lax.broadcasted_iota(jnp.int32, (2 * TOK, TOK), 0)
    row = jnp.where(row < TOK, row, row - TOK)
    ahead = lax.broadcasted_iota(jnp.int32, (2 * TOK, TOK), 1) - row
    z, core = z_ref[0], core_ref[0]
    me = CORE * z + core
    chips = []
    for half, refs in ((core, (a_ref, b_ref)), (1 - core, (c_ref, d_ref))):
        for n, step in enumerate(STEPS):
            down = CORE * ((z - step) & (Z - 1))
            up = CORE * ((z + 1 + step) & (Z - 1))
            first = jnp.where(half == 0, down + 1, up)
            second = jnp.where(half == 0, down, up + 1)
            chips.append((refs[n // 4], 2 * (n % 4), (first, second)))
    top = jnp.full((2 * TOK, TOK), -1e30, F32)
    for n, (ref, low, blocks) in enumerate(chips):
        keys = ref[low : low + 2, :, :WIDE].reshape(2 * TOK, WIDE)
        scores = lax.dot_general(
            both, keys, (((1,), (1,)), ((), ())), preferred_element_type=F32
        )
        for h in range(2):
            part = scores[:, h * TOK : (h + 1) * TOK]
            part = jnp.where(ahead <= (me - blocks[h]) * TOK, part, -1e30)
            score_ref[n, :, h * TOK : (h + 1) * TOK] = part
            top = jnp.maximum(top, part)
    row_max = jnp.max(top, axis=-1, keepdims=True)
    total = jnp.zeros((2 * TOK, 2 * TOK), F32)
    value_sum = jnp.zeros((2 * TOK, WIDE), F32)
    for n, (ref, low, _) in enumerate(chips):
        terms = jnp.exp(score_ref[n] - row_max)
        total = total + terms
        values = ref[low : low + 2, :, WIDE:].reshape(2 * TOK, WIDE)
        value_sum = value_sum + jnp.dot(terms.astype(BF16), values, preferred_element_type=F32)
    ratio = value_sum / jnp.sum(total, axis=-1, keepdims=True)
    attended = ratio[:TOK] - lam_ref[0] * ratio[TOK:]
    mean_sq = jnp.mean(attended * attended, axis=-1, keepdims=True)
    head_rows = (attended * lax.rsqrt(mean_sq + NORM_EPS) * gain_ref[...]).astype(BF16)
    product = jnp.dot(head_rows, w_ref[...], preferred_element_type=F32).astype(BF16)
    for c in range(N_TP):
        piece = product[:, c * WIDE : (c + 1) * WIDE].reshape(N_TP, TOK // N_TP, WIDE)
        out_ref[:, 8 * c : 8 * (c + 1), :] = piece


def attend(z_at, core_at, lam, q, blocks, gain, w):
    vmem = pl.BlockSpec(memory_space=pltpu.VMEM)
    smem = pl.BlockSpec(memory_space=pltpu.SMEM)
    return pl.pallas_call(
        attend_kernel,
        out_shape=pltpu.VMEM((N_TP, TOK, WIDE), BF16),
        in_specs=[smem] * 3 + [vmem] * 7,
        out_specs=vmem,
        scratch_shapes=[pltpu.VMEM((Z, 2 * TOK, 2 * TOK), F32)],
        compiler_params=params(16),
        name="attend",
    )(z_at, core_at, lam, q, *(in_hbm(b) for b in blocks), gain, in_hbm(w))


def moved(array, source):
    pairs = []
    for z in range(Z):
        for core in range(CORE):
            sender = source(z, core)
            if sender is not None:
                pairs.append((sender[0] % Z * CORE + sender[1], z * CORE + core))
    return lax.ppermute(array, EP, pairs)


def along(array, by):
    return moved(array, lambda z, core: (z + by if core else z - by, core))


def across(array):
    return moved(array, lambda z, core: (z, 1 - core))


def exchanged(array, axes):
    return lax.all_to_all(array, axes, split_axis=0, concat_axis=0, tiled=True)


def collect_keys(keys, values, core_at):
    mine = jnp.concatenate([keys, values], axis=-1)
    first = moved(mine, lambda z, core: (z + 1, 0) if core else (z, 1))
    second = moved(mine, lambda z, core: (z + 1, 1) if core else None)
    pair = jnp.stack([first, jnp.where(core_at == 0, mine, second)])
    two = jnp.concatenate([pair, along(pair, 4)], axis=0)
    four = jnp.concatenate([two, along(two, 2)], axis=0)
    rest = along(four, 1)
    other = across(four)
    return four, rest, other, across(rest)


def body(
    query_maps,
    key_maps,
    value_rows,
    head_lambda,
    head_gain,
    out_weight,
    token_rows,
    norm_gain,
    expert_ids,
    route_weights,
    gate_weight,
    up_weight,
    down_weight,
):
    z_at = lax.axis_index("z").astype(jnp.int32)
    core_at = lax.axis_index("core").astype(jnp.int32)
    tp_at = lax.axis_index(TP).astype(jnp.int32)
    ids = expert_ids.T
    packed = dispatch(tp_at.reshape(1), token_rows, norm_gain.reshape(1, MODEL), ids)
    arrived = exchanged(packed, EP)
    blocks = collect_keys(
        key_maps.reshape(TOK, WIDE), value_rows.reshape(TOK, WIDE), core_at
    )
    proj = attend(
        z_at.reshape(1),
        core_at.reshape(1),
        head_lambda,
        query_maps.reshape(TOK, WIDE),
        blocks,
        head_gain.reshape(1, WIDE),
        out_weight,
    )
    high, low = weigh(ids, route_weights.T)
    spread = compact(arrived)
    x = exchanged(spread, TP)
    terms = ffn(x, gate_weight[0], up_weight[0], down_weight[0], proj)
    y = exchanged(terms, TP)
    back, mixed_rows = reduce_terms(y)
    returned = exchanged(back, EP)
    mixed_experts = combine(returned, high, low)
    return (mixed_rows, mixed_experts)


def solution(mesh):
    fine = Mesh(mesh.devices.reshape(Z, CORE, Y, X), ("z", "core", "y", "x"))
    placed = (
        P(EP, TP, None),
        P(EP, TP, None),
        P(EP, TP, None),
        P(TP),
        P(),
        P(TP, None),
        P(EP, None),
        P(),
        P(EP, None),
        P(EP, None),
        P(EP, None, TP),
        P(EP, None, TP),
        P(EP, TP, None),
    )
    return jax.shard_map(
        body,
        mesh=fine,
        in_specs=placed,
        out_specs=(P((*EP, *TP), None), P(EP, TP)),
        check_vma=False,
    )
```

```python
import jax
import jax.numpy as jnp
from jax import lax
from jax.experimental import pallas as pl
from jax.experimental.pallas import tpu as pltpu
from jax.sharding import Mesh, PartitionSpec as P


NORM_EPS = 1e-05
CLAMP_LIMIT = 7.0
GATE_SLOPE = 1.702
BF16 = jnp.bfloat16
F32 = jnp.float32

Z, CORE, Y, X = 16, 2, 4, 4
EP = ("z", "core")
TP = ("y", "x")
N_EP = Z * CORE
N_TP = Y * X
TOK = 128
CAP = 20
PAD = 24
ROWS = N_EP * CAP
PADDED = N_EP * PAD
WIDE = 128
MODEL = N_TP * WIDE
OUT_ROWS = ROWS + TOK

STEPS = (0, 8, 4, 12, 2, 10, 6, 14, 1, 9, 5, 13, 3, 11, 7, 15)
MIB = 1 << 20


def in_vmem(array):
    return pltpu.with_memory_space_constraint(array, pltpu.VMEM)


def in_hbm(array):
    return pltpu.with_memory_space_constraint(array, pltpu.HBM)


def params(mib):
    return pltpu.CompilerParams(vmem_limit_bytes=mib * MIB)


def routing(ids, values=None):
    expert = lax.broadcasted_iota(jnp.int32, (N_EP, TOK), 0)
    named = jnp.zeros((N_EP, TOK), F32)
    weight = jnp.zeros((N_EP, TOK), F32)
    for k in range(ids.shape[0]):
        hit = ids[k : k + 1, :] == expert
        named = named + jnp.where(hit, 1.0, 0.0)
        if values is not None:
            weight = weight + jnp.where(hit, values[k : k + 1, :], 0.0)
    earlier = lax.broadcasted_iota(jnp.int32, (TOK, TOK), 0) < lax.broadcasted_iota(
        jnp.int32, (TOK, TOK), 1
    )
    rank = jnp.dot(
        named.astype(BF16),
        jnp.where(earlier, 1.0, 0.0).astype(BF16),
        preferred_element_type=F32,
    )
    slot = jnp.where(named > 0.5, rank.astype(jnp.int32), -1)
    place = lax.broadcasted_iota(jnp.int32, (PAD, TOK), 0)
    pieces = []
    for e in range(N_EP):
        here = slot[e : e + 1, :] == place
        pieces.append(jnp.where(here, 1.0 if values is None else weight[e : e + 1, :], 0.0))
    return jnp.concatenate(pieces, axis=0)


def dispatch_kernel(at_ref, rows_ref, part_ref, gain_ref, ids_ref, out_ref):
    rows = rows_ref[...].astype(F32)
    mean_sq = jnp.mean(rows * rows, axis=-1, keepdims=True)
    part = part_ref[...].astype(F32) * lax.rsqrt(mean_sq + NORM_EPS) * gain_ref[...]
    chosen = routing(ids_ref[...]).astype(BF16)
    packed = jnp.dot(chosen, part.astype(BF16), preferred_element_type=F32)
    out_ref[...] = packed.astype(BF16).reshape(N_EP, PAD, WIDE)


def dispatch(at, token_rows, gain, ids):
    return pl.pallas_call(
        dispatch_kernel,
        out_shape=jax.ShapeDtypeStruct((N_EP, PAD, WIDE), BF16),
        grid_spec=pltpu.PrefetchScalarGridSpec(
            num_scalar_prefetch=1,
            grid=(1,),
            in_specs=[
                pl.BlockSpec((TOK, MODEL), lambda i, at: (0, 0)),
                pl.BlockSpec((TOK, WIDE), lambda i, at: (0, at[0])),
                pl.BlockSpec((1, WIDE), lambda i, at: (0, at[0])),
                pl.BlockSpec((4, TOK), lambda i, at: (0, 0)),
            ],
            out_specs=pl.BlockSpec((N_EP, PAD, WIDE), lambda i, at: (0, 0, 0)),
        ),
        compiler_params=params(8),
        name="dispatch",
    )(at, *(in_hbm(a) for a in (token_rows, token_rows, gain, ids)))


COMPACT_STEPS = 2
COMPACT_SRC = N_EP // COMPACT_STEPS


def compact_kernel(in_ref, out_ref):
    to = lax.broadcasted_iota(jnp.int32, (2 * CAP, 2 * PAD), 0)
    src = lax.broadcasted_iota(jnp.int32, (2 * CAP, 2 * PAD), 1)
    pick = jnp.where(src == jnp.where(to < CAP, to, to + (PAD - CAP)), 1.0, 0.0).astype(BF16)
    for g in range(0, COMPACT_SRC, 2):
        block = in_ref[g : g + 2].reshape(2 * PAD, WIDE)
        kept = jnp.dot(pick, block, preferred_element_type=F32).astype(BF16)
        for t in range(N_TP):
            out_ref[t, CAP * g : CAP * (g + 2), :] = kept


def compact(arrived):
    return pl.pallas_call(
        compact_kernel,
        out_shape=pltpu.HBM((N_TP, ROWS, WIDE), BF16),
        grid=(COMPACT_STEPS,),
        in_specs=[pl.BlockSpec((COMPACT_SRC, PAD, WIDE), lambda i: (i, 0, 0))],
        out_specs=pl.BlockSpec((N_TP, COMPACT_SRC * CAP, WIDE), lambda i: (0, i, 0)),
        compiler_params=params(8),
        name="compact",
    )(arrived)


FFN_ROWS = ROWS // 2


def ffn_kernel(x_ref, wg_hbm, wu_hbm, wd_hbm, proj_ref, out_ref, wg_ref, wu_ref, wd_ref, sems):
    loads = [
        pltpu.make_async_copy(src, dst, sems.at[n])
        for n, (src, dst) in enumerate(((wg_hbm, wg_ref), (wu_hbm, wu_ref), (wd_hbm, wd_ref)))
    ]
    for load in loads:
        load.start()
    out_ref[:, ROWS:, :] = proj_ref[...]
    for low in range(0, ROWS, FFN_ROWS):
        here = slice(low, low + FFN_ROWS)
        rows = jnp.concatenate([x_ref[t, here, :] for t in range(N_TP)], axis=-1)
        if low == 0:
            loads[0].wait()
        gate = jnp.dot(rows, wg_ref[...], preferred_element_type=F32)
        if low == 0:
            loads[1].wait()
        up = jnp.dot(rows, wu_ref[...], preferred_element_type=F32)
        gated = jnp.minimum(gate, CLAMP_LIMIT)
        clipped = jnp.clip(up, -CLAMP_LIMIT, CLAMP_LIMIT)
        active = ((clipped + 1.0) * gated * jax.nn.sigmoid(GATE_SLOPE * gated)).astype(BF16)
        if low == 0:
            loads[2].wait()
        terms = jnp.dot(active, wd_ref[...], preferred_element_type=F32).astype(BF16)
        for t in range(N_TP):
            out_ref[t, here, :] = terms[:, t * WIDE : (t + 1) * WIDE]


def ffn(x, wg, wu, wd, proj):
    vmem = pl.BlockSpec(memory_space=pltpu.VMEM)
    hbm = pl.BlockSpec(memory_space=pl.ANY)
    return pl.pallas_call(
        ffn_kernel,
        out_shape=pltpu.VMEM((N_TP, OUT_ROWS, WIDE), BF16),
        in_specs=[vmem, hbm, hbm, hbm, vmem],
        out_specs=vmem,
        scratch_shapes=[
            pltpu.VMEM(wg.shape, BF16),
            pltpu.VMEM(wu.shape, BF16),
            pltpu.VMEM(wd.shape, BF16),
            pltpu.SemaphoreType.DMA((3,)),
        ],
        compiler_params=params(16),
        name="ffn",
    )(
        in_vmem(x),
        *(in_hbm(w) for w in (wg, wu, wd)),
        in_vmem(proj),
    )


def summed_rows(in_ref, low, count):
    total = in_ref[0, low : low + count, :].astype(F32)
    for t in range(1, N_TP):
        total = total + in_ref[t, low : low + count, :].astype(F32)
    return total.astype(BF16)


def reduce_kernel(in_ref, pack_ref, mixed_ref):
    to = lax.broadcasted_iota(jnp.int32, (2 * PAD, 2 * CAP), 0)
    src = lax.broadcasted_iota(jnp.int32, (2 * PAD, 2 * CAP), 1)
    hit = to == jnp.where(src < CAP, src, src + (PAD - CAP))
    place = jnp.where(hit, 1.0, 0.0).astype(BF16)
    for g in range(0, N_EP, 2):
        block = summed_rows(in_ref, CAP * g, 2 * CAP)
        spread = jnp.dot(place, block, preferred_element_type=F32).astype(BF16)
        pack_ref[g : g + 2] = spread.reshape(2, PAD, WIDE)
    for c in range(N_TP):
        mixed_ref[:, c * WIDE : (c + 1) * WIDE] = summed_rows(in_ref, ROWS + 8 * c, 8)


def reduce_terms(y):
    vmem = pl.BlockSpec(memory_space=pltpu.VMEM)
    return pl.pallas_call(
        reduce_kernel,
        out_shape=(
            pltpu.VMEM((N_EP, PAD, WIDE), BF16),
            jax.ShapeDtypeStruct((TOK // N_TP, MODEL), BF16),
        ),
        in_specs=[vmem],
        out_specs=(vmem, vmem),
        compiler_params=params(8),
        name="reduce_terms",
    )(in_vmem(y))


def weigh_kernel(ids_ref, weights_ref, high_ref, low_ref):
    spread = routing(ids_ref[...], weights_ref[...]).T
    high = spread.astype(BF16)
    high_ref[...] = high
    low_ref[...] = (spread - high.astype(F32)).astype(BF16)


def weigh(ids, weights):
    vmem = pl.BlockSpec(memory_space=pltpu.VMEM)
    return pl.pallas_call(
        weigh_kernel,
        out_shape=(pltpu.VMEM((TOK, PADDED), BF16),) * 2,
        in_specs=[vmem] * 2,
        out_specs=(vmem, vmem),
        compiler_params=params(8),
        name="weigh",
    )(ids, weights)


def combine_kernel(back_ref, high_ref, low_ref, out_ref):
    back = back_ref[...].reshape(PADDED, WIDE)
    mixed = jnp.dot(high_ref[...], back, preferred_element_type=F32)
    mixed = mixed + jnp.dot(low_ref[...], back, preferred_element_type=F32)
    out_ref[...] = mixed.astype(BF16)


def combine(back, high, low):
    vmem = pl.BlockSpec(memory_space=pltpu.VMEM)
    return pl.pallas_call(
        combine_kernel,
        out_shape=jax.ShapeDtypeStruct((TOK, WIDE), BF16),
        in_specs=[vmem] * 3,
        out_specs=vmem,
        compiler_params=params(8),
        name="combine",
    )(*(in_vmem(a) for a in (back, high, low)))


def attend_kernel(z_ref, core_ref, q_ref, swapped_ref, a_ref, b_ref, own_ref, other_ref, score_ref):
    lane = lax.broadcasted_iota(jnp.int32, (TOK, WIDE), 1)
    parts = []
    for ref in (q_ref, swapped_ref):
        q = (ref[...].astype(F32) * (64**-0.5)).astype(BF16)
        zero = jnp.zeros_like(q)
        parts += [jnp.where(lane < 64, q, zero), jnp.where(lane < 64, zero, q)]
    queries = jnp.concatenate(parts, axis=0)
    row = lax.broadcasted_iota(jnp.int32, (2 * TOK, TOK), 0)
    row = jnp.where(row < TOK, row, row - TOK)
    ahead = lax.broadcasted_iota(jnp.int32, (2 * TOK, TOK), 1) - row
    z, core = z_ref[0], core_ref[0]
    mine, theirs = CORE * z + core, CORE * z + 1 - core
    sign = 2 * core - 1
    blocks = [CORE * ((z + sign * step) & (Z - 1)) + core for step in STEPS]
    top = jnp.full((4 * TOK, TOK), -1e30, F32)
    for n in range(0, Z, 2):
        keys = (a_ref, b_ref)[n // 8][n % 8 : n % 8 + 2, :, :WIDE].reshape(2 * TOK, WIDE)
        scores = lax.dot_general(
            queries, keys, (((1,), (1,)), ((), ())), preferred_element_type=F32
        )
        for h in range(2):
            cols = slice(h * TOK, (h + 1) * TOK)
            part = jnp.concatenate(
                [
                    jnp.where(
                        ahead <= (who - blocks[n + h]) * TOK,
                        scores[2 * TOK * i : 2 * TOK * (i + 1), cols],
                        -1e30,
                    )
                    for i, who in enumerate((mine, theirs))
                ],
                axis=0,
            )
            score_ref[n // 2, :, cols] = part
            top = jnp.maximum(top, part)
    row_max = jnp.max(top, axis=-1, keepdims=True)
    total = jnp.zeros((4 * TOK, 2 * TOK), F32)
    value_sum = jnp.zeros((4 * TOK, WIDE), F32)
    for n in range(0, Z, 2):
        terms = jnp.exp(score_ref[n // 2] - row_max)
        total = total + terms
        values = (a_ref, b_ref)[n // 8][n % 8 : n % 8 + 2, :, WIDE:].reshape(2 * TOK, WIDE)
        value_sum = value_sum + jnp.dot(terms.astype(BF16), values, preferred_element_type=F32)
    total = jnp.sum(total, axis=-1, keepdims=True)
    wide = lax.broadcasted_iota(jnp.int32, (4 * TOK, WIDE), 1)
    beside = jnp.where(wide < 64, row_max, total)
    for i, ref in enumerate((own_ref, other_ref)):
        rows = slice(2 * TOK * i, 2 * TOK * (i + 1))
        ref[:, :WIDE] = value_sum[rows]
        ref[:, WIDE:] = beside[rows]


def attend(z_at, core_at, q, swapped, blocks):
    vmem = pl.BlockSpec(memory_space=pltpu.VMEM)
    smem = pl.BlockSpec(memory_space=pltpu.SMEM)
    part = jax.ShapeDtypeStruct((2 * TOK, 2 * WIDE), F32)
    return pl.pallas_call(
        attend_kernel,
        out_shape=(part, part),
        in_specs=[smem] * 2 + [vmem] * 4,
        out_specs=(vmem, vmem),
        scratch_shapes=[pltpu.VMEM((Z // 2, 4 * TOK, 2 * TOK), F32)],
        compiler_params=params(20),
        name="attend",
    )(z_at, core_at, q, swapped, *blocks)


def project_kernel(lam_ref, own_ref, other_ref, gain_ref, w_ref, out_ref):
    tops = [ref[:, WIDE : WIDE + 1] for ref in (own_ref, other_ref)]
    totals = [ref[:, WIDE + 64 : WIDE + 65] for ref in (own_ref, other_ref)]
    top = jnp.maximum(*tops)
    scales = [jnp.exp(t - top) for t in tops]
    total = totals[0] * scales[0] + totals[1] * scales[1]
    ratio = (own_ref[:, :WIDE] * scales[0] + other_ref[:, :WIDE] * scales[1]) / total
    attended = ratio[:TOK] - lam_ref[0] * ratio[TOK:]
    mean_sq = jnp.mean(attended * attended, axis=-1, keepdims=True)
    head_rows = (attended * lax.rsqrt(mean_sq + NORM_EPS) * gain_ref[...]).astype(BF16)
    product = jnp.dot(head_rows, w_ref[...], preferred_element_type=F32).astype(BF16)
    for c in range(N_TP):
        piece = product[:, c * WIDE : (c + 1) * WIDE].reshape(N_TP, TOK // N_TP, WIDE)
        out_ref[:, 8 * c : 8 * (c + 1), :] = piece


def project(lam, own, other, gain, w):
    vmem = pl.BlockSpec(memory_space=pltpu.VMEM)
    return pl.pallas_call(
        project_kernel,
        out_shape=pltpu.VMEM((N_TP, TOK, WIDE), BF16),
        in_specs=[pl.BlockSpec(memory_space=pltpu.SMEM)] + [vmem] * 4,
        out_specs=vmem,
        compiler_params=params(8),
        name="project",
    )(lam, own, other, gain, w)


def moved(array, source):
    pairs = []
    for z in range(Z):
        for core in range(CORE):
            sender = source(z, core)
            if sender is not None:
                pairs.append((sender[0] % Z * CORE + sender[1], z * CORE + core))
    return lax.ppermute(array, EP, pairs)


def along(array, by):
    return moved(array, lambda z, core: (z + by if core else z - by, core))


def across(array):
    return moved(array, lambda z, core: (z, 1 - core))


def exchanged(array, axes):
    return lax.all_to_all(array, axes, split_axis=0, concat_axis=0, tiled=True)


def collect_keys(keys, values):
    held = jnp.concatenate([keys, values], axis=-1)[None]
    held = jnp.concatenate([held, along(held, 8)], axis=0)
    held = jnp.concatenate([held, along(held, 4)], axis=0)
    held = jnp.concatenate([held, along(held, 2)], axis=0)
    return held, along(held, 1)


def body(
    query_maps,
    key_maps,
    value_rows,
    head_lambda,
    head_gain,
    out_weight,
    token_rows,
    norm_gain,
    expert_ids,
    route_weights,
    gate_weight,
    up_weight,
    down_weight,
):
    z_at = lax.axis_index("z").astype(jnp.int32)
    core_at = lax.axis_index("core").astype(jnp.int32)
    tp_at = lax.axis_index(TP).astype(jnp.int32)
    ids = expert_ids.T
    packed = dispatch(tp_at.reshape(1), token_rows, norm_gain.reshape(1, MODEL), ids)
    arrived = exchanged(packed, EP)
    blocks = collect_keys(key_maps.reshape(TOK, WIDE), value_rows.reshape(TOK, WIDE))
    queries = query_maps.reshape(TOK, WIDE)
    swapped = across(queries)
    own, theirs = attend(z_at.reshape(1), core_at.reshape(1), queries, swapped, blocks)
    other = across(theirs)
    proj = project(head_lambda, own, other, head_gain.reshape(1, WIDE), out_weight)
    high, low = weigh(ids, route_weights.T)
    spread = compact(arrived)
    x = exchanged(spread, TP)
    terms = ffn(x, gate_weight[0], up_weight[0], down_weight[0], proj)
    y = exchanged(terms, TP)
    back, mixed_rows = reduce_terms(y)
    returned = exchanged(back, EP)
    mixed_experts = combine(returned, high, low)
    return (mixed_rows, mixed_experts)


def solution(mesh):
    fine = Mesh(mesh.devices.reshape(Z, CORE, Y, X), ("z", "core", "y", "x"))
    placed = (
        P(EP, TP, None),
        P(EP, TP, None),
        P(EP, TP, None),
        P(TP),
        P(),
        P(TP, None),
        P(EP, None),
        P(),
        P(EP, None),
        P(EP, None),
        P(EP, None, TP),
        P(EP, None, TP),
        P(EP, TP, None),
    )
    return jax.shard_map(
        body,
        mesh=fine,
        in_specs=placed,
        out_specs=(P((*EP, *TP), None), P(EP, TP)),
        check_vma=False,
    )
```

```python
import jax
import jax.numpy as jnp
from jax import lax
from jax.experimental import pallas as pl
from jax.experimental.pallas import tpu as pltpu
from jax.sharding import Mesh, PartitionSpec as P


NORM_EPS = 1e-05
CLAMP_LIMIT = 7.0
GATE_SLOPE = 1.702
BF16 = jnp.bfloat16
F32 = jnp.float32

Z, CORE, Y, X = 16, 2, 4, 4
EP = ("z", "core")
TP = ("y", "x")
N_EP = Z * CORE
N_TP = Y * X
TOK = 128
CAP = 20
ROWS = N_EP * CAP
QUARTER = 4
WIDE = 128
MODEL = N_TP * WIDE
OUT_ROWS = ROWS + TOK

STEPS = (0, 4, 2, 6, 1, 5, 3, 7)
MIB = 1 << 20


def in_vmem(array):
    return pltpu.with_memory_space_constraint(array, pltpu.VMEM)


def in_hbm(array):
    return pltpu.with_memory_space_constraint(array, pltpu.HBM)


def params(mib):
    return pltpu.CompilerParams(vmem_limit_bytes=mib * MIB)


def routing(ids, values=None):
    expert = lax.broadcasted_iota(jnp.int32, (N_EP, TOK), 0)
    named = jnp.zeros((N_EP, TOK), F32)
    weight = jnp.zeros((N_EP, TOK), F32)
    for k in range(ids.shape[0]):
        hit = ids[k : k + 1, :] == expert
        named = named + jnp.where(hit, 1.0, 0.0)
        if values is not None:
            weight = weight + jnp.where(hit, values[k : k + 1, :], 0.0)
    earlier = lax.broadcasted_iota(jnp.int32, (TOK, TOK), 0) < lax.broadcasted_iota(
        jnp.int32, (TOK, TOK), 1
    )
    rank = jnp.dot(
        named.astype(BF16),
        jnp.where(earlier, 1.0, 0.0).astype(BF16),
        preferred_element_type=F32,
    )
    slot = jnp.where(named > 0.5, rank, -1.0)
    row = lax.broadcasted_iota(jnp.int32, (ROWS, N_EP), 0)
    first = lax.broadcasted_iota(jnp.int32, (ROWS, N_EP), 1) * CAP
    owner = jnp.where((row >= first) & (row < first + CAP), 1.0, 0.0).astype(BF16)
    parts = [slot, expert.astype(F32)]
    if values is not None:
        for _ in range(3):
            parts.append(weight.astype(BF16).astype(F32))
            weight = weight - parts[-1]
    spread = [jnp.dot(owner, p.astype(BF16), preferred_element_type=F32) for p in parts]
    place = lax.broadcasted_iota(jnp.int32, (ROWS, TOK), 0).astype(F32) - CAP * spread[1]
    value = 1.0 if values is None else spread[2] + spread[3] + spread[4]
    return jnp.where(spread[0] == place, value, 0.0)


def dispatch_kernel(at_ref, rows_ref, part_ref, gain_ref, ids_ref, out_ref):
    rows = rows_ref[...].astype(F32)
    mean_sq = jnp.mean(rows * rows, axis=-1, keepdims=True)
    part = part_ref[...].astype(F32) * lax.rsqrt(mean_sq + NORM_EPS) * gain_ref[...]
    chosen = routing(ids_ref[...]).astype(BF16)
    packed = jnp.dot(chosen, part.astype(BF16), preferred_element_type=F32)
    out_ref[...] = packed.astype(BF16)


def dispatch(at, token_rows, gain, ids):
    return pl.pallas_call(
        dispatch_kernel,
        out_shape=jax.ShapeDtypeStruct((ROWS, WIDE), BF16),
        grid_spec=pltpu.PrefetchScalarGridSpec(
            num_scalar_prefetch=1,
            grid=(1,),
            in_specs=[
                pl.BlockSpec((TOK, MODEL), lambda i, at: (0, 0)),
                pl.BlockSpec((TOK, WIDE), lambda i, at: (0, at[0])),
                pl.BlockSpec((1, WIDE), lambda i, at: (0, at[0])),
                pl.BlockSpec((4, TOK), lambda i, at: (0, 0)),
            ],
            out_specs=pl.BlockSpec((ROWS, WIDE), lambda i, at: (0, 0)),
        ),
        compiler_params=params(8),
        name="dispatch",
    )(at, *(in_hbm(a) for a in (token_rows, token_rows, gain, ids)))


FFN_ROWS = ROWS // 2


def ffn_kernel(x_ref, wg_hbm, wu_hbm, wd_hbm, proj_ref, out_ref, wg_ref, wu_ref, wd_ref, sems):
    loads = [
        pltpu.make_async_copy(src, dst, sems.at[n])
        for n, (src, dst) in enumerate(((wg_hbm, wg_ref), (wu_hbm, wu_ref), (wd_hbm, wd_ref)))
    ]
    for load in loads:
        load.start()
    out_ref[:, ROWS:, :] = proj_ref[...]
    for low in range(0, ROWS, FFN_ROWS):
        here = slice(low, low + FFN_ROWS)
        rows = jnp.concatenate([x_ref[t, here, :] for t in range(N_TP)], axis=-1)
        if low == 0:
            loads[0].wait()
        gate = jnp.dot(rows, wg_ref[...], preferred_element_type=F32)
        if low == 0:
            loads[1].wait()
        up = jnp.dot(rows, wu_ref[...], preferred_element_type=F32)
        gated = jnp.minimum(gate, CLAMP_LIMIT)
        clipped = jnp.clip(up, -CLAMP_LIMIT, CLAMP_LIMIT)
        active = ((clipped + 1.0) * gated * jax.nn.sigmoid(GATE_SLOPE * gated)).astype(BF16)
        if low == 0:
            loads[2].wait()
        terms = jnp.dot(active, wd_ref[...], preferred_element_type=F32).astype(BF16)
        for t in range(N_TP):
            out_ref[t, here, :] = terms[:, t * WIDE : (t + 1) * WIDE]


def ffn(x, wg, wu, wd, proj):
    vmem = pl.BlockSpec(memory_space=pltpu.VMEM)
    hbm = pl.BlockSpec(memory_space=pl.ANY)
    return pl.pallas_call(
        ffn_kernel,
        out_shape=pltpu.VMEM((N_TP, OUT_ROWS, WIDE), BF16),
        in_specs=[vmem, hbm, hbm, hbm, vmem],
        out_specs=vmem,
        scratch_shapes=[
            pltpu.VMEM(wg.shape, BF16),
            pltpu.VMEM(wu.shape, BF16),
            pltpu.VMEM(wd.shape, BF16),
            pltpu.SemaphoreType.DMA((3,)),
        ],
        compiler_params=params(16),
        name="ffn",
    )(
        in_vmem(x),
        *(in_hbm(w) for w in (wg, wu, wd)),
        in_vmem(proj),
    )


SUM_ROWS = 32


def summed_rows(in_ref, low, count):
    total = in_ref[0, low : low + count, :].astype(F32)
    for t in range(1, N_TP):
        total = total + in_ref[t, low : low + count, :].astype(F32)
    return total.astype(BF16)


def reduce_kernel(in_ref, pack_ref, mixed_ref):
    for low in range(0, ROWS, SUM_ROWS):
        pack_ref[low : low + SUM_ROWS, :] = summed_rows(in_ref, low, SUM_ROWS)
    for c in range(N_TP):
        mixed_ref[:, c * WIDE : (c + 1) * WIDE] = summed_rows(in_ref, ROWS + 8 * c, 8)


def reduce_terms(y):
    vmem = pl.BlockSpec(memory_space=pltpu.VMEM)
    return pl.pallas_call(
        reduce_kernel,
        out_shape=(
            jax.ShapeDtypeStruct((ROWS, WIDE), BF16),
            jax.ShapeDtypeStruct((TOK // N_TP, MODEL), BF16),
        ),
        in_specs=[vmem],
        out_specs=(vmem, vmem),
        compiler_params=params(8),
        name="reduce_terms",
    )(in_vmem(y))


def weigh_kernel(ids_ref, weights_ref, high_ref, low_ref):
    spread = routing(ids_ref[...], weights_ref[...]).T
    high = spread.astype(BF16)
    high_ref[...] = high
    low_ref[...] = (spread - high.astype(F32)).astype(BF16)


def weigh(ids, weights):
    vmem = pl.BlockSpec(memory_space=pltpu.VMEM)
    return pl.pallas_call(
        weigh_kernel,
        out_shape=(pltpu.VMEM((TOK, ROWS), BF16),) * 2,
        in_specs=[vmem] * 2,
        out_specs=(vmem, vmem),
        compiler_params=params(8),
        name="weigh",
    )(ids, weights)


def combine_kernel(back_ref, high_ref, low_ref, out_ref):
    back = back_ref[...]
    mixed = jnp.dot(high_ref[...], back, preferred_element_type=F32)
    mixed = mixed + jnp.dot(low_ref[...], back, preferred_element_type=F32)
    out_ref[...] = mixed.astype(BF16)


def combine(back, high, low):
    vmem = pl.BlockSpec(memory_space=pltpu.VMEM)
    return pl.pallas_call(
        combine_kernel,
        out_shape=jax.ShapeDtypeStruct((TOK, WIDE), BF16),
        in_specs=[vmem] * 3,
        out_specs=vmem,
        compiler_params=params(8),
        name="combine",
    )(*(in_vmem(a) for a in (back, high, low)))


def attend_kernel(z_ref, core_ref, q_ref, swapped_ref, a_ref, b_ref, own_ref, other_ref, score_ref):
    lane = lax.broadcasted_iota(jnp.int32, (TOK, WIDE), 1)
    parts = []
    for ref in (q_ref, swapped_ref):
        q = (ref[...].astype(F32) * (64**-0.5)).astype(BF16)
        zero = jnp.zeros_like(q)
        parts += [jnp.where(lane < 64, q, zero), jnp.where(lane < 64, zero, q)]
    queries = jnp.concatenate(parts, axis=0)
    row = lax.broadcasted_iota(jnp.int32, (2 * TOK, TOK), 0)
    row = jnp.where(row < TOK, row, row - TOK)
    ahead = lax.broadcasted_iota(jnp.int32, (2 * TOK, TOK), 1) - row
    z, core = z_ref[0], core_ref[0]
    mine, theirs = CORE * z + core, CORE * z + 1 - core
    blocks = []
    for step in STEPS:
        down = CORE * ((z - step) & (Z - 1))
        up = CORE * ((z + 1 + step) & (Z - 1))
        blocks += [jnp.where(core == 0, down + 1, up), jnp.where(core == 0, down, up + 1)]
    top = jnp.full((4 * TOK, TOK), -1e30, F32)
    for n in range(0, Z, 2):
        keys = (a_ref, b_ref)[n // 8][n % 8 : n % 8 + 2, :, :WIDE].reshape(2 * TOK, WIDE)
        scores = lax.dot_general(
            queries, keys, (((1,), (1,)), ((), ())), preferred_element_type=F32
        )
        for h in range(2):
            cols = slice(h * TOK, (h + 1) * TOK)
            part = jnp.concatenate(
                [
                    jnp.where(
                        ahead <= (who - blocks[n + h]) * TOK,
                        scores[2 * TOK * i : 2 * TOK * (i + 1), cols],
                        -1e30,
                    )
                    for i, who in enumerate((mine, theirs))
                ],
                axis=0,
            )
            score_ref[n // 2, :, cols] = part
            top = jnp.maximum(top, part)
    row_max = jnp.max(top, axis=-1, keepdims=True)
    total = jnp.zeros((4 * TOK, 2 * TOK), F32)
    value_sum = jnp.zeros((4 * TOK, WIDE), F32)
    for n in range(0, Z, 2):
        terms = jnp.exp(score_ref[n // 2] - row_max)
        total = total + terms
        values = (a_ref, b_ref)[n // 8][n % 8 : n % 8 + 2, :, WIDE:].reshape(2 * TOK, WIDE)
        value_sum = value_sum + jnp.dot(terms.astype(BF16), values, preferred_element_type=F32)
    total = jnp.sum(total, axis=-1, keepdims=True)
    wide = lax.broadcasted_iota(jnp.int32, (4 * TOK, WIDE), 1)
    beside = jnp.where(wide < 64, row_max, total)
    for i, ref in enumerate((own_ref, other_ref)):
        rows = slice(2 * TOK * i, 2 * TOK * (i + 1))
        ref[:, :WIDE] = value_sum[rows]
        ref[:, WIDE:] = beside[rows]


def attend(z_at, core_at, q, swapped, blocks):
    vmem = pl.BlockSpec(memory_space=pltpu.VMEM)
    smem = pl.BlockSpec(memory_space=pltpu.SMEM)
    part = jax.ShapeDtypeStruct((2 * TOK, 2 * WIDE), F32)
    return pl.pallas_call(
        attend_kernel,
        out_shape=(part, part),
        in_specs=[smem] * 2 + [vmem] * 4,
        out_specs=(vmem, vmem),
        scratch_shapes=[pltpu.VMEM((Z // 2, 4 * TOK, 2 * TOK), F32)],
        compiler_params=params(20),
        name="attend",
    )(z_at, core_at, q, swapped, *blocks)


def project_kernel(lam_ref, own_ref, other_ref, gain_ref, w_ref, out_ref):
    tops = [ref[:, WIDE : WIDE + 1] for ref in (own_ref, other_ref)]
    totals = [ref[:, WIDE + 64 : WIDE + 65] for ref in (own_ref, other_ref)]
    top = jnp.maximum(*tops)
    scales = [jnp.exp(t - top) for t in tops]
    total = totals[0] * scales[0] + totals[1] * scales[1]
    ratio = (own_ref[:, :WIDE] * scales[0] + other_ref[:, :WIDE] * scales[1]) / total
    attended = ratio[:TOK] - lam_ref[0] * ratio[TOK:]
    mean_sq = jnp.mean(attended * attended, axis=-1, keepdims=True)
    head_rows = (attended * lax.rsqrt(mean_sq + NORM_EPS) * gain_ref[...]).astype(BF16)
    product = jnp.dot(head_rows, w_ref[...], preferred_element_type=F32).astype(BF16)
    for c in range(N_TP):
        piece = product[:, c * WIDE : (c + 1) * WIDE].reshape(N_TP, TOK // N_TP, WIDE)
        out_ref[:, 8 * c : 8 * (c + 1), :] = piece


def project(lam, own, other, gain, w):
    vmem = pl.BlockSpec(memory_space=pltpu.VMEM)
    return pl.pallas_call(
        project_kernel,
        out_shape=pltpu.VMEM((N_TP, TOK, WIDE), BF16),
        in_specs=[pl.BlockSpec(memory_space=pltpu.SMEM)] + [vmem] * 4,
        out_specs=vmem,
        compiler_params=params(8),
        name="project",
    )(lam, own, other, gain, in_hbm(w))


def moved(array, source):
    pairs = []
    for z in range(Z):
        for core in range(CORE):
            sender = source(z, core)
            if sender is not None:
                pairs.append((sender[0] % Z * CORE + sender[1], z * CORE + core))
    return lax.ppermute(array, EP, pairs)


def along(array, by):
    return moved(array, lambda z, core: (z + by if core else z - by, core))


def across(array):
    return moved(array, lambda z, core: (z, 1 - core))


def exchanged(array, axes):
    return lax.all_to_all(array, axes, split_axis=0, concat_axis=0, tiled=True)


def exchanged_rows(rows):
    return exchanged(rows.reshape(ROWS // QUARTER, QUARTER, WIDE), EP).reshape(ROWS, WIDE)


def collect_keys(keys, values, core_at):
    mine = jnp.concatenate([keys, values], axis=-1)
    first = moved(mine, lambda z, core: (z + 1, 0) if core else (z, 1))
    second = moved(mine, lambda z, core: (z + 1, 1) if core else None)
    held = jnp.stack([first, jnp.where(core_at == 0, mine, second)])
    held = jnp.concatenate([held, along(held, 4)], axis=0)
    held = jnp.concatenate([held, along(held, 2)], axis=0)
    return held, along(held, 1)


def body(
    query_maps,
    key_maps,
    value_rows,
    head_lambda,
    head_gain,
    out_weight,
    token_rows,
    norm_gain,
    expert_ids,
    route_weights,
    gate_weight,
    up_weight,
    down_weight,
):
    z_at = lax.axis_index("z").astype(jnp.int32)
    core_at = lax.axis_index("core").astype(jnp.int32)
    tp_at = lax.axis_index(TP).astype(jnp.int32)
    ids = expert_ids.T
    packed = dispatch(tp_at.reshape(1), token_rows, norm_gain.reshape(1, MODEL), ids)
    arrived = exchanged_rows(packed)
    blocks = collect_keys(key_maps.reshape(TOK, WIDE), value_rows.reshape(TOK, WIDE), core_at)
    queries = query_maps.reshape(TOK, WIDE)
    swapped = across(queries)
    own, theirs = attend(z_at.reshape(1), core_at.reshape(1), queries, swapped, blocks)
    other = across(theirs)
    proj = project(head_lambda, own, other, head_gain.reshape(1, WIDE), out_weight)
    high, low = weigh(ids, route_weights.T)
    spread = jnp.broadcast_to(arrived[None], (N_TP, ROWS, WIDE))
    x = exchanged(spread, TP)
    terms = ffn(x, gate_weight[0], up_weight[0], down_weight[0], proj)
    y = exchanged(terms, TP)
    back, mixed_rows = reduce_terms(y)
    returned = exchanged_rows(back)
    mixed_experts = combine(returned, high, low)
    return (mixed_rows, mixed_experts)


def solution(mesh):
    fine = Mesh(mesh.devices.reshape(Z, CORE, Y, X), ("z", "core", "y", "x"))
    placed = (
        P(EP, TP, None),
        P(EP, TP, None),
        P(EP, TP, None),
        P(TP),
        P(),
        P(TP, None),
        P(EP, None),
        P(),
        P(EP, None),
        P(EP, None),
        P(EP, None, TP),
        P(EP, None, TP),
        P(EP, TP, None),
    )
    return jax.shard_map(
        body,
        mesh=fine,
        in_specs=placed,
        out_specs=(P((*EP, *TP), None), P(EP, TP)),
        check_vma=False,
    )
```

```python
import functools

import jax
import jax.numpy as jnp
from jax import lax
from jax.experimental import pallas as pl
from jax.experimental.pallas import tpu as pltpu
from jax.sharding import Mesh, PartitionSpec as P


NORM_EPS = 1e-05
CLAMP_LIMIT = 7.0
GATE_SLOPE = 1.702
BF16 = jnp.bfloat16
F32 = jnp.float32

Z, CORE, Y, X = 16, 2, 4, 4
EP = ("z", "core")
TP = ("y", "x")
N_EP = Z * CORE
N_TP = Y * X
TOK = 128
CAP = 20
ROWS = N_EP * CAP
QUARTER = 4
WIDE = 128
MODEL = N_TP * WIDE
OUT_ROWS = ROWS + TOK

STEPS = (0, 4, 2, 6, 1, 5, 3, 7)
MIB = 1 << 20


def in_vmem(array):
    return pltpu.with_memory_space_constraint(array, pltpu.VMEM)


def in_hbm(array):
    return pltpu.with_memory_space_constraint(array, pltpu.HBM)


def params(mib):
    return pltpu.CompilerParams(vmem_limit_bytes=mib * MIB)


def routing(ids, values=None):
    expert = lax.broadcasted_iota(jnp.int32, (N_EP, TOK), 0)
    named = jnp.zeros((N_EP, TOK), F32)
    weight = jnp.zeros((N_EP, TOK), F32)
    for k in range(ids.shape[0]):
        hit = ids[k : k + 1, :] == expert
        named = named + jnp.where(hit, 1.0, 0.0)
        if values is not None:
            weight = weight + jnp.where(hit, values[k : k + 1, :], 0.0)
    earlier = lax.broadcasted_iota(jnp.int32, (TOK, TOK), 0) < lax.broadcasted_iota(
        jnp.int32, (TOK, TOK), 1
    )
    rank = jnp.dot(
        named.astype(BF16),
        jnp.where(earlier, 1.0, 0.0).astype(BF16),
        preferred_element_type=F32,
    )
    slot = jnp.where(named > 0.5, rank, -1.0)
    row = lax.broadcasted_iota(jnp.int32, (ROWS, N_EP), 0)
    first = lax.broadcasted_iota(jnp.int32, (ROWS, N_EP), 1) * CAP
    owner = jnp.where((row >= first) & (row < first + CAP), 1.0, 0.0).astype(BF16)
    parts = [slot, expert.astype(F32)]
    if values is not None:
        for _ in range(3):
            parts.append(weight.astype(BF16).astype(F32))
            weight = weight - parts[-1]
    spread = [jnp.dot(owner, p.astype(BF16), preferred_element_type=F32) for p in parts]
    place = lax.broadcasted_iota(jnp.int32, (ROWS, TOK), 0).astype(F32) - CAP * spread[1]
    value = 1.0 if values is None else spread[2] + spread[3] + spread[4]
    return jnp.where(spread[0] == place, value, 0.0)


def dispatch_kernel(at_ref, rows_ref, part_ref, gain_ref, ids_ref, out_ref):
    rows = rows_ref[...].astype(F32)
    mean_sq = jnp.mean(rows * rows, axis=-1, keepdims=True)
    part = part_ref[...].astype(F32) * lax.rsqrt(mean_sq + NORM_EPS) * gain_ref[...]
    chosen = routing(ids_ref[...]).astype(BF16)
    packed = jnp.dot(chosen, part.astype(BF16), preferred_element_type=F32)
    out_ref[...] = packed.astype(BF16)


def dispatch(at, token_rows, gain, ids):
    return pl.pallas_call(
        dispatch_kernel,
        out_shape=jax.ShapeDtypeStruct((ROWS, WIDE), BF16),
        grid_spec=pltpu.PrefetchScalarGridSpec(
            num_scalar_prefetch=1,
            grid=(1,),
            in_specs=[
                pl.BlockSpec((TOK, MODEL), lambda i, at: (0, 0)),
                pl.BlockSpec((TOK, WIDE), lambda i, at: (0, at[0])),
                pl.BlockSpec((1, WIDE), lambda i, at: (0, at[0])),
                pl.BlockSpec((4, TOK), lambda i, at: (0, 0)),
            ],
            out_specs=pl.BlockSpec((ROWS, WIDE), lambda i, at: (0, 0)),
        ),
        compiler_params=params(8),
        name="dispatch",
    )(at, *(in_hbm(a) for a in (token_rows, token_rows, gain, ids)))


def spread_kernel(in_ref, out_hbm, sems):
    copies = [
        pltpu.make_async_copy(in_ref, out_hbm.at[t], sems.at[t]) for t in range(N_TP)
    ]
    for copy in copies:
        copy.start()
    for copy in copies:
        copy.wait()


def spread_rows(rows):
    return pl.pallas_call(
        spread_kernel,
        out_shape=pltpu.HBM((N_TP, ROWS, WIDE), BF16),
        in_specs=[pl.BlockSpec(memory_space=pltpu.VMEM)],
        out_specs=pl.BlockSpec(memory_space=pl.ANY),
        scratch_shapes=[pltpu.SemaphoreType.DMA((N_TP,))],
        compiler_params=params(4),
        name="spread_rows",
    )(in_vmem(rows))


FFN_ROWS = ROWS // 2


def ffn_kernel(x_ref, wg_hbm, wu_hbm, wd_hbm, proj_ref, out_ref, wg_ref, wu_ref, wd_ref, sems):
    loads = [
        pltpu.make_async_copy(src, dst, sems.at[n])
        for n, (src, dst) in enumerate(((wg_hbm, wg_ref), (wu_hbm, wu_ref), (wd_hbm, wd_ref)))
    ]
    for load in loads:
        load.start()
    out_ref[:, ROWS:, :] = proj_ref[...]
    for low in range(0, ROWS, FFN_ROWS):
        here = slice(low, low + FFN_ROWS)
        rows = jnp.concatenate([x_ref[t, here, :] for t in range(N_TP)], axis=-1)
        if low == 0:
            loads[0].wait()
        gate = jnp.dot(rows, wg_ref[...], preferred_element_type=F32)
        if low == 0:
            loads[1].wait()
        up = jnp.dot(rows, wu_ref[...], preferred_element_type=F32)
        gated = jnp.minimum(gate, CLAMP_LIMIT)
        clipped = jnp.clip(up, -CLAMP_LIMIT, CLAMP_LIMIT)
        active = ((clipped + 1.0) * gated * jax.nn.sigmoid(GATE_SLOPE * gated)).astype(BF16)
        if low == 0:
            loads[2].wait()
        terms = jnp.dot(active, wd_ref[...], preferred_element_type=F32).astype(BF16)
        for t in range(N_TP):
            out_ref[t, here, :] = terms[:, t * WIDE : (t + 1) * WIDE]


def ffn(x, wg, wu, wd, proj):
    vmem = pl.BlockSpec(memory_space=pltpu.VMEM)
    hbm = pl.BlockSpec(memory_space=pl.ANY)
    return pl.pallas_call(
        ffn_kernel,
        out_shape=pltpu.VMEM((N_TP, OUT_ROWS, WIDE), BF16),
        in_specs=[vmem, hbm, hbm, hbm, vmem],
        out_specs=vmem,
        scratch_shapes=[
            pltpu.VMEM(wg.shape, BF16),
            pltpu.VMEM(wu.shape, BF16),
            pltpu.VMEM(wd.shape, BF16),
            pltpu.SemaphoreType.DMA((3,)),
        ],
        compiler_params=params(16),
        name="ffn",
    )(
        in_vmem(x),
        *(in_hbm(w) for w in (wg, wu, wd)),
        in_vmem(proj),
    )


SUM_ROWS = 32


def summed_rows(in_ref, low, count):
    total = in_ref[0, low : low + count, :].astype(F32)
    for t in range(1, N_TP):
        total = total + in_ref[t, low : low + count, :].astype(F32)
    return total.astype(BF16)


def reduce_kernel(in_ref, pack_ref, mixed_ref):
    for low in range(0, ROWS, SUM_ROWS):
        pack_ref[low : low + SUM_ROWS, :] = summed_rows(in_ref, low, SUM_ROWS)
    for c in range(N_TP):
        mixed_ref[:, c * WIDE : (c + 1) * WIDE] = summed_rows(in_ref, ROWS + 8 * c, 8)


def reduce_terms(y):
    vmem = pl.BlockSpec(memory_space=pltpu.VMEM)
    return pl.pallas_call(
        reduce_kernel,
        out_shape=(
            jax.ShapeDtypeStruct((ROWS, WIDE), BF16),
            jax.ShapeDtypeStruct((TOK // N_TP, MODEL), BF16),
        ),
        in_specs=[vmem],
        out_specs=(vmem, vmem),
        compiler_params=params(8),
        name="reduce_terms",
    )(in_vmem(y))


def weigh_kernel(ids_ref, weights_ref, high_ref, low_ref):
    spread = routing(ids_ref[...], weights_ref[...]).T
    high = spread.astype(BF16)
    high_ref[...] = high
    low_ref[...] = (spread - high.astype(F32)).astype(BF16)


def weigh(ids, weights):
    vmem = pl.BlockSpec(memory_space=pltpu.VMEM)
    return pl.pallas_call(
        weigh_kernel,
        out_shape=(pltpu.VMEM((TOK, ROWS), BF16),) * 2,
        in_specs=[vmem] * 2,
        out_specs=(vmem, vmem),
        compiler_params=params(8),
        name="weigh",
    )(ids, weights)


def combine_kernel(back_ref, high_ref, low_ref, out_ref):
    back = back_ref[...]
    mixed = jnp.dot(high_ref[...], back, preferred_element_type=F32)
    mixed = mixed + jnp.dot(low_ref[...], back, preferred_element_type=F32)
    out_ref[...] = mixed.astype(BF16)


def combine(back, high, low):
    vmem = pl.BlockSpec(memory_space=pltpu.VMEM)
    return pl.pallas_call(
        combine_kernel,
        out_shape=jax.ShapeDtypeStruct((TOK, WIDE), BF16),
        in_specs=[vmem] * 3,
        out_specs=vmem,
        compiler_params=params(8),
        name="combine",
    )(*(in_vmem(a) for a in (back, high, low)))


def attend_kernel(late, z_ref, core_ref, q_ref, swapped_ref, keys_ref, *refs):
    found_ref, *out_refs, score_ref = refs if late else (None, *refs)
    lane = lax.broadcasted_iota(jnp.int32, (TOK, WIDE), 1)
    parts = []
    for ref in (q_ref, swapped_ref):
        q = (ref[...].astype(F32) * (64**-0.5)).astype(BF16)
        zero = jnp.zeros_like(q)
        parts += [jnp.where(lane < 64, q, zero), jnp.where(lane < 64, zero, q)]
    queries = jnp.concatenate(parts, axis=0)
    row = lax.broadcasted_iota(jnp.int32, (2 * TOK, TOK), 0)
    row = jnp.where(row < TOK, row, row - TOK)
    ahead = lax.broadcasted_iota(jnp.int32, (2 * TOK, TOK), 1) - row
    z, core = z_ref[0], core_ref[0]
    mine, theirs = CORE * z + core, CORE * z + 1 - core
    blocks = []
    for step in STEPS[4:] if late else STEPS[:4]:
        down = CORE * ((z - step) & (Z - 1))
        up = CORE * ((z + 1 + step) & (Z - 1))
        blocks += [jnp.where(core == 0, down + 1, up), jnp.where(core == 0, down, up + 1)]
    top = jnp.full((4 * TOK, TOK), -1e30, F32)
    for n in range(0, len(blocks), 2):
        keys = keys_ref[n : n + 2, :, :WIDE].reshape(2 * TOK, WIDE)
        scores = lax.dot_general(
            queries, keys, (((1,), (1,)), ((), ())), preferred_element_type=F32
        )
        for h in range(2):
            cols = slice(h * TOK, (h + 1) * TOK)
            part = jnp.concatenate(
                [
                    jnp.where(
                        ahead <= (who - blocks[n + h]) * TOK,
                        scores[2 * TOK * i : 2 * TOK * (i + 1), cols],
                        -1e30,
                    )
                    for i, who in enumerate((mine, theirs))
                ],
                axis=0,
            )
            score_ref[n // 2, :, cols] = part
            top = jnp.maximum(top, part)
    row_max = jnp.max(top, axis=-1, keepdims=True)
    if late:
        row_max = jnp.maximum(row_max, found_ref[:, WIDE : WIDE + 1])
    total = jnp.zeros((4 * TOK, 2 * TOK), F32)
    value_sum = jnp.zeros((4 * TOK, WIDE), F32)
    for n in range(0, len(blocks), 2):
        terms = jnp.exp(score_ref[n // 2] - row_max)
        total = total + terms
        values = keys_ref[n : n + 2, :, WIDE:].reshape(2 * TOK, WIDE)
        value_sum = value_sum + jnp.dot(terms.astype(BF16), values, preferred_element_type=F32)
    total = jnp.sum(total, axis=-1, keepdims=True)
    if late:
        scale = jnp.exp(found_ref[:, WIDE : WIDE + 1] - row_max)
        total = total + found_ref[:, WIDE + 64 : WIDE + 65] * scale
        value_sum = value_sum + found_ref[:, :WIDE] * scale
    wide = lax.broadcasted_iota(jnp.int32, (4 * TOK, WIDE), 1)
    beside = jnp.where(wide < 64, row_max, total)
    count = 4 * TOK // len(out_refs)
    for i, ref in enumerate(out_refs):
        ref[:, :WIDE] = value_sum[i * count : (i + 1) * count]
        ref[:, WIDE:] = beside[i * count : (i + 1) * count]


def attend(z_at, core_at, q, swapped, keys, found=None):
    vmem = pl.BlockSpec(memory_space=pltpu.VMEM)
    smem = pl.BlockSpec(memory_space=pltpu.SMEM)
    late = found is not None
    out = ((2 * TOK, 2 * WIDE),) * 2 if late else ((4 * TOK, 2 * WIDE),)
    return pl.pallas_call(
        functools.partial(attend_kernel, late),
        out_shape=tuple(jax.ShapeDtypeStruct(shape, F32) for shape in out),
        in_specs=[smem] * 2 + [vmem] * (4 if late else 3),
        out_specs=(vmem,) * len(out),
        scratch_shapes=[pltpu.VMEM((Z // 4, 4 * TOK, 2 * TOK), F32)],
        compiler_params=params(14),
        name="attend_late" if late else "attend_early",
    )(z_at, core_at, q, swapped, keys, *(found or ()))


def project_kernel(lam_ref, own_ref, other_ref, gain_ref, w_ref, out_ref):
    tops = [ref[:, WIDE : WIDE + 1] for ref in (own_ref, other_ref)]
    totals = [ref[:, WIDE + 64 : WIDE + 65] for ref in (own_ref, other_ref)]
    top = jnp.maximum(*tops)
    scales = [jnp.exp(t - top) for t in tops]
    total = totals[0] * scales[0] + totals[1] * scales[1]
    ratio = (own_ref[:, :WIDE] * scales[0] + other_ref[:, :WIDE] * scales[1]) / total
    attended = ratio[:TOK] - lam_ref[0] * ratio[TOK:]
    mean_sq = jnp.mean(attended * attended, axis=-1, keepdims=True)
    head_rows = (attended * lax.rsqrt(mean_sq + NORM_EPS) * gain_ref[...]).astype(BF16)
    product = jnp.dot(head_rows, w_ref[...], preferred_element_type=F32).astype(BF16)
    for c in range(N_TP):
        piece = product[:, c * WIDE : (c + 1) * WIDE].reshape(N_TP, TOK // N_TP, WIDE)
        out_ref[:, 8 * c : 8 * (c + 1), :] = piece


def project(lam, own, other, gain, w):
    vmem = pl.BlockSpec(memory_space=pltpu.VMEM)
    return pl.pallas_call(
        project_kernel,
        out_shape=pltpu.VMEM((N_TP, TOK, WIDE), BF16),
        in_specs=[pl.BlockSpec(memory_space=pltpu.SMEM)] + [vmem] * 4,
        out_specs=vmem,
        compiler_params=params(8),
        name="project",
    )(lam, own, other, gain, in_hbm(w))


def moved(array, source):
    pairs = []
    for z in range(Z):
        for core in range(CORE):
            sender = source(z, core)
            if sender is not None:
                pairs.append((sender[0] % Z * CORE + sender[1], z * CORE + core))
    return lax.ppermute(array, EP, pairs)


def along(array, by):
    return moved(array, lambda z, core: (z + by if core else z - by, core))


def across(array):
    return moved(array, lambda z, core: (z, 1 - core))


def exchanged(array, axes):
    return lax.all_to_all(array, axes, split_axis=0, concat_axis=0, tiled=True)


def exchanged_rows(rows):
    return exchanged(rows.reshape(ROWS // QUARTER, QUARTER, WIDE), EP).reshape(ROWS, WIDE)


def collect_keys(keys, values, core_at):
    mine = jnp.concatenate([keys, values], axis=-1)
    first = moved(mine, lambda z, core: (z + 1, 0) if core else (z, 1))
    second = moved(mine, lambda z, core: (z + 1, 1) if core else None)
    held = jnp.stack([first, jnp.where(core_at == 0, mine, second)])
    held = jnp.concatenate([held, along(held, 4)], axis=0)
    held = jnp.concatenate([held, along(held, 2)], axis=0)
    return held, along(held, 1)


def body(
    query_maps,
    key_maps,
    value_rows,
    head_lambda,
    head_gain,
    out_weight,
    token_rows,
    norm_gain,
    expert_ids,
    route_weights,
    gate_weight,
    up_weight,
    down_weight,
):
    z_at = lax.axis_index("z").astype(jnp.int32)
    core_at = lax.axis_index("core").astype(jnp.int32)
    tp_at = lax.axis_index(TP).astype(jnp.int32)
    ids = expert_ids.T
    packed = dispatch(tp_at.reshape(1), token_rows, norm_gain.reshape(1, MODEL), ids)
    arrived = exchanged_rows(packed)
    blocks = collect_keys(key_maps.reshape(TOK, WIDE), value_rows.reshape(TOK, WIDE), core_at)
    queries = query_maps.reshape(TOK, WIDE)
    swapped = across(queries)
    at = z_at.reshape(1), core_at.reshape(1), queries, swapped
    found = attend(*at, blocks[0])
    own, theirs = attend(*at, blocks[1], found)
    other = across(theirs)
    proj = project(head_lambda, own, other, head_gain.reshape(1, WIDE), out_weight)
    high, low = weigh(ids, route_weights.T)
    spread = spread_rows(arrived)
    x = exchanged(spread, TP)
    terms = ffn(x, gate_weight[0], up_weight[0], down_weight[0], proj)
    y = exchanged(terms, TP)
    back, mixed_rows = reduce_terms(y)
    returned = exchanged_rows(back)
    mixed_experts = combine(returned, high, low)
    return (mixed_rows, mixed_experts)


def solution(mesh):
    fine = Mesh(mesh.devices.reshape(Z, CORE, Y, X), ("z", "core", "y", "x"))
    placed = (
        P(EP, TP, None),
        P(EP, TP, None),
        P(EP, TP, None),
        P(TP),
        P(),
        P(TP, None),
        P(EP, None),
        P(),
        P(EP, None),
        P(EP, None),
        P(EP, None, TP),
        P(EP, None, TP),
        P(EP, TP, None),
    )
    return jax.shard_map(
        body,
        mesh=fine,
        in_specs=placed,
        out_specs=(P((*EP, *TP), None), P(EP, TP)),
        check_vma=False,
    )
```

```python
import functools

import jax
import jax.numpy as jnp
from jax import lax
from jax.experimental import pallas as pl
from jax.experimental.pallas import tpu as pltpu
from jax.sharding import Mesh, PartitionSpec as P


NORM_EPS = 1e-05
CLAMP_LIMIT = 7.0
GATE_SLOPE = 1.702
BF16 = jnp.bfloat16
F32 = jnp.float32

Z, CORE, Y, X = 16, 2, 4, 4
EP = ("z", "core")
TP = ("y", "x")
N_EP = Z * CORE
N_TP = Y * X
TOK = 128
CAP = 20
ROWS = N_EP * CAP
QUARTER = 4
WIDE = 128
MODEL = N_TP * WIDE
OUT_ROWS = ROWS + TOK

STEPS = (0, 4, 2, 6, 1, 5, 3, 7)
MIB = 1 << 20


def in_vmem(array):
    return pltpu.with_memory_space_constraint(array, pltpu.VMEM)


def in_hbm(array):
    return pltpu.with_memory_space_constraint(array, pltpu.HBM)


def params(mib):
    return pltpu.CompilerParams(vmem_limit_bytes=mib * MIB)


def routing(ids, values=None):
    expert = lax.broadcasted_iota(jnp.int32, (N_EP, TOK), 0)
    named = jnp.zeros((N_EP, TOK), F32)
    weight = jnp.zeros((N_EP, TOK), F32)
    for k in range(ids.shape[0]):
        hit = ids[k : k + 1, :] == expert
        named = named + jnp.where(hit, 1.0, 0.0)
        if values is not None:
            weight = weight + jnp.where(hit, values[k : k + 1, :], 0.0)
    earlier = lax.broadcasted_iota(jnp.int32, (TOK, TOK), 0) < lax.broadcasted_iota(
        jnp.int32, (TOK, TOK), 1
    )
    rank = jnp.dot(
        named.astype(BF16),
        jnp.where(earlier, 1.0, 0.0).astype(BF16),
        preferred_element_type=F32,
    )
    slot = jnp.where(named > 0.5, rank, -1.0)
    row = lax.broadcasted_iota(jnp.int32, (ROWS, N_EP), 0)
    first = lax.broadcasted_iota(jnp.int32, (ROWS, N_EP), 1) * CAP
    owner = jnp.where((row >= first) & (row < first + CAP), 1.0, 0.0).astype(BF16)
    parts = [slot, expert.astype(F32)]
    if values is not None:
        for _ in range(3):
            parts.append(weight.astype(BF16).astype(F32))
            weight = weight - parts[-1]
    spread = [jnp.dot(owner, p.astype(BF16), preferred_element_type=F32) for p in parts]
    place = lax.broadcasted_iota(jnp.int32, (ROWS, TOK), 0).astype(F32) - CAP * spread[1]
    value = 1.0 if values is None else spread[2] + spread[3] + spread[4]
    return jnp.where(spread[0] == place, value, 0.0)


def dispatch_kernel(at_ref, rows_ref, part_ref, gain_ref, ids_ref, out_ref):
    rows = rows_ref[...].astype(F32)
    mean_sq = jnp.mean(rows * rows, axis=-1, keepdims=True)
    part = part_ref[...].astype(F32) * lax.rsqrt(mean_sq + NORM_EPS) * gain_ref[...]
    chosen = routing(ids_ref[...]).astype(BF16)
    packed = jnp.dot(chosen, part.astype(BF16), preferred_element_type=F32)
    out_ref[...] = packed.astype(BF16)


def dispatch(at, token_rows, gain, ids):
    return pl.pallas_call(
        dispatch_kernel,
        out_shape=jax.ShapeDtypeStruct((ROWS, WIDE), BF16),
        grid_spec=pltpu.PrefetchScalarGridSpec(
            num_scalar_prefetch=1,
            grid=(1,),
            in_specs=[
                pl.BlockSpec((TOK, MODEL), lambda i, at: (0, 0)),
                pl.BlockSpec((TOK, WIDE), lambda i, at: (0, at[0])),
                pl.BlockSpec((1, WIDE), lambda i, at: (0, at[0])),
                pl.BlockSpec((4, TOK), lambda i, at: (0, 0)),
            ],
            out_specs=pl.BlockSpec((ROWS, WIDE), lambda i, at: (0, 0)),
        ),
        compiler_params=params(8),
        name="dispatch",
    )(at, *(in_hbm(a) for a in (token_rows, token_rows, gain, ids)))


def spread_kernel(in_ref, out_hbm, sems):
    copies = [
        pltpu.make_async_copy(in_ref, out_hbm.at[t], sems.at[t]) for t in range(N_TP)
    ]
    for copy in copies:
        copy.start()
    for copy in copies:
        copy.wait()


def spread_rows(rows):
    return pl.pallas_call(
        spread_kernel,
        out_shape=pltpu.HBM((N_TP, ROWS, WIDE), BF16),
        in_specs=[pl.BlockSpec(memory_space=pltpu.VMEM)],
        out_specs=pl.BlockSpec(memory_space=pl.ANY),
        scratch_shapes=[pltpu.SemaphoreType.DMA((N_TP,))],
        compiler_params=params(4),
        name="spread_rows",
    )(in_vmem(rows))


FFN_ROWS = ROWS // 2


def ffn_kernel(x_ref, wg_hbm, wu_hbm, wd_hbm, proj_ref, out_ref, wg_ref, wu_ref, wd_ref, sems):
    loads = [
        pltpu.make_async_copy(src, dst, sems.at[n])
        for n, (src, dst) in enumerate(((wg_hbm, wg_ref), (wu_hbm, wu_ref), (wd_hbm, wd_ref)))
    ]
    for load in loads:
        load.start()
    out_ref[:, ROWS:, :] = proj_ref[...]
    for low in range(0, ROWS, FFN_ROWS):
        here = slice(low, low + FFN_ROWS)
        rows = jnp.concatenate([x_ref[t, here, :] for t in range(N_TP)], axis=-1)
        if low == 0:
            loads[0].wait()
        gate = jnp.dot(rows, wg_ref[...], preferred_element_type=F32)
        if low == 0:
            loads[1].wait()
        up = jnp.dot(rows, wu_ref[...], preferred_element_type=F32)
        gated = jnp.minimum(gate, CLAMP_LIMIT)
        clipped = jnp.clip(up, -CLAMP_LIMIT, CLAMP_LIMIT)
        active = ((clipped + 1.0) * gated * jax.nn.sigmoid(GATE_SLOPE * gated)).astype(BF16)
        if low == 0:
            loads[2].wait()
        terms = jnp.dot(active, wd_ref[...], preferred_element_type=F32).astype(BF16)
        for t in range(N_TP):
            out_ref[t, here, :] = terms[:, t * WIDE : (t + 1) * WIDE]


def ffn(x, wg, wu, wd, proj):
    vmem = pl.BlockSpec(memory_space=pltpu.VMEM)
    hbm = pl.BlockSpec(memory_space=pl.ANY)
    return pl.pallas_call(
        ffn_kernel,
        out_shape=pltpu.VMEM((N_TP, OUT_ROWS, WIDE), BF16),
        in_specs=[vmem, hbm, hbm, hbm, vmem],
        out_specs=vmem,
        scratch_shapes=[
            pltpu.VMEM(wg.shape, BF16),
            pltpu.VMEM(wu.shape, BF16),
            pltpu.VMEM(wd.shape, BF16),
            pltpu.SemaphoreType.DMA((3,)),
        ],
        compiler_params=params(16),
        name="ffn",
    )(
        in_vmem(x),
        *(in_hbm(w) for w in (wg, wu, wd)),
        in_vmem(proj),
    )


SUM_ROWS = 32


def summed_rows(in_ref, low, count):
    total = in_ref[0, low : low + count, :].astype(F32)
    for t in range(1, N_TP):
        total = total + in_ref[t, low : low + count, :].astype(F32)
    return total.astype(BF16)


def reduce_kernel(in_ref, pack_ref, mixed_ref):
    for low in range(0, ROWS, SUM_ROWS):
        pack_ref[low : low + SUM_ROWS, :] = summed_rows(in_ref, low, SUM_ROWS)
    for c in range(N_TP):
        mixed_ref[:, c * WIDE : (c + 1) * WIDE] = summed_rows(in_ref, ROWS + 8 * c, 8)


def reduce_terms(y):
    vmem = pl.BlockSpec(memory_space=pltpu.VMEM)
    return pl.pallas_call(
        reduce_kernel,
        out_shape=(
            jax.ShapeDtypeStruct((ROWS, WIDE), BF16),
            jax.ShapeDtypeStruct((TOK // N_TP, MODEL), BF16),
        ),
        in_specs=[vmem],
        out_specs=(vmem, vmem),
        compiler_params=params(8),
        name="reduce_terms",
    )(in_vmem(y))


def weigh_kernel(ids_ref, weights_ref, high_ref, low_ref):
    spread = routing(ids_ref[...], weights_ref[...]).T
    high = spread.astype(BF16)
    high_ref[...] = high
    low_ref[...] = (spread - high.astype(F32)).astype(BF16)


def weigh(ids, weights):
    vmem = pl.BlockSpec(memory_space=pltpu.VMEM)
    return pl.pallas_call(
        weigh_kernel,
        out_shape=(pltpu.VMEM((TOK, ROWS), BF16),) * 2,
        in_specs=[vmem] * 2,
        out_specs=(vmem, vmem),
        compiler_params=params(8),
        name="weigh",
    )(ids, weights)


def combine_kernel(back_ref, high_ref, low_ref, out_ref):
    back = back_ref[...]
    mixed = jnp.dot(high_ref[...], back, preferred_element_type=F32)
    mixed = mixed + jnp.dot(low_ref[...], back, preferred_element_type=F32)
    out_ref[...] = mixed.astype(BF16)


def combine(back, high, low):
    vmem = pl.BlockSpec(memory_space=pltpu.VMEM)
    return pl.pallas_call(
        combine_kernel,
        out_shape=jax.ShapeDtypeStruct((TOK, WIDE), BF16),
        in_specs=[vmem] * 3,
        out_specs=vmem,
        compiler_params=params(8),
        name="combine",
    )(*(in_vmem(a) for a in (back, high, low)))


def attend_kernel(late, z_ref, core_ref, q_ref, swapped_ref, keys_ref, *refs):
    found_ref, *out_refs, score_ref = refs if late else (None, *refs)
    lane = lax.broadcasted_iota(jnp.int32, (TOK, WIDE), 1)
    parts = []
    for ref in (q_ref, swapped_ref):
        q = (ref[...].astype(F32) * (64**-0.5)).astype(BF16)
        zero = jnp.zeros_like(q)
        parts += [jnp.where(lane < 64, q, zero), jnp.where(lane < 64, zero, q)]
    queries = jnp.concatenate(parts, axis=0)
    row = lax.broadcasted_iota(jnp.int32, (2 * TOK, TOK), 0)
    row = jnp.where(row < TOK, row, row - TOK)
    ahead = lax.broadcasted_iota(jnp.int32, (2 * TOK, TOK), 1) - row
    z, core = z_ref[0], core_ref[0]
    mine, theirs = CORE * z + core, CORE * z + 1 - core
    blocks = []
    for step in STEPS[4:] if late else STEPS[:4]:
        down = CORE * ((z - step) & (Z - 1))
        up = CORE * ((z + 1 + step) & (Z - 1))
        blocks += [jnp.where(core == 0, down + 1, up), jnp.where(core == 0, down, up + 1)]
    top = jnp.full((4 * TOK, TOK), -1e30, F32)
    for n in range(0, len(blocks), 2):
        keys = keys_ref[n : n + 2, :, :WIDE].reshape(2 * TOK, WIDE)
        scores = lax.dot_general(
            queries, keys, (((1,), (1,)), ((), ())), preferred_element_type=F32
        )
        for h in range(2):
            cols = slice(h * TOK, (h + 1) * TOK)
            part = jnp.concatenate(
                [
                    jnp.where(
                        ahead <= (who - blocks[n + h]) * TOK,
                        scores[2 * TOK * i : 2 * TOK * (i + 1), cols],
                        -1e30,
                    )
                    for i, who in enumerate((mine, theirs))
                ],
                axis=0,
            )
            score_ref[n // 2, :, cols] = part
            top = jnp.maximum(top, part)
    row_max = jnp.max(top, axis=-1, keepdims=True)
    if late:
        row_max = jnp.maximum(row_max, found_ref[:, WIDE : WIDE + 1])
    total = jnp.zeros((4 * TOK, 2 * TOK), F32)
    value_sum = jnp.zeros((4 * TOK, WIDE), F32)
    for n in range(0, len(blocks), 2):
        terms = jnp.exp(score_ref[n // 2] - row_max)
        total = total + terms
        values = keys_ref[n : n + 2, :, WIDE:].reshape(2 * TOK, WIDE)
        value_sum = value_sum + jnp.dot(terms.astype(BF16), values, preferred_element_type=F32)
    total = jnp.sum(total, axis=-1, keepdims=True)
    if late:
        scale = jnp.exp(found_ref[:, WIDE : WIDE + 1] - row_max)
        total = total + found_ref[:, WIDE + 64 : WIDE + 65] * scale
        value_sum = value_sum + found_ref[:, :WIDE] * scale
    wide = lax.broadcasted_iota(jnp.int32, (4 * TOK, WIDE), 1)
    beside = jnp.where(wide < 64, row_max, total)
    count = 4 * TOK // len(out_refs)
    for i, ref in enumerate(out_refs):
        ref[:, :WIDE] = value_sum[i * count : (i + 1) * count]
        ref[:, WIDE:] = beside[i * count : (i + 1) * count]


def attend(z_at, core_at, q, swapped, keys, found=None):
    vmem = pl.BlockSpec(memory_space=pltpu.VMEM)
    smem = pl.BlockSpec(memory_space=pltpu.SMEM)
    late = found is not None
    out = ((2 * TOK, 2 * WIDE),) * 2 if late else ((4 * TOK, 2 * WIDE),)
    return pl.pallas_call(
        functools.partial(attend_kernel, late),
        out_shape=tuple(jax.ShapeDtypeStruct(shape, F32) for shape in out),
        in_specs=[smem] * 2 + [vmem] * (4 if late else 3),
        out_specs=(vmem,) * len(out),
        scratch_shapes=[pltpu.VMEM((Z // 4, 4 * TOK, 2 * TOK), F32)],
        compiler_params=params(14),
        name="attend_late" if late else "attend_early",
    )(z_at, core_at, q, swapped, keys, *(found or ()))


def project_kernel(lam_ref, own_ref, other_ref, gain_ref, w_ref, out_ref):
    tops = [ref[:, WIDE : WIDE + 1] for ref in (own_ref, other_ref)]
    totals = [ref[:, WIDE + 64 : WIDE + 65] for ref in (own_ref, other_ref)]
    top = jnp.maximum(*tops)
    scales = [jnp.exp(t - top) for t in tops]
    total = totals[0] * scales[0] + totals[1] * scales[1]
    ratio = (own_ref[:, :WIDE] * scales[0] + other_ref[:, :WIDE] * scales[1]) / total
    attended = ratio[:TOK] - lam_ref[0] * ratio[TOK:]
    mean_sq = jnp.mean(attended * attended, axis=-1, keepdims=True)
    head_rows = (attended * lax.rsqrt(mean_sq + NORM_EPS) * gain_ref[...]).astype(BF16)
    product = jnp.dot(head_rows, w_ref[...], preferred_element_type=F32).astype(BF16)
    for c in range(N_TP):
        piece = product[:, c * WIDE : (c + 1) * WIDE].reshape(N_TP, TOK // N_TP, WIDE)
        out_ref[:, 8 * c : 8 * (c + 1), :] = piece


def project(lam, own, other, gain, w):
    vmem = pl.BlockSpec(memory_space=pltpu.VMEM)
    return pl.pallas_call(
        project_kernel,
        out_shape=pltpu.VMEM((N_TP, TOK, WIDE), BF16),
        in_specs=[pl.BlockSpec(memory_space=pltpu.SMEM)] + [vmem] * 4,
        out_specs=vmem,
        compiler_params=params(8),
        name="project",
    )(lam, own, other, gain, in_hbm(w))


def key_routes():
    devices = [(z, core) for z in range(Z) for core in range(CORE)]
    held = {(z, core): {(z + core) % Z} for z, core in devices}
    stages = []
    for by in (4, 2, 1):
        sender = {(z, c): ((z + by if c else z - by) % Z, c) for z, c in devices}
        stages.append((sender, held))
        if by > 1:
            held = {d: held[d] | held[sender[d]] for d in devices}
    need = {d: {chip for chip in held[d] if chip <= d[0]} for d in devices}
    routes = []
    for n, (sender, before) in reversed(list(enumerate(stages))):
        last = n == len(stages) - 1
        earlier = {d: need[d] & before[d] for d in devices}
        pairs = []
        for d in devices:
            used = before[sender[d]] & ({*range(d[0] + 1)} if last else need[d])
            if used:
                pairs.append((sender[d], d))
                earlier[sender[d]] = earlier[sender[d]] | used
        routes.insert(0, pairs)
        need = earlier
    first = [((z, 1), (z, 0)) for z in range(Z) if need[z, 0]]
    first += [(((z + 1) % Z, 0), (z, 1)) for z in range(Z) if need[z, 1]]
    second = [(((z + 1) % Z, 1), (z, 1)) for z in range(Z) if need[z, 1]]
    return [first, second, *routes]


def moved(array, pairs):
    flat = [(a[0] * CORE + a[1], b[0] * CORE + b[1]) for a, b in pairs]
    return lax.ppermute(array, EP, flat)


def across(array):
    return moved(array, [((z, 1 - core), (z, core)) for z in range(Z) for core in range(CORE)])


def exchanged(array, axes):
    return lax.all_to_all(array, axes, split_axis=0, concat_axis=0, tiled=True)


def exchanged_rows(rows):
    return exchanged(rows.reshape(ROWS // QUARTER, QUARTER, WIDE), EP).reshape(ROWS, WIDE)


def collect_keys(keys, values, core_at):
    routes = key_routes()
    mine = jnp.concatenate([keys, values], axis=-1)
    first = moved(mine, routes[0])
    second = moved(mine, routes[1])
    held = jnp.stack([first, jnp.where(core_at == 0, mine, second)])
    held = jnp.concatenate([held, moved(held, routes[2])], axis=0)
    held = jnp.concatenate([held, moved(held, routes[3])], axis=0)
    return held, moved(held, routes[4])


def body(
    query_maps,
    key_maps,
    value_rows,
    head_lambda,
    head_gain,
    out_weight,
    token_rows,
    norm_gain,
    expert_ids,
    route_weights,
    gate_weight,
    up_weight,
    down_weight,
):
    z_at = lax.axis_index("z").astype(jnp.int32)
    core_at = lax.axis_index("core").astype(jnp.int32)
    tp_at = lax.axis_index(TP).astype(jnp.int32)
    ids = expert_ids.T
    packed = dispatch(tp_at.reshape(1), token_rows, norm_gain.reshape(1, MODEL), ids)
    arrived = exchanged_rows(packed)
    blocks = collect_keys(key_maps.reshape(TOK, WIDE), value_rows.reshape(TOK, WIDE), core_at)
    queries = query_maps.reshape(TOK, WIDE)
    swapped = across(queries)
    at = z_at.reshape(1), core_at.reshape(1), queries, swapped
    found = attend(*at, blocks[0])
    own, theirs = attend(*at, blocks[1], found)
    other = across(theirs)
    proj = project(head_lambda, own, other, head_gain.reshape(1, WIDE), out_weight)
    high, low = weigh(ids, route_weights.T)
    spread = spread_rows(arrived)
    x = exchanged(spread, TP)
    terms = ffn(x, gate_weight[0], up_weight[0], down_weight[0], proj)
    y = exchanged(terms, TP)
    back, mixed_rows = reduce_terms(y)
    returned = exchanged_rows(back)
    mixed_experts = combine(returned, high, low)
    return (mixed_rows, mixed_experts)


def solution(mesh):
    fine = Mesh(mesh.devices.reshape(Z, CORE, Y, X), ("z", "core", "y", "x"))
    placed = (
        P(EP, TP, None),
        P(EP, TP, None),
        P(EP, TP, None),
        P(TP),
        P(),
        P(TP, None),
        P(EP, None),
        P(),
        P(EP, None),
        P(EP, None),
        P(EP, None, TP),
        P(EP, None, TP),
        P(EP, TP, None),
    )
    return jax.shard_map(
        body,
        mesh=fine,
        in_specs=placed,
        out_specs=(P((*EP, *TP), None), P(EP, TP)),
        check_vma=False,
    )
```

```python
import functools

import jax
import jax.numpy as jnp
from jax import lax
from jax.experimental import pallas as pl
from jax.experimental.pallas import tpu as pltpu
from jax.sharding import Mesh, PartitionSpec as P


NORM_EPS = 1e-05
CLAMP_LIMIT = 7.0
GATE_SLOPE = 1.702
BF16 = jnp.bfloat16
F32 = jnp.float32

Z, CORE, Y, X = 16, 2, 4, 4
EP = ("z", "core")
TP = ("y", "x")
N_EP = Z * CORE
N_TP = Y * X
TOK = 128
CAP = 20
ROWS = N_EP * CAP
QUARTER = 4
WIDE = 128
MODEL = N_TP * WIDE
OUT_ROWS = ROWS + TOK

STEPS = (0, 4, 2, 6, 1, 5, 3, 7)
MIB = 1 << 20


def in_vmem(array):
    return pltpu.with_memory_space_constraint(array, pltpu.VMEM)


def in_hbm(array):
    return pltpu.with_memory_space_constraint(array, pltpu.HBM)


def params(mib):
    return pltpu.CompilerParams(vmem_limit_bytes=mib * MIB)


def routing(ids, values=None):
    expert = lax.broadcasted_iota(jnp.int32, (N_EP, TOK), 0)
    named = jnp.zeros((N_EP, TOK), F32)
    weight = jnp.zeros((N_EP, TOK), F32)
    for k in range(ids.shape[0]):
        hit = ids[k : k + 1, :] == expert
        named = named + jnp.where(hit, 1.0, 0.0)
        if values is not None:
            weight = weight + jnp.where(hit, values[k : k + 1, :], 0.0)
    earlier = lax.broadcasted_iota(jnp.int32, (TOK, TOK), 0) < lax.broadcasted_iota(
        jnp.int32, (TOK, TOK), 1
    )
    rank = jnp.dot(
        named.astype(BF16),
        jnp.where(earlier, 1.0, 0.0).astype(BF16),
        preferred_element_type=F32,
    )
    slot = jnp.where(named > 0.5, rank, -1.0)
    row = lax.broadcasted_iota(jnp.int32, (ROWS, N_EP), 0)
    first = lax.broadcasted_iota(jnp.int32, (ROWS, N_EP), 1) * CAP
    owner = jnp.where((row >= first) & (row < first + CAP), 1.0, 0.0).astype(BF16)
    parts = [slot, expert.astype(F32)]
    if values is not None:
        for _ in range(3):
            parts.append(weight.astype(BF16).astype(F32))
            weight = weight - parts[-1]
    spread = [jnp.dot(owner, p.astype(BF16), preferred_element_type=F32) for p in parts]
    place = lax.broadcasted_iota(jnp.int32, (ROWS, TOK), 0).astype(F32) - CAP * spread[1]
    value = 1.0 if values is None else spread[2] + spread[3] + spread[4]
    return jnp.where(spread[0] == place, value, 0.0)


def dispatch_kernel(at_ref, ids_ref, rows_hbm, gain_hbm, out_ref, rows_ref, part_ref, gain_ref, sems):
    low = pl.multiple_of(at_ref[0] * WIDE, WIDE)
    copies = [
        pltpu.make_async_copy(rows_hbm, rows_ref, sems.at[0]),
        pltpu.make_async_copy(rows_hbm.at[:, pl.ds(low, WIDE)], part_ref, sems.at[1]),
        pltpu.make_async_copy(gain_hbm.at[:, pl.ds(low, WIDE)], gain_ref, sems.at[2]),
    ]
    for copy in copies:
        copy.start()
    chosen = routing(ids_ref[...]).astype(BF16)
    for copy in copies:
        copy.wait()
    rows = rows_ref[...].astype(F32)
    mean_sq = jnp.mean(rows * rows, axis=-1, keepdims=True)
    part = part_ref[...].astype(F32) * lax.rsqrt(mean_sq + NORM_EPS) * gain_ref[...]
    out_ref[...] = jnp.dot(chosen, part.astype(BF16), preferred_element_type=F32).astype(BF16)


def dispatch(at, token_rows, gain, ids):
    vmem = pl.BlockSpec(memory_space=pltpu.VMEM)
    hbm = pl.BlockSpec(memory_space=pl.ANY)
    return pl.pallas_call(
        dispatch_kernel,
        out_shape=jax.ShapeDtypeStruct((ROWS, WIDE), BF16),
        in_specs=[pl.BlockSpec(memory_space=pltpu.SMEM), vmem, hbm, hbm],
        out_specs=vmem,
        scratch_shapes=[
            pltpu.VMEM((TOK, MODEL), BF16),
            pltpu.VMEM((TOK, WIDE), BF16),
            pltpu.VMEM((1, WIDE), F32),
            pltpu.SemaphoreType.DMA((3,)),
        ],
        compiler_params=params(8),
        name="dispatch",
    )(at, *(in_hbm(a) for a in (ids, token_rows, gain)))


def spread_kernel(in_ref, out_hbm, sems):
    copies = [
        pltpu.make_async_copy(in_ref, out_hbm.at[t], sems.at[t]) for t in range(N_TP)
    ]
    for copy in copies:
        copy.start()
    for copy in copies:
        copy.wait()


def spread_rows(rows):
    return pl.pallas_call(
        spread_kernel,
        out_shape=pltpu.HBM((N_TP, ROWS, WIDE), BF16),
        in_specs=[pl.BlockSpec(memory_space=pltpu.VMEM)],
        out_specs=pl.BlockSpec(memory_space=pl.ANY),
        scratch_shapes=[pltpu.SemaphoreType.DMA((N_TP,))],
        compiler_params=params(4),
        name="spread_rows",
    )(in_vmem(rows))


def spread_kernel(in_ref, out_hbm, sems):
    copies = [
        pltpu.make_async_copy(in_ref, out_hbm.at[t], sems.at[t]) for t in range(N_TP)
    ]
    for copy in copies:
        copy.start()
    for copy in copies:
        copy.wait()


def spread_rows(rows):
    return pl.pallas_call(
        spread_kernel,
        out_shape=pltpu.HBM((N_TP, ROWS, WIDE), BF16),
        in_specs=[pl.BlockSpec(memory_space=pltpu.VMEM)],
        out_specs=pl.BlockSpec(memory_space=pl.ANY),
        scratch_shapes=[pltpu.SemaphoreType.DMA((N_TP,))],
        compiler_params=params(4),
        name="spread_rows",
    )(in_vmem(rows))


DOWN_COLS = 4 * WIDE


def ffn_kernel(x_ref, wg_hbm, wu_hbm, wd_hbm, proj_ref, out_ref, pair_ref, wd_ref, sems):
    units = wg_hbm.shape[1]
    loads = [
        pltpu.make_async_copy(wg_hbm, pair_ref.at[:, pl.ds(0, units)], sems.at[0]),
        pltpu.make_async_copy(wu_hbm, pair_ref.at[:, pl.ds(units, units)], sems.at[1]),
        pltpu.make_async_copy(wd_hbm, wd_ref, sems.at[2]),
    ]
    for load in loads:
        load.start()
    out_ref[:, ROWS:, :] = proj_ref[...]
    rows = jnp.concatenate([x_ref[t] for t in range(N_TP)], axis=-1)
    loads[0].wait()
    loads[1].wait()
    both = jnp.dot(rows, pair_ref[...], preferred_element_type=F32)
    gated = jnp.minimum(both[:, :units], CLAMP_LIMIT)
    clipped = jnp.clip(both[:, units:], -CLAMP_LIMIT, CLAMP_LIMIT)
    active = ((clipped + 1.0) * gated * jax.nn.sigmoid(GATE_SLOPE * gated)).astype(BF16)
    loads[2].wait()
    for low in range(0, MODEL, DOWN_COLS):
        terms = jnp.dot(active, wd_ref[:, low : low + DOWN_COLS], preferred_element_type=F32)
        for t in range(DOWN_COLS // WIDE):
            part = terms[:, t * WIDE : (t + 1) * WIDE].astype(BF16)
            out_ref[low // WIDE + t, :ROWS, :] = part


def ffn(x, wg, wu, wd, proj):
    vmem = pl.BlockSpec(memory_space=pltpu.VMEM)
    hbm = pl.BlockSpec(memory_space=pl.ANY)
    return pl.pallas_call(
        ffn_kernel,
        out_shape=pltpu.VMEM((N_TP, OUT_ROWS, WIDE), BF16),
        in_specs=[vmem, hbm, hbm, hbm, vmem],
        out_specs=vmem,
        scratch_shapes=[
            pltpu.VMEM((MODEL, 2 * wg.shape[1]), BF16),
            pltpu.VMEM(wd.shape, BF16),
            pltpu.SemaphoreType.DMA((3,)),
        ],
        compiler_params=params(16),
        name="ffn",
    )(in_vmem(x), *(in_hbm(w) for w in (wg, wu, wd)), in_vmem(proj))


SUM_ROWS = 32


def summed_rows(in_ref, low, count):
    total = in_ref[0, low : low + count, :].astype(F32)
    for t in range(1, N_TP):
        total = total + in_ref[t, low : low + count, :].astype(F32)
    return total.astype(BF16)


def reduce_kernel(in_ref, pack_ref, mixed_ref):
    for low in range(0, ROWS, SUM_ROWS):
        pack_ref[low : low + SUM_ROWS, :] = summed_rows(in_ref, low, SUM_ROWS)
    for c in range(N_TP):
        mixed_ref[:, c * WIDE : (c + 1) * WIDE] = summed_rows(in_ref, ROWS + 8 * c, 8)


def reduce_terms(y):
    vmem = pl.BlockSpec(memory_space=pltpu.VMEM)
    return pl.pallas_call(
        reduce_kernel,
        out_shape=(
            jax.ShapeDtypeStruct((ROWS, WIDE), BF16),
            jax.ShapeDtypeStruct((TOK // N_TP, MODEL), BF16),
        ),
        in_specs=[vmem],
        out_specs=(vmem, vmem),
        compiler_params=params(8),
        name="reduce_terms",
    )(in_vmem(y))


def weigh_kernel(ids_ref, weights_ref, high_ref, low_ref):
    spread = routing(ids_ref[...], weights_ref[...]).T
    high = spread.astype(BF16)
    high_ref[...] = high
    low_ref[...] = (spread - high.astype(F32)).astype(BF16)


def weigh(ids, weights):
    vmem = pl.BlockSpec(memory_space=pltpu.VMEM)
    return pl.pallas_call(
        weigh_kernel,
        out_shape=(pltpu.VMEM((TOK, ROWS), BF16),) * 2,
        in_specs=[vmem] * 2,
        out_specs=(vmem, vmem),
        compiler_params=params(8),
        name="weigh",
    )(ids, weights)


def combine_kernel(back_ref, high_ref, low_ref, out_ref):
    back = back_ref[...]
    mixed = jnp.dot(high_ref[...], back, preferred_element_type=F32)
    mixed = mixed + jnp.dot(low_ref[...], back, preferred_element_type=F32)
    out_ref[...] = mixed.astype(BF16)


def combine(back, high, low):
    vmem = pl.BlockSpec(memory_space=pltpu.VMEM)
    return pl.pallas_call(
        combine_kernel,
        out_shape=jax.ShapeDtypeStruct((TOK, WIDE), BF16),
        in_specs=[vmem] * 3,
        out_specs=vmem,
        compiler_params=params(8),
        name="combine",
    )(*(in_vmem(a) for a in (back, high, low)))


def attend_kernel(late, z_ref, core_ref, q_ref, swapped_ref, keys_ref, *refs):
    found_ref, *out_refs, score_ref = refs if late else (None, *refs)
    lane = lax.broadcasted_iota(jnp.int32, (TOK, WIDE), 1)
    parts = []
    for ref in (q_ref, swapped_ref):
        q = (ref[...].astype(F32) * (64**-0.5)).astype(BF16)
        zero = jnp.zeros_like(q)
        parts += [jnp.where(lane < 64, q, zero), jnp.where(lane < 64, zero, q)]
    queries = jnp.concatenate(parts, axis=0)
    row = lax.broadcasted_iota(jnp.int32, (2 * TOK, TOK), 0)
    row = jnp.where(row < TOK, row, row - TOK)
    ahead = lax.broadcasted_iota(jnp.int32, (2 * TOK, TOK), 1) - row
    z, core = z_ref[0], core_ref[0]
    mine, theirs = CORE * z + core, CORE * z + 1 - core
    blocks = []
    for step in STEPS[4:] if late else STEPS[:4]:
        down = CORE * ((z - step) & (Z - 1))
        up = CORE * ((z + 1 + step) & (Z - 1))
        blocks += [jnp.where(core == 0, down + 1, up), jnp.where(core == 0, down, up + 1)]
    top = jnp.full((4 * TOK, TOK), -1e30, F32)
    for n in range(0, len(blocks), 2):
        keys = keys_ref[n : n + 2, :, :WIDE].reshape(2 * TOK, WIDE)
        scores = lax.dot_general(
            queries, keys, (((1,), (1,)), ((), ())), preferred_element_type=F32
        )
        for h in range(2):
            cols = slice(h * TOK, (h + 1) * TOK)
            part = jnp.concatenate(
                [
                    jnp.where(
                        ahead <= (who - blocks[n + h]) * TOK,
                        scores[2 * TOK * i : 2 * TOK * (i + 1), cols],
                        -1e30,
                    )
                    for i, who in enumerate((mine, theirs))
                ],
                axis=0,
            )
            score_ref[n // 2, :, cols] = part
            top = jnp.maximum(top, part)
    row_max = jnp.max(top, axis=-1, keepdims=True)
    if late:
        row_max = jnp.maximum(row_max, found_ref[:, WIDE : WIDE + 1])
    total = jnp.zeros((4 * TOK, 2 * TOK), F32)
    value_sum = jnp.zeros((4 * TOK, WIDE), F32)
    for n in range(0, len(blocks), 2):
        terms = jnp.exp(score_ref[n // 2] - row_max)
        total = total + terms
        values = keys_ref[n : n + 2, :, WIDE:].reshape(2 * TOK, WIDE)
        value_sum = value_sum + jnp.dot(terms.astype(BF16), values, preferred_element_type=F32)
    total = jnp.sum(total, axis=-1, keepdims=True)
    if late:
        scale = jnp.exp(found_ref[:, WIDE : WIDE + 1] - row_max)
        total = total + found_ref[:, WIDE + 64 : WIDE + 65] * scale
        value_sum = value_sum + found_ref[:, :WIDE] * scale
    wide = lax.broadcasted_iota(jnp.int32, (4 * TOK, WIDE), 1)
    beside = jnp.where(wide < 64, row_max, total)
    count = 4 * TOK // len(out_refs)
    for i, ref in enumerate(out_refs):
        ref[:, :WIDE] = value_sum[i * count : (i + 1) * count]
        ref[:, WIDE:] = beside[i * count : (i + 1) * count]


def attend(z_at, core_at, q, swapped, keys, found=None):
    vmem = pl.BlockSpec(memory_space=pltpu.VMEM)
    smem = pl.BlockSpec(memory_space=pltpu.SMEM)
    late = found is not None
    out = ((2 * TOK, 2 * WIDE),) * 2 if late else ((4 * TOK, 2 * WIDE),)
    return pl.pallas_call(
        functools.partial(attend_kernel, late),
        out_shape=tuple(jax.ShapeDtypeStruct(shape, F32) for shape in out),
        in_specs=[smem] * 2 + [vmem] * (4 if late else 3),
        out_specs=(vmem,) * len(out),
        scratch_shapes=[pltpu.VMEM((Z // 4, 4 * TOK, 2 * TOK), F32)],
        compiler_params=params(14),
        name="attend_late" if late else "attend_early",
    )(z_at, core_at, q, swapped, keys, *(found or ()))


def project_kernel(lam_ref, own_ref, other_ref, gain_ref, w_ref, out_ref):
    tops = [ref[:, WIDE : WIDE + 1] for ref in (own_ref, other_ref)]
    totals = [ref[:, WIDE + 64 : WIDE + 65] for ref in (own_ref, other_ref)]
    top = jnp.maximum(*tops)
    scales = [jnp.exp(t - top) for t in tops]
    total = totals[0] * scales[0] + totals[1] * scales[1]
    ratio = (own_ref[:, :WIDE] * scales[0] + other_ref[:, :WIDE] * scales[1]) / total
    attended = ratio[:TOK] - lam_ref[0] * ratio[TOK:]
    mean_sq = jnp.mean(attended * attended, axis=-1, keepdims=True)
    head_rows = (attended * lax.rsqrt(mean_sq + NORM_EPS) * gain_ref[...]).astype(BF16)
    product = jnp.dot(head_rows, w_ref[...], preferred_element_type=F32).astype(BF16)
    for c in range(N_TP):
        piece = product[:, c * WIDE : (c + 1) * WIDE].reshape(N_TP, TOK // N_TP, WIDE)
        out_ref[:, 8 * c : 8 * (c + 1), :] = piece


def project(lam, own, other, gain, w):
    vmem = pl.BlockSpec(memory_space=pltpu.VMEM)
    return pl.pallas_call(
        project_kernel,
        out_shape=pltpu.VMEM((N_TP, TOK, WIDE), BF16),
        in_specs=[pl.BlockSpec(memory_space=pltpu.SMEM)] + [vmem] * 4,
        out_specs=vmem,
        compiler_params=params(8),
        name="project",
    )(lam, own, other, gain, in_hbm(w))


def key_routes():
    devices = [(z, core) for z in range(Z) for core in range(CORE)]
    held = {(z, core): {(z + core) % Z} for z, core in devices}
    stages = []
    for by in (4, 2, 1):
        sender = {(z, c): ((z + by if c else z - by) % Z, c) for z, c in devices}
        stages.append((sender, held))
        if by > 1:
            held = {d: held[d] | held[sender[d]] for d in devices}
    need = {d: {chip for chip in held[d] if chip <= d[0]} for d in devices}
    routes = []
    for n, (sender, before) in reversed(list(enumerate(stages))):
        last = n == len(stages) - 1
        earlier = {d: need[d] & before[d] for d in devices}
        pairs = []
        for d in devices:
            used = before[sender[d]] & ({*range(d[0] + 1)} if last else need[d])
            if used:
                pairs.append((sender[d], d))
                earlier[sender[d]] = earlier[sender[d]] | used
        routes.insert(0, pairs)
        need = earlier
    first = [((z, 1), (z, 0)) for z in range(Z) if need[z, 0]]
    first += [(((z + 1) % Z, 0), (z, 1)) for z in range(Z) if need[z, 1]]
    second = [(((z + 1) % Z, 1), (z, 1)) for z in range(Z) if need[z, 1]]
    return [first, second, *routes]


def moved(array, pairs):
    flat = [(a[0] * CORE + a[1], b[0] * CORE + b[1]) for a, b in pairs]
    return lax.ppermute(array, EP, flat)


def across(array):
    return moved(array, [((z, 1 - core), (z, core)) for z in range(Z) for core in range(CORE)])


def exchanged(array, axes):
    return lax.all_to_all(array, axes, split_axis=0, concat_axis=0, tiled=True)


def exchanged_rows(rows):
    return exchanged(rows.reshape(ROWS // QUARTER, QUARTER, WIDE), EP).reshape(ROWS, WIDE)


def collect_keys(keys, values, core_at):
    routes = key_routes()
    mine = jnp.concatenate([keys, values], axis=-1)
    first = moved(mine, routes[0])
    second = moved(mine, routes[1])
    held = jnp.stack([first, jnp.where(core_at == 0, mine, second)])
    held = jnp.concatenate([held, moved(held, routes[2])], axis=0)
    held = jnp.concatenate([held, moved(held, routes[3])], axis=0)
    return held, moved(held, routes[4])


def body(
    query_maps,
    key_maps,
    value_rows,
    head_lambda,
    head_gain,
    out_weight,
    token_rows,
    norm_gain,
    expert_ids,
    route_weights,
    gate_weight,
    up_weight,
    down_weight,
):
    z_at = lax.axis_index("z").astype(jnp.int32)
    core_at = lax.axis_index("core").astype(jnp.int32)
    tp_at = lax.axis_index(TP).astype(jnp.int32)
    ids = expert_ids.T
    packed = dispatch(tp_at.reshape(1), token_rows, norm_gain.reshape(1, MODEL), ids)
    arrived = exchanged_rows(packed)
    blocks = collect_keys(key_maps.reshape(TOK, WIDE), value_rows.reshape(TOK, WIDE), core_at)
    queries = query_maps.reshape(TOK, WIDE)
    swapped = across(queries)
    at = z_at.reshape(1), core_at.reshape(1), queries, swapped
    found = attend(*at, blocks[0])
    own, theirs = attend(*at, blocks[1], found)
    other = across(theirs)
    proj = project(head_lambda, own, other, head_gain.reshape(1, WIDE), out_weight)
    high, low = weigh(ids, route_weights.T)
    spread = spread_rows(arrived)
    x = exchanged(spread, TP)
    terms = ffn(x, gate_weight[0], up_weight[0], down_weight[0], proj)
    y = exchanged(terms, TP)
    back, mixed_rows = reduce_terms(y)
    returned = exchanged_rows(back)
    mixed_experts = combine(returned, high, low)
    return (mixed_rows, mixed_experts)


def solution(mesh):
    fine = Mesh(mesh.devices.reshape(Z, CORE, Y, X), ("z", "core", "y", "x"))
    placed = (
        P(EP, TP, None),
        P(EP, TP, None),
        P(EP, TP, None),
        P(TP),
        P(),
        P(TP, None),
        P(EP, None),
        P(),
        P(EP, None),
        P(EP, None),
        P(EP, None, TP),
        P(EP, None, TP),
        P(EP, TP, None),
    )
    return jax.shard_map(
        body,
        mesh=fine,
        in_specs=placed,
        out_specs=(P((*EP, *TP), None), P(EP, TP)),
        check_vma=False,
    )
```

```python
import functools

import jax
import jax.numpy as jnp
from jax import lax
from jax.experimental import pallas as pl
from jax.experimental.pallas import tpu as pltpu
from jax.sharding import Mesh, PartitionSpec as P


NORM_EPS = 1e-05
CLAMP_LIMIT = 7.0
GATE_SLOPE = 1.702
BF16 = jnp.bfloat16
F32 = jnp.float32

Z, CORE, Y, X = 16, 2, 4, 4
EP = ("z", "core")
EP_SENT = ("core", "z")
TP = ("y", "x")
N_EP = Z * CORE
N_TP = Y * X
TOK = 128
CAP = 20
ROWS = N_EP * CAP
QUARTER = 4
WIDE = 128
MODEL = N_TP * WIDE
OUT_ROWS = ROWS + TOK

STEPS = (0, 4, 2, 6, 1, 5, 3, 7)
MIB = 1 << 20


def in_vmem(array):
    return pltpu.with_memory_space_constraint(array, pltpu.VMEM)


def in_hbm(array):
    return pltpu.with_memory_space_constraint(array, pltpu.HBM)


def params(mib):
    return pltpu.CompilerParams(vmem_limit_bytes=mib * MIB)


def routing(ids, values=None):
    block = lax.broadcasted_iota(jnp.int32, (N_EP, TOK), 0)
    expert = CORE * (block % Z) + block // Z
    named = jnp.zeros((N_EP, TOK), F32)
    weight = jnp.zeros((N_EP, TOK), F32)
    for k in range(ids.shape[0]):
        hit = ids[k : k + 1, :] == expert
        named = named + jnp.where(hit, 1.0, 0.0)
        if values is not None:
            weight = weight + jnp.where(hit, values[k : k + 1, :], 0.0)
    earlier = lax.broadcasted_iota(jnp.int32, (TOK, TOK), 0) < lax.broadcasted_iota(
        jnp.int32, (TOK, TOK), 1
    )
    rank = jnp.dot(
        named.astype(BF16),
        jnp.where(earlier, 1.0, 0.0).astype(BF16),
        preferred_element_type=F32,
    )
    slot = jnp.where(named > 0.5, rank, -1.0)
    row = lax.broadcasted_iota(jnp.int32, (ROWS, N_EP), 0)
    first = lax.broadcasted_iota(jnp.int32, (ROWS, N_EP), 1) * CAP
    owner = jnp.where((row >= first) & (row < first + CAP), 1.0, 0.0).astype(BF16)
    parts = [slot, block.astype(F32)]
    if values is not None:
        for _ in range(3):
            parts.append(weight.astype(BF16).astype(F32))
            weight = weight - parts[-1]
    spread = [jnp.dot(owner, p.astype(BF16), preferred_element_type=F32) for p in parts]
    place = lax.broadcasted_iota(jnp.int32, (ROWS, TOK), 0).astype(F32) - CAP * spread[1]
    value = 1.0 if values is None else spread[2] + spread[3] + spread[4]
    return jnp.where(spread[0] == place, value, 0.0)


def dispatch_kernel(at_ref, rows_ref, part_ref, gain_ref, ids_ref, out_ref):
    rows = rows_ref[...].astype(F32)
    mean_sq = jnp.mean(rows * rows, axis=-1, keepdims=True)
    part = part_ref[...].astype(F32) * lax.rsqrt(mean_sq + NORM_EPS) * gain_ref[...]
    chosen = routing(ids_ref[...]).astype(BF16)
    packed = jnp.dot(chosen, part.astype(BF16), preferred_element_type=F32)
    out_ref[...] = packed.astype(BF16)


def dispatch(at, token_rows, gain, ids):
    return pl.pallas_call(
        dispatch_kernel,
        out_shape=jax.ShapeDtypeStruct((ROWS, WIDE), BF16),
        grid_spec=pltpu.PrefetchScalarGridSpec(
            num_scalar_prefetch=1,
            grid=(1,),
            in_specs=[
                pl.BlockSpec((TOK, MODEL), lambda i, at: (0, 0)),
                pl.BlockSpec((TOK, WIDE), lambda i, at: (0, at[0])),
                pl.BlockSpec((1, WIDE), lambda i, at: (0, at[0])),
                pl.BlockSpec((4, TOK), lambda i, at: (0, 0)),
            ],
            out_specs=pl.BlockSpec((ROWS, WIDE), lambda i, at: (0, 0)),
        ),
        compiler_params=params(8),
        name="dispatch",
    )(at, *(in_hbm(a) for a in (token_rows, token_rows, gain, ids)))


def spread_kernel(in_ref, out_hbm, sems):
    copies = [
        pltpu.make_async_copy(in_ref, out_hbm.at[t], sems.at[t]) for t in range(N_TP)
    ]
    for copy in copies:
        copy.start()
    for copy in copies:
        copy.wait()


def spread_rows(rows):
    return pl.pallas_call(
        spread_kernel,
        out_shape=pltpu.HBM((N_TP, ROWS, WIDE), BF16),
        in_specs=[pl.BlockSpec(memory_space=pltpu.VMEM)],
        out_specs=pl.BlockSpec(memory_space=pl.ANY),
        scratch_shapes=[pltpu.SemaphoreType.DMA((N_TP,))],
        compiler_params=params(4),
        name="spread_rows",
    )(in_vmem(rows))


def spread_kernel(in_ref, out_hbm, sems):
    copies = [
        pltpu.make_async_copy(in_ref, out_hbm.at[t], sems.at[t]) for t in range(N_TP)
    ]
    for copy in copies:
        copy.start()
    for copy in copies:
        copy.wait()


def spread_rows(rows):
    return pl.pallas_call(
        spread_kernel,
        out_shape=pltpu.HBM((N_TP, ROWS, WIDE), BF16),
        in_specs=[pl.BlockSpec(memory_space=pltpu.VMEM)],
        out_specs=pl.BlockSpec(memory_space=pl.ANY),
        scratch_shapes=[pltpu.SemaphoreType.DMA((N_TP,))],
        compiler_params=params(4),
        name="spread_rows",
    )(in_vmem(rows))


DOWN_COLS = 4 * WIDE


def ffn_kernel(x_ref, wg_hbm, wu_hbm, wd_hbm, proj_ref, out_ref, pair_ref, wd_ref, sems):
    units = wg_hbm.shape[1]
    loads = [
        pltpu.make_async_copy(wg_hbm, pair_ref.at[:, pl.ds(0, units)], sems.at[0]),
        pltpu.make_async_copy(wu_hbm, pair_ref.at[:, pl.ds(units, units)], sems.at[1]),
        pltpu.make_async_copy(wd_hbm, wd_ref, sems.at[2]),
    ]
    for load in loads:
        load.start()
    out_ref[:, ROWS:, :] = proj_ref[...]
    rows = jnp.concatenate([x_ref[t] for t in range(N_TP)], axis=-1)
    loads[0].wait()
    loads[1].wait()
    both = jnp.dot(rows, pair_ref[...], preferred_element_type=F32)
    gated = jnp.minimum(both[:, :units], CLAMP_LIMIT)
    clipped = jnp.clip(both[:, units:], -CLAMP_LIMIT, CLAMP_LIMIT)
    active = ((clipped + 1.0) * gated * jax.nn.sigmoid(GATE_SLOPE * gated)).astype(BF16)
    loads[2].wait()
    for low in range(0, MODEL, DOWN_COLS):
        terms = jnp.dot(active, wd_ref[:, low : low + DOWN_COLS], preferred_element_type=F32)
        for t in range(DOWN_COLS // WIDE):
            part = terms[:, t * WIDE : (t + 1) * WIDE].astype(BF16)
            out_ref[low // WIDE + t, :ROWS, :] = part


def ffn(x, wg, wu, wd, proj):
    vmem = pl.BlockSpec(memory_space=pltpu.VMEM)
    hbm = pl.BlockSpec(memory_space=pl.ANY)
    return pl.pallas_call(
        ffn_kernel,
        out_shape=pltpu.VMEM((N_TP, OUT_ROWS, WIDE), BF16),
        in_specs=[vmem, hbm, hbm, hbm, vmem],
        out_specs=vmem,
        scratch_shapes=[
            pltpu.VMEM((MODEL, 2 * wg.shape[1]), BF16),
            pltpu.VMEM(wd.shape, BF16),
            pltpu.SemaphoreType.DMA((3,)),
        ],
        compiler_params=params(16),
        name="ffn",
    )(in_vmem(x), *(in_hbm(w) for w in (wg, wu, wd)), in_vmem(proj))


SUM_ROWS = 32


def summed_rows(in_ref, low, count):
    total = in_ref[0, low : low + count, :].astype(F32)
    for t in range(1, N_TP):
        total = total + in_ref[t, low : low + count, :].astype(F32)
    return total.astype(BF16)


def reduce_kernel(in_ref, pack_ref, mixed_ref):
    for low in range(0, ROWS, SUM_ROWS):
        pack_ref[low : low + SUM_ROWS, :] = summed_rows(in_ref, low, SUM_ROWS)
    for c in range(N_TP):
        mixed_ref[:, c * WIDE : (c + 1) * WIDE] = summed_rows(in_ref, ROWS + 8 * c, 8)


def reduce_terms(y):
    vmem = pl.BlockSpec(memory_space=pltpu.VMEM)
    return pl.pallas_call(
        reduce_kernel,
        out_shape=(
            jax.ShapeDtypeStruct((ROWS, WIDE), BF16),
            jax.ShapeDtypeStruct((TOK // N_TP, MODEL), BF16),
        ),
        in_specs=[vmem],
        out_specs=(vmem, vmem),
        compiler_params=params(8),
        name="reduce_terms",
    )(in_vmem(y))


def weigh_kernel(ids_ref, weights_ref, high_ref, low_ref):
    spread = routing(ids_ref[...], weights_ref[...]).T
    high = spread.astype(BF16)
    high_ref[...] = high
    low_ref[...] = (spread - high.astype(F32)).astype(BF16)


def weigh(ids, weights):
    vmem = pl.BlockSpec(memory_space=pltpu.VMEM)
    return pl.pallas_call(
        weigh_kernel,
        out_shape=(pltpu.VMEM((TOK, ROWS), BF16),) * 2,
        in_specs=[vmem] * 2,
        out_specs=(vmem, vmem),
        compiler_params=params(8),
        name="weigh",
    )(ids, weights)


def combine_kernel(back_ref, high_ref, low_ref, out_ref):
    back = back_ref[...]
    mixed = jnp.dot(high_ref[...], back, preferred_element_type=F32)
    mixed = mixed + jnp.dot(low_ref[...], back, preferred_element_type=F32)
    out_ref[...] = mixed.astype(BF16)


def combine(back, high, low):
    vmem = pl.BlockSpec(memory_space=pltpu.VMEM)
    return pl.pallas_call(
        combine_kernel,
        out_shape=jax.ShapeDtypeStruct((TOK, WIDE), BF16),
        in_specs=[vmem] * 3,
        out_specs=vmem,
        compiler_params=params(8),
        name="combine",
    )(*(in_vmem(a) for a in (back, high, low)))


def attend_kernel(late, z_ref, core_ref, q_ref, swapped_ref, keys_ref, *refs):
    found_ref, *out_refs, score_ref = refs if late else (None, *refs)
    lane = lax.broadcasted_iota(jnp.int32, (TOK, WIDE), 1)
    parts = []
    for ref in (q_ref, swapped_ref):
        q = (ref[...].astype(F32) * (64**-0.5)).astype(BF16)
        zero = jnp.zeros_like(q)
        parts += [jnp.where(lane < 64, q, zero), jnp.where(lane < 64, zero, q)]
    queries = jnp.concatenate(parts, axis=0)
    row = lax.broadcasted_iota(jnp.int32, (2 * TOK, TOK), 0)
    row = jnp.where(row < TOK, row, row - TOK)
    ahead = lax.broadcasted_iota(jnp.int32, (2 * TOK, TOK), 1) - row
    z, core = z_ref[0], core_ref[0]
    mine, theirs = CORE * z + core, CORE * z + 1 - core
    blocks = []
    for step in STEPS[4:] if late else STEPS[:4]:
        down = CORE * ((z - step) & (Z - 1))
        up = CORE * ((z + 1 + step) & (Z - 1))
        blocks += [jnp.where(core == 0, down + 1, up), jnp.where(core == 0, down, up + 1)]
    top = jnp.full((4 * TOK, TOK), -1e30, F32)
    for n in range(0, len(blocks), 2):
        keys = keys_ref[n : n + 2, :, :WIDE].reshape(2 * TOK, WIDE)
        scores = lax.dot_general(
            queries, keys, (((1,), (1,)), ((), ())), preferred_element_type=F32
        )
        for h in range(2):
            cols = slice(h * TOK, (h + 1) * TOK)
            part = jnp.concatenate(
                [
                    jnp.where(
                        ahead <= (who - blocks[n + h]) * TOK,
                        scores[2 * TOK * i : 2 * TOK * (i + 1), cols],
                        -1e30,
                    )
                    for i, who in enumerate((mine, theirs))
                ],
                axis=0,
            )
            score_ref[n // 2, :, cols] = part
            top = jnp.maximum(top, part)
    row_max = jnp.max(top, axis=-1, keepdims=True)
    if late:
        row_max = jnp.maximum(row_max, found_ref[:, WIDE : WIDE + 1])
    total = jnp.zeros((4 * TOK, 2 * TOK), F32)
    value_sum = jnp.zeros((4 * TOK, WIDE), F32)
    for n in range(0, len(blocks), 2):
        terms = jnp.exp(score_ref[n // 2] - row_max)
        total = total + terms
        values = keys_ref[n : n + 2, :, WIDE:].reshape(2 * TOK, WIDE)
        value_sum = value_sum + jnp.dot(terms.astype(BF16), values, preferred_element_type=F32)
    total = jnp.sum(total, axis=-1, keepdims=True)
    if late:
        scale = jnp.exp(found_ref[:, WIDE : WIDE + 1] - row_max)
        total = total + found_ref[:, WIDE + 64 : WIDE + 65] * scale
        value_sum = value_sum + found_ref[:, :WIDE] * scale
    wide = lax.broadcasted_iota(jnp.int32, (4 * TOK, WIDE), 1)
    beside = jnp.where(wide < 64, row_max, total)
    count = 4 * TOK // len(out_refs)
    for i, ref in enumerate(out_refs):
        ref[:, :WIDE] = value_sum[i * count : (i + 1) * count]
        ref[:, WIDE:] = beside[i * count : (i + 1) * count]


def attend(z_at, core_at, q, swapped, keys, found=None):
    vmem = pl.BlockSpec(memory_space=pltpu.VMEM)
    smem = pl.BlockSpec(memory_space=pltpu.SMEM)
    late = found is not None
    out = ((2 * TOK, 2 * WIDE),) * 2 if late else ((4 * TOK, 2 * WIDE),)
    return pl.pallas_call(
        functools.partial(attend_kernel, late),
        out_shape=tuple(jax.ShapeDtypeStruct(shape, F32) for shape in out),
        in_specs=[smem] * 2 + [vmem] * (4 if late else 3),
        out_specs=(vmem,) * len(out),
        scratch_shapes=[pltpu.VMEM((Z // 4, 4 * TOK, 2 * TOK), F32)],
        compiler_params=params(14),
        name="attend_late" if late else "attend_early",
    )(z_at, core_at, q, swapped, keys, *(found or ()))


def project_kernel(lam_ref, own_ref, other_ref, gain_ref, w_ref, out_ref):
    tops = [ref[:, WIDE : WIDE + 1] for ref in (own_ref, other_ref)]
    totals = [ref[:, WIDE + 64 : WIDE + 65] for ref in (own_ref, other_ref)]
    top = jnp.maximum(*tops)
    scales = [jnp.exp(t - top) for t in tops]
    total = totals[0] * scales[0] + totals[1] * scales[1]
    ratio = (own_ref[:, :WIDE] * scales[0] + other_ref[:, :WIDE] * scales[1]) / total
    attended = ratio[:TOK] - lam_ref[0] * ratio[TOK:]
    mean_sq = jnp.mean(attended * attended, axis=-1, keepdims=True)
    head_rows = (attended * lax.rsqrt(mean_sq + NORM_EPS) * gain_ref[...]).astype(BF16)
    product = jnp.dot(head_rows, w_ref[...], preferred_element_type=F32).astype(BF16)
    for c in range(N_TP):
        piece = product[:, c * WIDE : (c + 1) * WIDE].reshape(N_TP, TOK // N_TP, WIDE)
        out_ref[:, 8 * c : 8 * (c + 1), :] = piece


def project(lam, own, other, gain, w):
    vmem = pl.BlockSpec(memory_space=pltpu.VMEM)
    return pl.pallas_call(
        project_kernel,
        out_shape=pltpu.VMEM((N_TP, TOK, WIDE), BF16),
        in_specs=[pl.BlockSpec(memory_space=pltpu.SMEM)] + [vmem] * 4,
        out_specs=vmem,
        compiler_params=params(8),
        name="project",
    )(lam, own, other, gain, in_hbm(w))


def key_routes():
    devices = [(z, core) for z in range(Z) for core in range(CORE)]
    held = {(z, core): {(z + core) % Z} for z, core in devices}
    stages = []
    for by in (4, 2, 1):
        sender = {(z, c): ((z + by if c else z - by) % Z, c) for z, c in devices}
        stages.append((sender, held))
        if by > 1:
            held = {d: held[d] | held[sender[d]] for d in devices}
    need = {d: {chip for chip in held[d] if chip <= d[0]} for d in devices}
    routes = []
    for n, (sender, before) in reversed(list(enumerate(stages))):
        last = n == len(stages) - 1
        earlier = {d: need[d] & before[d] for d in devices}
        pairs = []
        for d in devices:
            used = before[sender[d]] & ({*range(d[0] + 1)} if last else need[d])
            if used:
                pairs.append((sender[d], d))
                earlier[sender[d]] = earlier[sender[d]] | used
        routes.insert(0, pairs)
        need = earlier
    first = [((z, 1), (z, 0)) for z in range(Z) if need[z, 0]]
    first += [(((z + 1) % Z, 0), (z, 1)) for z in range(Z) if need[z, 1]]
    second = [(((z + 1) % Z, 1), (z, 1)) for z in range(Z) if need[z, 1]]
    return [first, second, *routes]


def moved(array, pairs):
    flat = [(a[0] * CORE + a[1], b[0] * CORE + b[1]) for a, b in pairs]
    return lax.ppermute(array, EP, flat)


def across(array):
    return moved(array, [((z, 1 - core), (z, core)) for z in range(Z) for core in range(CORE)])


def exchanged(array, axes):
    return lax.all_to_all(array, axes, split_axis=0, concat_axis=0, tiled=True)


def exchanged_rows(rows):
    return exchanged(rows.reshape(ROWS // QUARTER, QUARTER, WIDE), EP_SENT).reshape(ROWS, WIDE)


def collect_keys(keys, values, core_at):
    routes = key_routes()
    mine = jnp.concatenate([keys, values], axis=-1)
    first = moved(mine, routes[0])
    second = moved(mine, routes[1])
    held = jnp.stack([first, jnp.where(core_at == 0, mine, second)])
    held = jnp.concatenate([held, moved(held, routes[2])], axis=0)
    held = jnp.concatenate([held, moved(held, routes[3])], axis=0)
    return held, moved(held, routes[4])


def body(
    query_maps,
    key_maps,
    value_rows,
    head_lambda,
    head_gain,
    out_weight,
    token_rows,
    norm_gain,
    expert_ids,
    route_weights,
    gate_weight,
    up_weight,
    down_weight,
):
    z_at = lax.axis_index("z").astype(jnp.int32)
    core_at = lax.axis_index("core").astype(jnp.int32)
    tp_at = lax.axis_index(TP).astype(jnp.int32)
    ids = expert_ids.T
    packed = dispatch(tp_at.reshape(1), token_rows, norm_gain.reshape(1, MODEL), ids)
    arrived = exchanged_rows(packed)
    blocks = collect_keys(key_maps.reshape(TOK, WIDE), value_rows.reshape(TOK, WIDE), core_at)
    queries = query_maps.reshape(TOK, WIDE)
    swapped = across(queries)
    at = z_at.reshape(1), core_at.reshape(1), queries, swapped
    found = attend(*at, blocks[0])
    own, theirs = attend(*at, blocks[1], found)
    other = across(theirs)
    proj = project(head_lambda, own, other, head_gain.reshape(1, WIDE), out_weight)
    high, low = weigh(ids, route_weights.T)
    spread = spread_rows(arrived)
    x = exchanged(spread, TP)
    terms = ffn(x, gate_weight[0], up_weight[0], down_weight[0], proj)
    y = exchanged(terms, TP)
    back, mixed_rows = reduce_terms(y)
    returned = exchanged_rows(back)
    mixed_experts = combine(returned, high, low)
    return (mixed_rows, mixed_experts)


def solution(mesh):
    fine = Mesh(mesh.devices.reshape(Z, CORE, Y, X), ("z", "core", "y", "x"))
    placed = (
        P(EP, TP, None),
        P(EP, TP, None),
        P(EP, TP, None),
        P(TP),
        P(),
        P(TP, None),
        P(EP, None),
        P(),
        P(EP, None),
        P(EP, None),
        P(EP, None, TP),
        P(EP, None, TP),
        P(EP, TP, None),
    )
    return jax.shard_map(
        body,
        mesh=fine,
        in_specs=placed,
        out_specs=(P((*EP, *TP), None), P(EP, TP)),
        check_vma=False,
    )
```

```python
import functools

import jax
import jax.numpy as jnp
from jax import lax
from jax.experimental import pallas as pl
from jax.experimental.pallas import tpu as pltpu
from jax.sharding import Mesh, PartitionSpec as P


NORM_EPS = 1e-05
CLAMP_LIMIT = 7.0
GATE_SLOPE = 1.702
BF16 = jnp.bfloat16
F32 = jnp.float32

Z, CORE, Y, X = 16, 2, 4, 4
EP = ("z", "core")
TP = ("y", "x")
N_EP = Z * CORE
N_TP = Y * X
TOK = 128
CAP = 20
ROWS = N_EP * CAP
QUARTER = 4
WIDE = 128
MODEL = N_TP * WIDE
OUT_ROWS = ROWS + TOK

STEPS = (0, 4, 2, 6, 1, 5, 3, 7)
MIB = 1 << 20


def in_vmem(array):
    return pltpu.with_memory_space_constraint(array, pltpu.VMEM)


def in_hbm(array):
    return pltpu.with_memory_space_constraint(array, pltpu.HBM)


def params(mib):
    return pltpu.CompilerParams(vmem_limit_bytes=mib * MIB)


def routing(ids, values=None):
    expert = lax.broadcasted_iota(jnp.int32, (N_EP, TOK), 0)
    named = jnp.zeros((N_EP, TOK), F32)
    weight = jnp.zeros((N_EP, TOK), F32)
    for k in range(ids.shape[0]):
        hit = ids[k : k + 1, :] == expert
        named = named + jnp.where(hit, 1.0, 0.0)
        if values is not None:
            weight = weight + jnp.where(hit, values[k : k + 1, :], 0.0)
    earlier = lax.broadcasted_iota(jnp.int32, (TOK, TOK), 0) < lax.broadcasted_iota(
        jnp.int32, (TOK, TOK), 1
    )
    rank = jnp.dot(
        named.astype(BF16),
        jnp.where(earlier, 1.0, 0.0).astype(BF16),
        preferred_element_type=F32,
    )
    slot = jnp.where(named > 0.5, rank, -1.0)
    row = lax.broadcasted_iota(jnp.int32, (ROWS, N_EP), 0)
    first = lax.broadcasted_iota(jnp.int32, (ROWS, N_EP), 1) * CAP
    owner = jnp.where((row >= first) & (row < first + CAP), 1.0, 0.0).astype(BF16)
    parts = [slot, expert.astype(F32)]
    if values is not None:
        for _ in range(3):
            parts.append(weight.astype(BF16).astype(F32))
            weight = weight - parts[-1]
    spread = [jnp.dot(owner, p.astype(BF16), preferred_element_type=F32) for p in parts]
    place = lax.broadcasted_iota(jnp.int32, (ROWS, TOK), 0).astype(F32) - CAP * spread[1]
    value = 1.0 if values is None else spread[2] + spread[3] + spread[4]
    return jnp.where(spread[0] == place, value, 0.0)


def dispatch_kernel(at_ref, rows_ref, part_ref, gain_ref, ids_ref, out_ref):
    rows = rows_ref[...].astype(F32)
    mean_sq = jnp.mean(rows * rows, axis=-1, keepdims=True)
    part = part_ref[...].astype(F32) * lax.rsqrt(mean_sq + NORM_EPS) * gain_ref[...]
    chosen = routing(ids_ref[...]).astype(BF16)
    packed = jnp.dot(chosen, part.astype(BF16), preferred_element_type=F32)
    out_ref[...] = packed.astype(BF16)


def dispatch(at, token_rows, gain, ids):
    return pl.pallas_call(
        dispatch_kernel,
        out_shape=jax.ShapeDtypeStruct((ROWS, WIDE), BF16),
        grid_spec=pltpu.PrefetchScalarGridSpec(
            num_scalar_prefetch=1,
            grid=(1,),
            in_specs=[
                pl.BlockSpec((TOK, MODEL), lambda i, at: (0, 0)),
                pl.BlockSpec((TOK, WIDE), lambda i, at: (0, at[0])),
                pl.BlockSpec((1, WIDE), lambda i, at: (0, at[0])),
                pl.BlockSpec((4, TOK), lambda i, at: (0, 0)),
            ],
            out_specs=pl.BlockSpec((ROWS, WIDE), lambda i, at: (0, 0)),
        ),
        compiler_params=params(8),
        name="dispatch",
    )(at, *(in_hbm(a) for a in (token_rows, token_rows, gain, ids)))


def spread_kernel(in_ref, out_hbm, sems):
    copies = [
        pltpu.make_async_copy(in_ref, out_hbm.at[t], sems.at[t]) for t in range(N_TP)
    ]
    for copy in copies:
        copy.start()
    for copy in copies:
        copy.wait()


def spread_rows(rows):
    return pl.pallas_call(
        spread_kernel,
        out_shape=pltpu.HBM((N_TP, ROWS, WIDE), BF16),
        in_specs=[pl.BlockSpec(memory_space=pltpu.VMEM)],
        out_specs=pl.BlockSpec(memory_space=pl.ANY),
        scratch_shapes=[pltpu.SemaphoreType.DMA((N_TP,))],
        compiler_params=params(4),
        name="spread_rows",
    )(in_vmem(rows))


def spread_kernel(in_ref, out_hbm, sems):
    copies = [
        pltpu.make_async_copy(in_ref, out_hbm.at[t], sems.at[t]) for t in range(N_TP)
    ]
    for copy in copies:
        copy.start()
    for copy in copies:
        copy.wait()


def spread_rows(rows):
    return pl.pallas_call(
        spread_kernel,
        out_shape=pltpu.HBM((N_TP, ROWS, WIDE), BF16),
        in_specs=[pl.BlockSpec(memory_space=pltpu.VMEM)],
        out_specs=pl.BlockSpec(memory_space=pl.ANY),
        scratch_shapes=[pltpu.SemaphoreType.DMA((N_TP,))],
        compiler_params=params(4),
        name="spread_rows",
    )(in_vmem(rows))


DOWN_COLS = 4 * WIDE


def ffn_kernel(x_ref, wg_hbm, wu_hbm, wd_hbm, proj_ref, out_ref, pair_ref, wd_ref, sems):
    units = wg_hbm.shape[1]
    loads = [
        pltpu.make_async_copy(wg_hbm, pair_ref.at[:, pl.ds(0, units)], sems.at[0]),
        pltpu.make_async_copy(wu_hbm, pair_ref.at[:, pl.ds(units, units)], sems.at[1]),
        pltpu.make_async_copy(wd_hbm, wd_ref, sems.at[2]),
    ]
    for load in loads:
        load.start()
    out_ref[:, ROWS:, :] = proj_ref[...]
    rows = jnp.concatenate([x_ref[t] for t in range(N_TP)], axis=-1)
    loads[0].wait()
    loads[1].wait()
    both = jnp.dot(rows, pair_ref[...], preferred_element_type=F32)
    gated = jnp.minimum(both[:, :units], CLAMP_LIMIT)
    clipped = jnp.clip(both[:, units:], -CLAMP_LIMIT, CLAMP_LIMIT)
    active = ((clipped + 1.0) * gated * jax.nn.sigmoid(GATE_SLOPE * gated)).astype(BF16)
    loads[2].wait()
    for low in range(0, MODEL, DOWN_COLS):
        terms = jnp.dot(active, wd_ref[:, low : low + DOWN_COLS], preferred_element_type=F32)
        for t in range(DOWN_COLS // WIDE):
            part = terms[:, t * WIDE : (t + 1) * WIDE].astype(BF16)
            out_ref[low // WIDE + t, :ROWS, :] = part


def ffn(x, wg, wu, wd, proj):
    vmem = pl.BlockSpec(memory_space=pltpu.VMEM)
    hbm = pl.BlockSpec(memory_space=pl.ANY)
    return pl.pallas_call(
        ffn_kernel,
        out_shape=pltpu.VMEM((N_TP, OUT_ROWS, WIDE), BF16),
        in_specs=[vmem, hbm, hbm, hbm, vmem],
        out_specs=vmem,
        scratch_shapes=[
            pltpu.VMEM((MODEL, 2 * wg.shape[1]), BF16),
            pltpu.VMEM(wd.shape, BF16),
            pltpu.SemaphoreType.DMA((3,)),
        ],
        compiler_params=params(16),
        name="ffn",
    )(in_vmem(x), *(in_hbm(w) for w in (wg, wu, wd)), in_vmem(proj))


SUM_ROWS = 32


def summed_rows(in_ref, low, count):
    total = in_ref[0, low : low + count, :].astype(F32)
    for t in range(1, N_TP):
        total = total + in_ref[t, low : low + count, :].astype(F32)
    return total.astype(BF16)


def reduce_kernel(in_ref, pack_ref, mixed_ref):
    for low in range(0, ROWS, SUM_ROWS):
        pack_ref[low : low + SUM_ROWS, :] = summed_rows(in_ref, low, SUM_ROWS)
    for c in range(N_TP):
        mixed_ref[:, c * WIDE : (c + 1) * WIDE] = summed_rows(in_ref, ROWS + 8 * c, 8)


def reduce_terms(y):
    vmem = pl.BlockSpec(memory_space=pltpu.VMEM)
    return pl.pallas_call(
        reduce_kernel,
        out_shape=(
            jax.ShapeDtypeStruct((ROWS, WIDE), BF16),
            jax.ShapeDtypeStruct((TOK // N_TP, MODEL), BF16),
        ),
        in_specs=[vmem],
        out_specs=(vmem, vmem),
        compiler_params=params(8),
        name="reduce_terms",
    )(in_vmem(y))


def weigh_kernel(ids_ref, weights_ref, high_ref, low_ref):
    spread = routing(ids_ref[...], weights_ref[...]).T
    high = spread.astype(BF16)
    high_ref[...] = high
    low_ref[...] = (spread - high.astype(F32)).astype(BF16)


def weigh(ids, weights):
    vmem = pl.BlockSpec(memory_space=pltpu.VMEM)
    return pl.pallas_call(
        weigh_kernel,
        out_shape=(pltpu.VMEM((TOK, ROWS), BF16),) * 2,
        in_specs=[vmem] * 2,
        out_specs=(vmem, vmem),
        compiler_params=params(8),
        name="weigh",
    )(ids, weights)


def combine_kernel(back_ref, high_ref, low_ref, out_ref):
    back = back_ref[...]
    mixed = jnp.dot(high_ref[...], back, preferred_element_type=F32)
    mixed = mixed + jnp.dot(low_ref[...], back, preferred_element_type=F32)
    out_ref[...] = mixed.astype(BF16)


def combine(back, high, low):
    vmem = pl.BlockSpec(memory_space=pltpu.VMEM)
    return pl.pallas_call(
        combine_kernel,
        out_shape=jax.ShapeDtypeStruct((TOK, WIDE), BF16),
        in_specs=[vmem] * 3,
        out_specs=vmem,
        compiler_params=params(8),
        name="combine",
    )(*(in_vmem(a) for a in (back, high, low)))


def attend_kernel(late, z_ref, core_ref, q_ref, swapped_ref, keys_ref, *refs):
    found_ref, *out_refs, score_ref = refs if late else (None, *refs)
    lane = lax.broadcasted_iota(jnp.int32, (TOK, WIDE), 1)
    parts = []
    for ref in (q_ref, swapped_ref):
        q = (ref[...].astype(F32) * (64**-0.5)).astype(BF16)
        zero = jnp.zeros_like(q)
        parts += [jnp.where(lane < 64, q, zero), jnp.where(lane < 64, zero, q)]
    queries = jnp.concatenate(parts, axis=0)
    row = lax.broadcasted_iota(jnp.int32, (2 * TOK, TOK), 0)
    row = jnp.where(row < TOK, row, row - TOK)
    ahead = lax.broadcasted_iota(jnp.int32, (2 * TOK, TOK), 1) - row
    z, core = z_ref[0], core_ref[0]
    mine, theirs = CORE * z + core, CORE * z + 1 - core
    blocks = []
    for step in STEPS[4:] if late else STEPS[:4]:
        down = CORE * ((z - step) & (Z - 1))
        up = CORE * ((z + 1 + step) & (Z - 1))
        blocks += [jnp.where(core == 0, down + 1, up), jnp.where(core == 0, down, up + 1)]
    top = jnp.full((4 * TOK, TOK), -1e30, F32)
    for n in range(0, len(blocks), 2):
        keys = keys_ref[n : n + 2, :, :WIDE].reshape(2 * TOK, WIDE)
        scores = lax.dot_general(
            queries, keys, (((1,), (1,)), ((), ())), preferred_element_type=F32
        )
        for h in range(2):
            cols = slice(h * TOK, (h + 1) * TOK)
            part = jnp.concatenate(
                [
                    jnp.where(
                        ahead <= (who - blocks[n + h]) * TOK,
                        scores[2 * TOK * i : 2 * TOK * (i + 1), cols],
                        -1e30,
                    )
                    for i, who in enumerate((mine, theirs))
                ],
                axis=0,
            )
            score_ref[n // 2, :, cols] = part
            top = jnp.maximum(top, part)
    row_max = jnp.max(top, axis=-1, keepdims=True)
    if late:
        row_max = jnp.maximum(row_max, found_ref[:, WIDE : WIDE + 1])
    total = jnp.zeros((4 * TOK, 2 * TOK), F32)
    value_sum = jnp.zeros((4 * TOK, WIDE), F32)
    for n in range(0, len(blocks), 2):
        terms = jnp.exp(score_ref[n // 2] - row_max)
        total = total + terms
        values = keys_ref[n : n + 2, :, WIDE:].reshape(2 * TOK, WIDE)
        value_sum = value_sum + jnp.dot(terms.astype(BF16), values, preferred_element_type=F32)
    total = jnp.sum(total, axis=-1, keepdims=True)
    if late:
        scale = jnp.exp(found_ref[:, WIDE : WIDE + 1] - row_max)
        total = total + found_ref[:, WIDE + 64 : WIDE + 65] * scale
        value_sum = value_sum + found_ref[:, :WIDE] * scale
    wide = lax.broadcasted_iota(jnp.int32, (4 * TOK, WIDE), 1)
    beside = jnp.where(wide < 64, row_max, total)
    count = 4 * TOK // len(out_refs)
    for i, ref in enumerate(out_refs):
        ref[:, :WIDE] = value_sum[i * count : (i + 1) * count]
        ref[:, WIDE:] = beside[i * count : (i + 1) * count]


def attend(z_at, core_at, q, swapped, keys, found=None):
    vmem = pl.BlockSpec(memory_space=pltpu.VMEM)
    smem = pl.BlockSpec(memory_space=pltpu.SMEM)
    late = found is not None
    out = ((2 * TOK, 2 * WIDE),) * 2 if late else ((4 * TOK, 2 * WIDE),)
    return pl.pallas_call(
        functools.partial(attend_kernel, late),
        out_shape=tuple(jax.ShapeDtypeStruct(shape, F32) for shape in out),
        in_specs=[smem] * 2 + [vmem] * (4 if late else 3),
        out_specs=(vmem,) * len(out),
        scratch_shapes=[pltpu.VMEM((Z // 4, 4 * TOK, 2 * TOK), F32)],
        compiler_params=params(14),
        name="attend_late" if late else "attend_early",
    )(z_at, core_at, q, swapped, keys, *(found or ()))


def project_kernel(lam_ref, own_ref, other_ref, gain_ref, w_ref, out_ref):
    tops = [ref[:, WIDE : WIDE + 1] for ref in (own_ref, other_ref)]
    totals = [ref[:, WIDE + 64 : WIDE + 65] for ref in (own_ref, other_ref)]
    top = jnp.maximum(*tops)
    scales = [jnp.exp(t - top) for t in tops]
    total = totals[0] * scales[0] + totals[1] * scales[1]
    ratio = (own_ref[:, :WIDE] * scales[0] + other_ref[:, :WIDE] * scales[1]) / total
    attended = ratio[:TOK] - lam_ref[0] * ratio[TOK:]
    mean_sq = jnp.mean(attended * attended, axis=-1, keepdims=True)
    head_rows = (attended * lax.rsqrt(mean_sq + NORM_EPS) * gain_ref[...]).astype(BF16)
    product = jnp.dot(head_rows, w_ref[...], preferred_element_type=F32).astype(BF16)
    for c in range(N_TP):
        piece = product[:, c * WIDE : (c + 1) * WIDE].reshape(N_TP, TOK // N_TP, WIDE)
        out_ref[:, 8 * c : 8 * (c + 1), :] = piece


def project(lam, own, other, gain, w):
    vmem = pl.BlockSpec(memory_space=pltpu.VMEM)
    return pl.pallas_call(
        project_kernel,
        out_shape=pltpu.VMEM((N_TP, TOK, WIDE), BF16),
        in_specs=[pl.BlockSpec(memory_space=pltpu.SMEM)] + [vmem] * 4,
        out_specs=vmem,
        compiler_params=params(8),
        name="project",
    )(lam, own, other, gain, in_hbm(w))


def key_routes():
    devices = [(z, core) for z in range(Z) for core in range(CORE)]
    held = {(z, core): {(z + core) % Z} for z, core in devices}
    stages = []
    for by in (4, 2, 1):
        sender = {(z, c): ((z + by if c else z - by) % Z, c) for z, c in devices}
        stages.append((sender, held))
        if by > 1:
            held = {d: held[d] | held[sender[d]] for d in devices}
    need = {d: {chip for chip in held[d] if chip <= d[0]} for d in devices}
    routes = []
    for n, (sender, before) in reversed(list(enumerate(stages))):
        last = n == len(stages) - 1
        earlier = {d: need[d] & before[d] for d in devices}
        pairs = []
        for d in devices:
            used = before[sender[d]] & ({*range(d[0] + 1)} if last else need[d])
            if used:
                pairs.append((sender[d], d))
                earlier[sender[d]] = earlier[sender[d]] | used
        routes.insert(0, pairs)
        need = earlier
    first = [((z, 1), (z, 0)) for z in range(Z) if need[z, 0]]
    first += [(((z + 1) % Z, 0), (z, 1)) for z in range(Z) if need[z, 1]]
    second = [(((z + 1) % Z, 1), (z, 1)) for z in range(Z) if need[z, 1]]
    return [first, second, *routes]


def moved(array, pairs):
    flat = [(a[0] * CORE + a[1], b[0] * CORE + b[1]) for a, b in pairs]
    return lax.ppermute(array, EP, flat)


def across(array):
    return moved(array, [((z, 1 - core), (z, core)) for z in range(Z) for core in range(CORE)])


def exchanged(array, axes):
    return lax.all_to_all(array, axes, split_axis=0, concat_axis=0, tiled=True)


def exchanged_rows(rows):
    return exchanged(rows.reshape(ROWS // QUARTER, QUARTER, WIDE), EP).reshape(ROWS, WIDE)


def collect_keys(keys, values, core_at):
    routes = key_routes()
    mine = jnp.concatenate([keys, values], axis=-1)
    first = moved(mine, routes[0])
    second = moved(mine, routes[1])
    held = jnp.stack([first, jnp.where(core_at == 0, mine, second)])
    held = jnp.concatenate([held, moved(held, routes[2])], axis=0)
    held = jnp.concatenate([held, moved(held, routes[3])], axis=0)
    return held, moved(held, routes[4])


def body(
    query_maps,
    key_maps,
    value_rows,
    head_lambda,
    head_gain,
    out_weight,
    token_rows,
    norm_gain,
    expert_ids,
    route_weights,
    gate_weight,
    up_weight,
    down_weight,
):
    z_at = lax.axis_index("z").astype(jnp.int32)
    core_at = lax.axis_index("core").astype(jnp.int32)
    tp_at = lax.axis_index(TP).astype(jnp.int32)
    ids = expert_ids.T
    packed = dispatch(tp_at.reshape(1), token_rows, norm_gain.reshape(1, MODEL), ids)
    arrived = exchanged_rows(packed)
    blocks = collect_keys(key_maps.reshape(TOK, WIDE), value_rows.reshape(TOK, WIDE), core_at)
    queries = query_maps.reshape(TOK, WIDE)
    swapped = across(queries)
    at = z_at.reshape(1), core_at.reshape(1), queries, swapped
    found = attend(*at, blocks[0])
    own, theirs = attend(*at, blocks[1], found)
    other = across(theirs)
    proj = project(head_lambda, own, other, head_gain.reshape(1, WIDE), out_weight)
    high, low = weigh(ids, route_weights.T)
    spread = spread_rows(arrived)
    x = exchanged(spread, TP)
    terms = ffn(x, gate_weight[0], up_weight[0], down_weight[0], proj)
    y = exchanged(terms, TP)
    back, mixed_rows = reduce_terms(y)
    returned = exchanged_rows(back)
    mixed_experts = combine(returned, high, low)
    return (mixed_rows, mixed_experts)


def solution(mesh):
    fine = Mesh(mesh.devices.reshape(Z, CORE, Y, X), ("z", "core", "y", "x"))
    placed = (
        P(EP, TP, None),
        P(EP, TP, None),
        P(EP, TP, None),
        P(TP),
        P(),
        P(TP, None),
        P(EP, None),
        P(),
        P(EP, None),
        P(EP, None),
        P(EP, None, TP),
        P(EP, None, TP),
        P(EP, TP, None),
    )
    return jax.shard_map(
        body,
        mesh=fine,
        in_specs=placed,
        out_specs=(P((*EP, *TP), None), P(EP, TP)),
        check_vma=False,
    )
```
